128 devices in a mesh: sp: 32 (over z, y, core), tp: 4 (over x).
Axes of the slice: x: 4, y: 4, z: 4, core: 2. Of those that a mesh axis runs over, the one named last changes fastest.
Arguments:
- input_activations: bfloat16 [32768, 2048], P(('sp', 'tp')), may hold values from -6 to 6
- norm_gain: float32 [2048], replicated, may hold values from 0.5 to 1.5
- w_gate: bfloat16 [2048, 2048], P('sp', 'tp'), may hold values from -0.125 to 0.125
- w_value: bfloat16 [2048, 2048], P('sp', 'tp'), may hold values from -0.125 to 0.125
- w_state_in: bfloat16 [2048, 1024], P('sp', 'tp'), may hold values from -0.125 to 0.125
- w_state_out: bfloat16 [2048, 1024], P('sp', 'tp'), may hold values from -0.125 to 0.125
- w_step_forward: bfloat16 [2048, 32], P('sp', 'tp'), may hold values from -0.03125 to 0.03125
- w_step_backward: bfloat16 [2048, 32], P('sp', 'tp'), may hold values from -0.03125 to 0.03125
- step_offset: float32 [2, 32], P(None, 'tp'), may hold values from -0.5 to 0.5
- fading_speed: float32 [2, 32], P(None, 'tp'), may hold values from 0.3 to 1
- conv_value: float32 [3, 2048], P(None, 'tp'), may hold values from -3.5 to 3.5
- conv_state_in: float32 [3, 1024], P(None, 'tp'), may hold values from -3.5 to 3.5
- conv_state_out: float32 [3, 1024], P(None, 'tp'), may hold values from -3.5 to 3.5
- out_gain: float32 [2048], P('tp'), may hold values from 0.5 to 1.5
- w_out: bfloat16 [2048, 2048], P('tp', 'sp'), may hold values from -0.125 to 0.125
Outputs:
- mixer_out: bfloat16 [32768, 2048], P(('sp', 'tp'))
The draws below stay inside these ranges and needn't reach their ends.
All inputs are finite; a program needn't handle non-finite values.
Results may differ from the reference program's by a relative error of at most 0.015.
Values may be sent and summed in bfloat16 or wider, within the bound.
A program may use at most 128 MiB of HBM per device.

```python
import math
import jax
import jax.numpy as jnp
from jax import lax

D = 2048
HEADS = 32
HEAD_DIM = 64
GROUPS = 8
STATE = 128
BLOCK = 128
WIDTH = 2048
SEQ = 32768


def block_levels(rng, dims, split, low, high):
    gain, own = 1.0, jax.random.fold_in(rng, 6)
    for axis_at, shards_of in split:
        heights = jnp.exp(jax.random.uniform(jax.random.fold_in(own, axis_at), (shards_of,), jnp.float32, low / len(split), high / len(split)))
        gain = gain * jnp.repeat(heights, dims[axis_at] // shards_of).reshape([-1 if axis == axis_at else 1 for axis in range(len(dims))])
    return gain


def gaussian(rng, extent, spread, bound, shards=(), dtype=jnp.bfloat16):
    drawn = jax.random.normal(rng, extent, jnp.float32) * spread
    if len(shards) > 0:
        drawn = block_levels(rng, extent, shards, -0.22, 0.18) * drawn
    return jnp.clip(drawn, min=-bound, max=bound).astype(dtype)


def setup_inputs(seed: int = 0) -> dict:
    key_list = jax.random.split(jax.random.key(seed), 16)
    return {
        "input_activations": gaussian(key_list[0], (SEQ, D), 1.0, 6.0, ((0, 128),)),
        "norm_gain": jnp.clip(1.0 + 0.1 * jax.random.normal(key_list[1], (D,), jnp.float32), 0.5, 1.5),
        "w_gate": gaussian(key_list[2], (D, WIDTH), D ** -0.5, 0.125, ((0, 32), (1, 4))),
        "w_value": gaussian(key_list[3], (D, WIDTH), D ** -0.5, 0.125, ((0, 32), (1, 4))),
        "w_state_in": gaussian(key_list[4], (D, GROUPS * STATE), D ** -0.5, 0.125, ((0, 32), (1, 4))),
        "w_state_out": gaussian(key_list[5], (D, GROUPS * STATE), D ** -0.5, 0.125, ((0, 32), (1, 4))),
        "w_step_forward": gaussian(key_list[6], (D, HEADS), (16 * D) ** -0.5, 0.03125, ((0, 32), (1, 4))),
        "w_step_backward": gaussian(key_list[7], (D, HEADS), (16 * D) ** -0.5, 0.03125, ((0, 32), (1, 4))),
        "step_offset": jnp.clip(jax.random.uniform(key_list[8], (2, HEADS), jnp.float32, -0.5, 0.5) * block_levels(key_list[8], (2, HEADS), ((1, 4),), -0.4, 0.0), -0.5, 0.5),
        "fading_speed": jnp.clip(jnp.exp(math.log(1.0) - 1.2039728 * jax.random.uniform(key_list[9], (2, HEADS), jnp.float32) ** block_levels(key_list[9], (2, HEADS), ((1, 4),), -0.2, 0.2)), 0.3, 1.0),
        "conv_value": gaussian(key_list[10], (3, WIDTH), 3 ** -0.5, 3.5, ((1, 4),), jnp.float32),
        "conv_state_in": gaussian(key_list[11], (3, GROUPS * STATE), 3 ** -0.5, 3.5, ((1, 4),), jnp.float32),
        "conv_state_out": gaussian(key_list[12], (3, GROUPS * STATE), 3 ** -0.5, 3.5, ((1, 4),), jnp.float32),
        "out_gain": jnp.clip(1.0 + 0.1 * jax.random.normal(key_list[13], (WIDTH,), jnp.float32), 0.5, 1.5),
        "w_out": gaussian(key_list[14], (WIDTH, D), WIDTH ** -0.5, 0.125, ((0, 4), (1, 32))),
    }


epsilon = 1e-06
HIGHEST_PRECISION = lax.Precision.HIGHEST

def rms_rows(values):
    wide = values.astype(jnp.float32)
    return wide * lax.rsqrt(lax.optimization_barrier(jnp.mean(wide * wide, axis=-1, keepdims=True)) + epsilon)

def short_filter(values, taps):
    wide = values.astype(jnp.float32)
    padded = jnp.pad(wide, ((1, 1), (0, 0)))
    mixed = taps[0] * padded[:-2] + taps[1] * padded[1:-1] + taps[2] * padded[2:]
    return jax.nn.silu(mixed).astype(jnp.bfloat16)

def sweep(signal, step_size, rate, inward, outward):
    sequence_extent = signal.shape[0]
    count = sequence_extent // BLOCK
    ratio = HEADS // GROUPS
    blocks = signal.reshape(count, BLOCK, GROUPS, ratio, HEAD_DIM).astype(jnp.float32)
    step_blocks = step_size.reshape(count, BLOCK, GROUPS, ratio)
    inward_blocks = inward.reshape(count, BLOCK, GROUPS, STATE).astype(jnp.float32)
    outward_blocks = outward.reshape(count, BLOCK, GROUPS, STATE).astype(jnp.float32)
    log_decay = -step_blocks * rate.reshape(GROUPS, ratio)
    lower = (jnp.arange(BLOCK)[:, None] >= jnp.arange(BLOCK)[None, :])[:, :, None, None]

    def advance(state, inputs):
        values, steps, inner, outer, logs = inputs
        within = jnp.cumsum(logs, axis=0)
        gaps = within[:, None] - within[None]
        decay = jnp.where(lower, jnp.exp(jnp.where(lower, gaps, 0.0)), 0.0)
        intersect = jnp.einsum('qgn,kgn->qkg', outer, inner, precision=HIGHEST_PRECISION)
        weights_mix = intersect[..., None] * decay * steps[None]
        result = jnp.einsum('qkgr,kgrp->qgrp', weights_mix, values, precision=HIGHEST_PRECISION)
        result = result + jnp.einsum('qgn,grpn->qgrp', outer, state, precision=HIGHEST_PRECISION) * jnp.exp(within)[..., None]
        final = within[-1]
        scaling_factor = jnp.exp(final[None] - within) * steps
        added = jnp.einsum('qgn,qgrp->grpn', inner, values * scaling_factor[..., None], precision=HIGHEST_PRECISION)
        return (state * jnp.exp(final)[..., None, None] + added, result)
    start_state = jnp.zeros((GROUPS, ratio, HEAD_DIM, STATE), jnp.float32)
    _, outputs = lax.scan(advance, start_state, (blocks, step_blocks, inward_blocks, outward_blocks, log_decay))
    return outputs.reshape(sequence_extent, WIDTH)

def reference(input_activations, norm_gain, w_gate, w_value, w_state_in, w_state_out, w_step_forward, w_step_backward, step_offset, fading_speed, conv_value, conv_state_in, conv_state_out, out_gain, w_out):
    normed = (rms_rows(input_activations) * norm_gain).astype(jnp.bfloat16)

    def project(scaling_factor):
        return jnp.dot(normed, scaling_factor, preferred_element_type=jnp.float32).astype(jnp.bfloat16)
    gate = project(w_gate)
    value = project(w_value)
    inward_raw = project(w_state_in)
    outward_raw = project(w_state_out)
    raw_forward = project(w_step_forward)
    raw_backward = project(w_step_backward)
    shift = math.log(SEQ)
    step_forward = jax.nn.softplus(raw_forward.astype(jnp.float32) + step_offset[0] - shift)
    step_backward = jax.nn.softplus(raw_backward.astype(jnp.float32) + step_offset[1] - shift)
    signal = short_filter(value, conv_value).reshape(SEQ, HEADS, HEAD_DIM)
    inward = short_filter(inward_raw, conv_state_in).reshape(SEQ, GROUPS, STATE)
    outward = short_filter(outward_raw, conv_state_out).reshape(SEQ, GROUPS, STATE)
    forward = sweep(signal, step_forward, fading_speed[0], inward, outward)
    backward = sweep(signal[::-1], step_backward[::-1], fading_speed[1], inward[::-1], outward[::-1])[::-1]
    gated = (forward + backward) * jax.nn.silu(gate.astype(jnp.float32))
    grouped = rms_rows(gated.reshape(SEQ, GROUPS, WIDTH // GROUPS)).reshape(SEQ, WIDTH)
    mixed = (grouped * out_gain).astype(jnp.bfloat16)
    return jnp.dot(mixed, w_out, preferred_element_type=jnp.float32).astype(jnp.bfloat16)
```

```python
import functools
import math

import jax
import jax.numpy as jnp
from jax import lax
from jax.experimental import pallas as pl
from jax.experimental.pallas import tpu as pltpu
from jax.sharding import Mesh
from jax.sharding import PartitionSpec as P

HEAD_DIM = 64
STATE = 128
BLOCK = 128
SP = ("z", "y", "c")
SP_TP = ("z", "y", "c", "x")
EPSILON = 1e-06
MESH = pl.DeviceIdType.MESH
HALO = 16


def place():
    return [lax.axis_index(name) for name in ("z", "y", "c", "x")]


def step(at, by):
    return lax.rem(at + by + 4, 4)


def stretch_at(z, y, c, by):
    n = lax.rem(z * 8 + y * 2 + c + by + 32, 32)
    return {"z": n // 8, "y": lax.rem(n // 2, 4), "c": lax.rem(n, 2)}


class Wire:
    def __init__(self, send, recv):
        self.send, self.recv, self.count, self.sent = send, recv, 0, []

    def describe(self, ref, to):
        k = self.count
        self.count += 1
        return pltpu.make_async_remote_copy(
            src_ref=ref,
            dst_ref=ref,
            send_sem=self.send.at[k],
            recv_sem=self.recv.at[k],
            device_id=to,
            device_id_type=MESH,
        )

    def go(self, ref, to):
        copy = self.describe(ref, to)
        copy.start()
        self.sent.append(copy)
        return copy

    def drain(self):
        for copy in self.sent:
            copy.wait_send()


class Ring:
    def __init__(self, wire, axis, at, block, low, high):
        self.wire, self.at = wire, at
        self.up, self.down = {axis: step(at, 1)}, {axis: step(at, 3)}
        self.block, self.low, self.high = block, low, high

    def start(self):
        self.a = self.wire.go(self.block(self.at), self.up)
        self.b = self.wire.go(self.block(self.at), self.down)

    def forward(self):
        self.a.wait_recv()
        self.c = self.wire.go(self.low(step(self.at, 3)), self.up)
        self.b.wait_recv()
        self.d = self.wire.go(self.high(step(self.at, 1)), self.down)

    def finish(self):
        self.c.wait_recv()
        self.d.wait_recv()


def greet(others):
    barrier = pltpu.get_barrier_semaphore()
    for other in others:
        pl.semaphore_signal(barrier, inc=1, device_id=other, device_id_type=MESH)
    pl.semaphore_wait(barrier, len(others))


def ring_peers(z, y, c, x):
    return [
        {"x": step(x, 1)},
        {"x": step(x, 3)},
        {"y": step(y, 1)},
        {"y": step(y, 3)},
        {"z": step(z, 1)},
        {"z": step(z, 3)},
        {"c": 1 - c},
    ]


def project_kernel(
    tokens_ref,
    gain_ref,
    a_ref,
    g_ref,
    o_ref,
    mixed_ref,
    gate_ref,
    steps_ref,
    wo_ref,
    tokens,
    edges,
    normed,
    wa,
    wg,
    wo,
    send,
    recv,
    halo_send,
    halo_recv,
    local_sem,
):
    z, y, c, x = place()
    wire = Wire(send, recv)
    rows = tokens_ref.shape[0]
    half = rows // 2
    own = [
        pltpu.make_async_copy(tokens_ref, tokens.at[x], local_sem.at[0]),
        pltpu.make_async_copy(a_ref, wa.at[z, y, c], local_sem.at[1]),
        pltpu.make_async_copy(g_ref, wg.at[z, y, c], local_sem.at[2]),
        pltpu.make_async_copy(o_ref, wo.at[z, y, c, x], local_sem.at[3]),
    ]
    for copy in own:
        copy.start()
    ahead = [dict(stretch_at(z, y, c, 1), x=k) for k in range(4)]
    behind = [dict(stretch_at(z, y, c, 31), x=k) for k in range(4)]
    greet(ring_peers(z, y, c, x) + ahead + behind)
    for copy in own:
        copy.wait()

    halos = [
        [
            pltpu.make_async_remote_copy(
                src_ref=tokens.at[x, pl.ds(offset, HALO)],
                dst_ref=edges.at[slot],
                send_sem=halo_send.at[4 * slot + k],
                recv_sem=halo_recv.at[slot],
                device_id=to,
                device_id_type=MESH,
            )
            for k, to in enumerate(group)
        ]
        for slot, (group, offset) in enumerate(((ahead, rows - HALO), (behind, 0)))
    ]

    @pl.when(x == 3)
    def _():
        for copy in halos[0]:
            copy.start()

    @pl.when(x == 0)
    def _():
        for copy in halos[1]:
            copy.start()

    wo_x = Ring(
        wire,
        "x",
        x,
        lambda at: wo.at[z, y, c, at],
        lambda at: wo.at[z, y, c, at, pl.ds(0, 32)],
        lambda at: wo.at[z, y, c, at, pl.ds(32, 32)],
    )
    wo_x.start()
    low, high = pl.ds(0, half), pl.ds(half, half)
    up, down = {"x": step(x, 1)}, {"x": step(x, 3)}
    up_low = wire.go(tokens.at[x, low], up)
    down_high = wire.go(tokens.at[x, high], down)
    up_high = wire.go(tokens.at[x, high], up)
    down_low = wire.go(tokens.at[x, low], down)

    a_first = Ring(
        wire,
        "y",
        y,
        lambda at: wa.at[z, at, c],
        lambda at: wa.at[z, at, c, pl.ds(0, 32)],
        lambda at: wa.at[z, at, c, pl.ds(32, 32)],
    )
    g_first = Ring(
        wire,
        "z",
        z,
        lambda at: wg.at[at, y, c],
        lambda at: wg.at[at, y, c, pl.ds(0, 32)],
        lambda at: wg.at[at, y, c, pl.ds(32, 32)],
    )
    a_first.start()
    g_first.start()

    def normalize(ref, count, to):
        @pl.loop(0, count // 16)
        def _(k):
            start = pl.multiple_of(k * 16, 16)
            wide = ref[pl.ds(start, 16), :].astype(jnp.float32)
            scale = lax.rsqrt(jnp.mean(wide * wide, axis=-1, keepdims=True) + EPSILON)
            normed[pl.ds(pl.multiple_of(to + start, 16), 16), :] = (
                wide * scale * gain_ref[...]
            ).astype(jnp.bfloat16)

    def main_row(shard):
        return HALO + shard * rows

    normalize(tokens.at[x], rows, main_row(x))

    a_first.forward()
    g_first.forward()
    wo_x.forward()
    a_first.finish()
    a_second = Ring(
        wire,
        "z",
        z,
        lambda at: wa.at[at, :, c],
        lambda at: wa.at[at, pl.ds(0, 2), c],
        lambda at: wa.at[at, pl.ds(2, 2), c],
    )
    a_second.start()
    partner = {"c": 1 - c}
    a_pair = [wire.go(wa.at[z, :, c], partner)]
    g_first.finish()
    g_second = Ring(
        wire,
        "y",
        y,
        lambda at: wg.at[:, at, c],
        lambda at: wg.at[pl.ds(0, 2), at, c],
        lambda at: wg.at[pl.ds(2, 2), at, c],
    )
    g_second.start()
    g_pair = [wire.go(wg.at[:, y, c], partner)]
    wo_x.finish()
    lo_first = Ring(
        wire,
        "y",
        y,
        lambda at: wo.at[z, at, c, pl.ds(0, 2)],
        lambda at: wo.at[z, at, c, 0],
        lambda at: wo.at[z, at, c, 1],
    )
    hi_first = Ring(
        wire,
        "z",
        z,
        lambda at: wo.at[at, y, c, pl.ds(2, 2)],
        lambda at: wo.at[at, y, c, 2],
        lambda at: wo.at[at, y, c, 3],
    )
    lo_first.start()
    hi_first.start()

    for slot in range(2):
        halos[slot][0].wait_recv()
    normalize(edges.at[0], HALO, 0)
    normalize(edges.at[1], HALO, main_row(4))

    up_low.wait_recv()
    far_low = wire.go(tokens.at[step(x, 3), low], up)
    down_high.wait_recv()
    far_high = wire.go(tokens.at[step(x, 1), high], down)
    normalize(tokens.at[step(x, 3), low], half, main_row(step(x, 3)))
    normalize(tokens.at[step(x, 1), high], half, main_row(step(x, 1)) + half)

    a_second.forward()
    a_pair.append(wire.go(wa.at[step(z, 3), :, c], partner))
    a_pair.append(wire.go(wa.at[step(z, 1), :, c], partner))
    g_second.forward()
    g_pair.append(wire.go(wg.at[:, step(y, 3), c], partner))
    g_pair.append(wire.go(wg.at[:, step(y, 1), c], partner))
    lo_first.forward()
    hi_first.forward()
    lo_first.finish()
    lo_second = Ring(
        wire,
        "z",
        z,
        lambda at: wo.at[at, :, c, pl.ds(0, 2)],
        lambda at: wo.at[at, pl.ds(0, 2), c, pl.ds(0, 2)],
        lambda at: wo.at[at, pl.ds(2, 2), c, pl.ds(0, 2)],
    )
    lo_second.start()
    hi_first.finish()
    hi_second = Ring(
        wire,
        "y",
        y,
        lambda at: wo.at[:, at, c, pl.ds(2, 2)],
        lambda at: wo.at[pl.ds(0, 2), at, c, pl.ds(2, 2)],
        lambda at: wo.at[pl.ds(2, 2), at, c, pl.ds(2, 2)],
    )
    hi_second.start()
    wo_pair = [
        wire.go(wo.at[z, :, c, pl.ds(0, 2)], partner),
        wire.go(wo.at[:, y, c, pl.ds(2, 2)], partner),
    ]

    up_high.wait_recv()
    down_low.wait_recv()
    normalize(tokens.at[step(x, 3), high], half, main_row(step(x, 3)) + half)
    normalize(tokens.at[step(x, 1), low], half, main_row(step(x, 1)))

    a_second.finish()
    a_pair.append(wire.go(wa.at[step(z, 2), :, c], partner))
    g_second.finish()
    g_pair.append(wire.go(wg.at[:, step(y, 2), c], partner))
    for copy in a_pair + g_pair:
        copy.wait_recv()

    lead = wa.shape[4] - 128

    def project(start, count):
        taken = pl.ds(start, count)

        @pl.loop(0, lead // 256)
        def _(k):
            columns = pl.ds(pl.multiple_of(k * 256, 256), 256)
            weight = wa[:, :, :, :, columns].reshape(-1, 256)
            mixed_ref[taken, columns] = jnp.dot(
                normed[taken, :], weight, preferred_element_type=jnp.float32
            ).astype(jnp.bfloat16)

    def project_rest(shard):
        taken = pl.ds(main_row(shard), rows)
        kept = pl.ds(pl.multiple_of(shard * rows, rows), rows)

        @pl.loop(0, wg.shape[4] // 256)
        def _(k):
            columns = pl.ds(pl.multiple_of(k * 256, 256), 256)
            weight = wg[:, :, :, :, columns].reshape(-1, 256)
            gate_ref[kept, columns] = jnp.dot(
                normed[taken, :], weight, preferred_element_type=jnp.float32
            ).astype(jnp.bfloat16)

        weight = wa[:, :, :, :, lead:].reshape(-1, 128)
        steps_ref[kept, :] = jnp.dot(
            normed[taken, :], weight, preferred_element_type=jnp.float32
        ).astype(jnp.bfloat16)

    def whole(shard):
        project(pl.multiple_of(main_row(shard), 16), rows)
        project_rest(shard)

    @pl.loop(0, 3)
    def _(k):
        whole(lax.rem(x + 3 + k, 4))

    project(0, HALO)
    project(main_row(4), HALO)

    lo_second.forward()
    hi_second.forward()
    for by in (3, 1):
        wo_pair.append(wire.go(wo.at[step(z, by), :, c, pl.ds(0, 2)], partner))
        wo_pair.append(wire.go(wo.at[:, step(y, by), c, pl.ds(2, 2)], partner))

    far_low.wait_recv()
    far_high.wait_recv()
    normalize(tokens.at[step(x, 2)], rows, main_row(step(x, 2)))
    whole(step(x, 2))

    lo_second.finish()
    hi_second.finish()
    wo_pair.append(wire.go(wo.at[step(z, 2), :, c, pl.ds(0, 2)], partner))
    wo_pair.append(wire.go(wo.at[:, step(y, 2), c, pl.ds(2, 2)], partner))
    for copy in wo_pair:
        copy.wait_recv()
    out = pltpu.make_async_copy(wo, wo_ref, local_sem.at[0])
    out.start()
    wire.drain()

    @pl.when(x == 3)
    def _():
        for copy in halos[0]:
            copy.wait_send()

    @pl.when(x == 0)
    def _():
        for copy in halos[1]:
            copy.wait_send()

    out.wait()


COPIES = 80


def gather_and_project(tokens, gain, a, g, o):
    rows, width = tokens.shape
    return pl.pallas_call(
        project_kernel,
        out_shape=(
            jax.ShapeDtypeStruct((4 * rows + 2 * HALO, a.shape[1] - 128), jnp.bfloat16),
            jax.ShapeDtypeStruct((4 * rows, g.shape[1]), jnp.bfloat16),
            jax.ShapeDtypeStruct((4 * rows, 128), jnp.bfloat16),
            jax.ShapeDtypeStruct((4, 4, 2, 4, *o.shape), jnp.bfloat16),
        ),
        in_specs=[
            pl.BlockSpec(memory_space=pl.ANY),
            pl.BlockSpec(memory_space=pltpu.VMEM),
            pl.BlockSpec(memory_space=pl.ANY),
            pl.BlockSpec(memory_space=pl.ANY),
            pl.BlockSpec(memory_space=pl.ANY),
        ],
        out_specs=(
            pl.BlockSpec(memory_space=pltpu.VMEM),
            pl.BlockSpec(memory_space=pltpu.VMEM),
            pl.BlockSpec(memory_space=pltpu.VMEM),
            pl.BlockSpec(memory_space=pl.ANY),
        ),
        scratch_shapes=[
            pltpu.VMEM((4, rows, width), jnp.bfloat16),
            pltpu.VMEM((2, HALO, width), jnp.bfloat16),
            pltpu.VMEM((4 * rows + 2 * HALO, width), jnp.bfloat16),
            pltpu.VMEM((4, 4, 2, *a.shape), jnp.bfloat16),
            pltpu.VMEM((4, 4, 2, *g.shape), jnp.bfloat16),
            pltpu.VMEM((4, 4, 2, 4, *o.shape), jnp.bfloat16),
            pltpu.SemaphoreType.DMA((COPIES,)),
            pltpu.SemaphoreType.DMA((COPIES,)),
            pltpu.SemaphoreType.DMA((8,)),
            pltpu.SemaphoreType.DMA((2,)),
            pltpu.SemaphoreType.DMA((4,)),
        ],
        compiler_params=pltpu.CompilerParams(
            collective_id=0, has_side_effects=True, vmem_limit_bytes=60 * 2**20
        ),
        name="gather_project",
    )(tokens, gain.reshape(1, -1), a, g, o)


def prefix(shard, axis, combine, identity, reverse):
    length, place = lax.axis_size(axis), lax.axis_index(axis)
    everything = jax.tree.map(lambda part: lax.all_gather(part, axis), shard)
    start = jax.tree.map(
        lambda part, zero: jnp.broadcast_to(jnp.asarray(zero, part.dtype), part.shape),
        shard,
        identity,
    )

    def hop(k, before):
        at = length - 1 - k if reverse else k
        reached = at > place if reverse else at < place
        new = combine(before, jax.tree.map(lambda part: part[at], everything))
        return jax.tree.map(lambda a, b: jnp.where(reached, a, b), new, before)

    return lax.fori_loop(0, length, hop, start)


def nothing_yet(shard, identity):
    return jax.tree.map(
        lambda a, e: jnp.broadcast_to(jnp.asarray(e, a.dtype), a.shape), shard, identity
    )


def carried_in(shard, axes, combine, identity, reverse):
    before = start = nothing_yet(shard, identity)
    subtotal = shard
    for axis in reversed(axes):
        length, place = lax.axis_size(axis), lax.axis_index(axis)
        pieces = jax.tree.map(lambda part: lax.all_gather(part, axis), subtotal)
        inside, subtotal = start, start
        for k in reversed(range(length)) if reverse else range(length):
            passed = k > place if reverse else k < place
            subtotal = combine(subtotal, jax.tree.map(lambda part: part[k], pieces))
            inside = jax.tree.map(lambda new, old: jnp.where(passed, new, old), subtotal, inside)
        before = combine(inside, before)
    return before


def rms_rows(values):
    wide = values.astype(jnp.float32)
    return wide * lax.rsqrt(jnp.mean(wide * wide, axis=-1, keepdims=True) + EPSILON)


def short_filter(padded, taps):
    wide = padded.astype(jnp.float32)
    mixed = taps[0] * wide[:-2] + taps[1] * wide[1:-1] + taps[2] * wide[2:]
    return jax.nn.silu(mixed).astype(jnp.bfloat16)


def one_way(signal, step_size, rate, inward, outward, intersect):
    sequence_extent, groups, ratio, width = signal.shape
    states = inward.shape[2]
    count = sequence_extent // BLOCK
    blocks = signal.reshape(count, BLOCK, groups, ratio, width).astype(jnp.float32)
    step_blocks = step_size.reshape(count, BLOCK, groups, ratio)
    within = jnp.cumsum(-step_blocks * rate, axis=1)
    final = within[:, -1]
    scaling_factor = jnp.exp(final[:, None] - within) * step_blocks
    inward_blocks = inward.reshape(count, BLOCK, groups, states).astype(jnp.float32)
    outward_blocks = outward.reshape(count, BLOCK, groups, states).astype(jnp.float32)
    block_states = jnp.einsum(
        "cqgn,cqgrp->cgrpn",
        inward_blocks,
        blocks * scaling_factor[..., None],
        precision=lax.Precision.HIGHEST,
    )

    def advance(state, inputs):
        return (state * inputs[1][..., None, None] + inputs[0], state)

    start_state = jnp.zeros((groups, ratio, width, states), jnp.float32)
    last_state, before = lax.scan(advance, start_state, (block_states, jnp.exp(final)))
    lower = (jnp.arange(BLOCK)[:, None] >= jnp.arange(BLOCK)[None, :])[None, :, :, None, None]
    gaps = within[:, :, None] - within[:, None]
    decay = jnp.where(lower, jnp.exp(jnp.where(lower, gaps, 0.0)), 0.0)
    weights_mix = intersect[..., None] * decay * step_blocks[:, None]
    diagonal = jnp.einsum("cqkgr,ckgrp->cqgrp", weights_mix, blocks, precision=lax.Precision.HIGHEST)
    carried = (
        jnp.einsum("cqgn,cgrpn->cqgrp", outward_blocks, before, precision=lax.Precision.HIGHEST)
        * jnp.exp(within)[..., None]
    )
    running = jnp.cumsum(final, axis=0)
    from_start = (within + (running - final)[:, None]).reshape(sequence_extent, groups, ratio)
    outputs = (diagonal + carried).reshape(sequence_extent, groups, ratio, width)
    return (
        outputs,
        from_start,
        jnp.exp(running[-1]),
        last_state,
        outward_blocks.reshape(sequence_extent, groups, states),
    )


def read_in(outward_wide, incoming, from_start):
    return (
        jnp.einsum("lgn,grpn->lgrp", outward_wide, incoming, precision=lax.Precision.HIGHEST)
        * jnp.exp(from_start)[..., None]
    )


def link(earlier, later):
    return (earlier[0] * later[0], earlier[1] * later[0][..., None, None] + later[1])


def combine_ways(ahead, behind, ahead_state, behind_state):
    forward = ahead[0] + read_in(ahead[4], ahead_state, ahead[1])
    backward = behind[0] + read_in(behind[4], behind_state, behind[1])
    return forward + backward[::-1]


def local(
    input_activations,
    norm_gain,
    w_gate,
    w_value,
    w_state_in,
    w_state_out,
    w_step_forward,
    w_step_backward,
    step_offset,
    fading_speed,
    conv_value,
    conv_state_in,
    conv_state_out,
    out_gain,
    w_out,
):
    heads_local = w_step_forward.shape[1]
    a = jnp.concatenate(
        [
            w_value,
            w_state_in,
            w_state_out,
            w_step_forward,
            w_step_backward,
            jnp.zeros((w_value.shape[0], 128 - 2 * heads_local), jnp.bfloat16),
        ],
        axis=1,
    )
    mixed_in, gate, raw, wo = gather_and_project(input_activations, norm_gain, a, w_gate, w_out.T)
    sequence_extent = gate.shape[0]
    stretch = lax.axis_index(SP)
    row = lax.broadcasted_iota(jnp.int32, (sequence_extent + 2, 1), 0)
    outside = ((row == 0) & (stretch == 0)) | (
        (row == sequence_extent + 1) & (stretch == lax.axis_size(SP) - 1)
    )
    padded = jnp.where(outside, 0, mixed_in[HALO - 1 : 1 - HALO])
    raw_forward, raw_backward = raw[:, :heads_local], raw[:, heads_local : 2 * heads_local]
    taps = jnp.concatenate([conv_value, conv_state_in, conv_state_out], axis=1)
    filtered = short_filter(padded, taps)
    content_breadth = w_value.shape[1]
    state_width = w_state_in.shape[1]
    groups_local = state_width // STATE
    ratio = heads_local // groups_local
    signal = filtered[:, :content_breadth].reshape(sequence_extent, groups_local, ratio, HEAD_DIM)
    inward = filtered[:, content_breadth : content_breadth + state_width].reshape(
        sequence_extent, groups_local, STATE
    )
    outward = filtered[:, content_breadth + state_width :].reshape(
        sequence_extent, groups_local, STATE
    )
    shift = math.log(sequence_extent * lax.axis_size(SP))
    forward_step = jax.nn.softplus(
        raw_forward.astype(jnp.float32) + step_offset[0] - shift
    ).reshape(sequence_extent, groups_local, ratio)
    backward_step = jax.nn.softplus(
        raw_backward.astype(jnp.float32) + step_offset[1] - shift
    ).reshape(sequence_extent, groups_local, ratio)
    rates = fading_speed.reshape(2, groups_local, ratio)
    count = sequence_extent // BLOCK
    intersect = jnp.einsum(
        "cqgn,ckgn->cqkg",
        outward.reshape(count, BLOCK, groups_local, STATE),
        inward.reshape(count, BLOCK, groups_local, STATE),
        preferred_element_type=jnp.float32,
    )
    flipped = intersect[::-1, ::-1, ::-1]
    ahead = one_way(signal, forward_step, rates[0], inward, outward, intersect)
    behind = one_way(
        signal[::-1], backward_step[::-1], rates[1], inward[::-1], outward[::-1], flipped
    )
    ahead_in = carried_in(
        (ahead[2], ahead[3]),
        SP,
        link,
        (jnp.ones_like(ahead[2]), jnp.zeros_like(ahead[3])),
        False,
    )
    behind_in = carried_in(
        (behind[2], behind[3]),
        SP,
        link,
        (jnp.ones_like(behind[2]), jnp.zeros_like(behind[3])),
        True,
    )
    combined = combine_ways(ahead, behind, ahead_in[1], behind_in[1])
    gated = combined.reshape(sequence_extent, content_breadth) * jax.nn.silu(
        gate.astype(jnp.float32)
    )
    grouped = rms_rows(
        gated.reshape(sequence_extent, groups_local, content_breadth // groups_local)
    ).reshape(sequence_extent, content_breadth)
    mixed = (grouped * out_gain).astype(jnp.bfloat16)
    everything = lax.all_to_all(
        mixed.reshape(4, sequence_extent // 4, content_breadth), "x", split_axis=0, concat_axis=0
    )
    whole = wo.reshape(-1, 4, HEAD_DIM, content_breadth)
    result = jnp.einsum("xtk,sxnk->tsn", everything, whole, preferred_element_type=jnp.float32)
    return result.reshape(sequence_extent // 4, -1).astype(jnp.bfloat16)


def solution(mesh):
    torus = Mesh(mesh.devices.reshape(4, 4, 2, 4), SP_TP)
    return jax.shard_map(
        local,
        mesh=torus,
        in_specs=(
            P(SP_TP, None),
            P(),
            P(SP, "x"),
            P(SP, "x"),
            P(SP, "x"),
            P(SP, "x"),
            P(SP, "x"),
            P(SP, "x"),
            P(None, "x"),
            P(None, "x"),
            P(None, "x"),
            P(None, "x"),
            P(None, "x"),
            P("x"),
            P("x", SP),
        ),
        out_specs=P(SP_TP, None),
        check_vma=False,
    )
```

```python
import functools
import math

import jax
import jax.numpy as jnp
from jax import lax
from jax.experimental import pallas as pl
from jax.experimental.pallas import tpu as pltpu
from jax.sharding import Mesh
from jax.sharding import PartitionSpec as P

HEAD_DIM = 64
STATE = 128
BLOCK = 128
SP = ("z", "y", "c")
SP_TP = ("z", "y", "c", "x")
EPSILON = 1e-06
MESH = pl.DeviceIdType.MESH
HALO = 16


def place():
    return [lax.axis_index(name) for name in ("z", "y", "c", "x")]


def step(at, by):
    return lax.rem(at + by + 4, 4)


def stretch_at(z, y, c, by):
    n = lax.rem(z * 8 + y * 2 + c + by + 32, 32)
    return {"z": n // 8, "y": lax.rem(n // 2, 4), "c": lax.rem(n, 2)}


class Wire:
    def __init__(self, send, recv):
        self.send, self.recv, self.count, self.sent = send, recv, 0, []

    def describe(self, ref, to):
        k = self.count
        self.count += 1
        return pltpu.make_async_remote_copy(
            src_ref=ref,
            dst_ref=ref,
            send_sem=self.send.at[k],
            recv_sem=self.recv.at[k],
            device_id=to,
            device_id_type=MESH,
        )

    def go(self, ref, to):
        copy = self.describe(ref, to)
        copy.start()
        self.sent.append(copy)
        return copy

    def drain(self):
        for copy in self.sent:
            copy.wait_send()


class Ring:
    def __init__(self, wire, axis, at, block, low, high):
        self.wire, self.at = wire, at
        self.up, self.down = {axis: step(at, 1)}, {axis: step(at, 3)}
        self.block, self.low, self.high = block, low, high

    def start(self):
        self.a = self.wire.go(self.block(self.at), self.up)
        self.b = self.wire.go(self.block(self.at), self.down)

    def forward(self):
        self.a.wait_recv()
        self.c = self.wire.go(self.low(step(self.at, 3)), self.up)
        self.b.wait_recv()
        self.d = self.wire.go(self.high(step(self.at, 1)), self.down)

    def finish(self):
        self.c.wait_recv()
        self.d.wait_recv()


def greet(others):
    barrier = pltpu.get_barrier_semaphore()
    for other in others:
        pl.semaphore_signal(barrier, inc=1, device_id=other, device_id_type=MESH)
    pl.semaphore_wait(barrier, len(others))


def ring_peers(z, y, c, x):
    return [
        {"x": step(x, 1)},
        {"x": step(x, 3)},
        {"y": step(y, 1)},
        {"y": step(y, 3)},
        {"z": step(z, 1)},
        {"z": step(z, 3)},
        {"c": 1 - c},
    ]


def project_kernel(
    tokens_ref,
    gain_ref,
    a_ref,
    g_ref,
    o_ref,
    mixed_ref,
    gate_ref,
    steps_ref,
    wo_ref,
    tokens,
    edges,
    normed,
    wa,
    wg,
    wo,
    send,
    recv,
    halo_send,
    halo_recv,
    local_sem,
):
    z, y, c, x = place()
    wire = Wire(send, recv)
    rows = tokens_ref.shape[0]
    half = rows // 2
    own = [
        pltpu.make_async_copy(tokens_ref, tokens.at[x], local_sem.at[0]),
        pltpu.make_async_copy(a_ref, wa.at[z, y, c], local_sem.at[1]),
        pltpu.make_async_copy(g_ref, wg.at[z, y, c], local_sem.at[2]),
        pltpu.make_async_copy(o_ref, wo.at[z, y, c, x], local_sem.at[3]),
    ]
    for copy in own:
        copy.start()
    ahead = [dict(stretch_at(z, y, c, 1), x=k) for k in range(4)]
    behind = [dict(stretch_at(z, y, c, 31), x=k) for k in range(4)]
    greet(ring_peers(z, y, c, x) + ahead + behind)
    for copy in own:
        copy.wait()

    halos = [
        [
            pltpu.make_async_remote_copy(
                src_ref=tokens.at[x, pl.ds(offset, HALO)],
                dst_ref=edges.at[slot],
                send_sem=halo_send.at[4 * slot + k],
                recv_sem=halo_recv.at[slot],
                device_id=to,
                device_id_type=MESH,
            )
            for k, to in enumerate(group)
        ]
        for slot, (group, offset) in enumerate(((ahead, rows - HALO), (behind, 0)))
    ]

    @pl.when(x == 3)
    def _():
        for copy in halos[0]:
            copy.start()

    @pl.when(x == 0)
    def _():
        for copy in halos[1]:
            copy.start()

    wo_x = Ring(
        wire,
        "x",
        x,
        lambda at: wo.at[z, y, c, at],
        lambda at: wo.at[z, y, c, at, pl.ds(0, 32)],
        lambda at: wo.at[z, y, c, at, pl.ds(32, 32)],
    )
    wo_x.start()
    low, high = pl.ds(0, half), pl.ds(half, half)
    up, down = {"x": step(x, 1)}, {"x": step(x, 3)}
    up_low = wire.go(tokens.at[x, low], up)
    down_high = wire.go(tokens.at[x, high], down)
    up_high = wire.go(tokens.at[x, high], up)
    down_low = wire.go(tokens.at[x, low], down)

    a_first = Ring(
        wire,
        "y",
        y,
        lambda at: wa.at[z, at, c],
        lambda at: wa.at[z, at, c, pl.ds(0, 32)],
        lambda at: wa.at[z, at, c, pl.ds(32, 32)],
    )
    g_first = Ring(
        wire,
        "z",
        z,
        lambda at: wg.at[at, y, c],
        lambda at: wg.at[at, y, c, pl.ds(0, 32)],
        lambda at: wg.at[at, y, c, pl.ds(32, 32)],
    )
    a_first.start()
    g_first.start()

    def normalize(ref, count, to):
        @pl.loop(0, count // 16)
        def _(k):
            start = pl.multiple_of(k * 16, 16)
            wide = ref[pl.ds(start, 16), :].astype(jnp.float32)
            scale = lax.rsqrt(jnp.mean(wide * wide, axis=-1, keepdims=True) + EPSILON)
            normed[pl.ds(pl.multiple_of(to + start, 16), 16), :] = (
                wide * scale * gain_ref[...]
            ).astype(jnp.bfloat16)

    def main_row(shard):
        return HALO + shard * rows

    normalize(tokens.at[x], rows, main_row(x))

    a_first.forward()
    g_first.forward()
    wo_x.forward()
    a_first.finish()
    a_second = Ring(
        wire,
        "z",
        z,
        lambda at: wa.at[at, :, c],
        lambda at: wa.at[at, pl.ds(0, 2), c],
        lambda at: wa.at[at, pl.ds(2, 2), c],
    )
    a_second.start()
    partner = {"c": 1 - c}
    a_pair = [wire.go(wa.at[z, :, c], partner)]
    g_first.finish()
    g_second = Ring(
        wire,
        "y",
        y,
        lambda at: wg.at[:, at, c],
        lambda at: wg.at[pl.ds(0, 2), at, c],
        lambda at: wg.at[pl.ds(2, 2), at, c],
    )
    g_second.start()
    g_pair = [wire.go(wg.at[:, y, c], partner)]
    wo_x.finish()
    lo_first = Ring(
        wire,
        "y",
        y,
        lambda at: wo.at[z, at, c, pl.ds(0, 2)],
        lambda at: wo.at[z, at, c, 0],
        lambda at: wo.at[z, at, c, 1],
    )
    hi_first = Ring(
        wire,
        "z",
        z,
        lambda at: wo.at[at, y, c, pl.ds(2, 2)],
        lambda at: wo.at[at, y, c, 2],
        lambda at: wo.at[at, y, c, 3],
    )
    lo_first.start()
    hi_first.start()

    for slot in range(2):
        halos[slot][0].wait_recv()
    normalize(edges.at[0], HALO, 0)
    normalize(edges.at[1], HALO, main_row(4))

    up_low.wait_recv()
    far_low = wire.go(tokens.at[step(x, 3), low], up)
    down_high.wait_recv()
    far_high = wire.go(tokens.at[step(x, 1), high], down)
    normalize(tokens.at[step(x, 3), low], half, main_row(step(x, 3)))
    normalize(tokens.at[step(x, 1), high], half, main_row(step(x, 1)) + half)

    a_second.forward()
    a_pair.append(wire.go(wa.at[step(z, 3), :, c], partner))
    a_pair.append(wire.go(wa.at[step(z, 1), :, c], partner))
    g_second.forward()
    g_pair.append(wire.go(wg.at[:, step(y, 3), c], partner))
    g_pair.append(wire.go(wg.at[:, step(y, 1), c], partner))
    lo_first.forward()
    hi_first.forward()
    lo_first.finish()
    lo_second = Ring(
        wire,
        "z",
        z,
        lambda at: wo.at[at, :, c, pl.ds(0, 2)],
        lambda at: wo.at[at, pl.ds(0, 2), c, pl.ds(0, 2)],
        lambda at: wo.at[at, pl.ds(2, 2), c, pl.ds(0, 2)],
    )
    lo_second.start()
    hi_first.finish()
    hi_second = Ring(
        wire,
        "y",
        y,
        lambda at: wo.at[:, at, c, pl.ds(2, 2)],
        lambda at: wo.at[pl.ds(0, 2), at, c, pl.ds(2, 2)],
        lambda at: wo.at[pl.ds(2, 2), at, c, pl.ds(2, 2)],
    )
    hi_second.start()
    wo_pair = [
        wire.go(wo.at[z, :, c, pl.ds(0, 2)], partner),
        wire.go(wo.at[:, y, c, pl.ds(2, 2)], partner),
    ]

    up_high.wait_recv()
    down_low.wait_recv()
    normalize(tokens.at[step(x, 3), high], half, main_row(step(x, 3)) + half)
    normalize(tokens.at[step(x, 1), low], half, main_row(step(x, 1)))

    a_second.finish()
    a_pair.append(wire.go(wa.at[step(z, 2), :, c], partner))
    g_second.finish()
    g_pair.append(wire.go(wg.at[:, step(y, 2), c], partner))
    for copy in a_pair + g_pair:
        copy.wait_recv()

    lead = wa.shape[4] - 128

    def project(start, count):
        taken = pl.ds(start, count)

        @pl.loop(0, lead // 256)
        def _(k):
            columns = pl.ds(pl.multiple_of(k * 256, 256), 256)
            weight = wa[:, :, :, :, columns].reshape(-1, 256)
            mixed_ref[taken, columns] = jnp.dot(
                normed[taken, :], weight, preferred_element_type=jnp.float32
            ).astype(jnp.bfloat16)

    def project_rest(shard):
        taken = pl.ds(main_row(shard), rows)
        kept = pl.ds(pl.multiple_of(shard * rows, rows), rows)

        @pl.loop(0, wg.shape[4] // 256)
        def _(k):
            columns = pl.ds(pl.multiple_of(k * 256, 256), 256)
            weight = wg[:, :, :, :, columns].reshape(-1, 256)
            gate_ref[kept, columns] = jnp.dot(
                normed[taken, :], weight, preferred_element_type=jnp.float32
            ).astype(jnp.bfloat16)

        weight = wa[:, :, :, :, lead:].reshape(-1, 128)
        steps_ref[kept, :] = jnp.dot(
            normed[taken, :], weight, preferred_element_type=jnp.float32
        ).astype(jnp.bfloat16)

    def whole(shard):
        project(pl.multiple_of(main_row(shard), 16), rows)
        project_rest(shard)

    @pl.loop(0, 3)
    def _(k):
        whole(lax.rem(x + 3 + k, 4))

    @pl.when(z * 8 + y * 2 + c > 0)
    def _():
        project(0, HALO)

    @pl.when(z * 8 + y * 2 + c == 0)
    def _():
        mixed_ref[0:HALO, :] = jnp.zeros((HALO, lead), jnp.bfloat16)

    @pl.when(z * 8 + y * 2 + c < 31)
    def _():
        project(main_row(4), HALO)

    @pl.when(z * 8 + y * 2 + c == 31)
    def _():
        mixed_ref[main_row(4) :, :] = jnp.zeros((HALO, lead), jnp.bfloat16)

    lo_second.forward()
    hi_second.forward()
    for by in (3, 1):
        wo_pair.append(wire.go(wo.at[step(z, by), :, c, pl.ds(0, 2)], partner))
        wo_pair.append(wire.go(wo.at[:, step(y, by), c, pl.ds(2, 2)], partner))

    far_low.wait_recv()
    far_high.wait_recv()
    normalize(tokens.at[step(x, 2)], rows, main_row(step(x, 2)))
    whole(step(x, 2))

    lo_second.finish()
    hi_second.finish()
    wo_pair.append(wire.go(wo.at[step(z, 2), :, c, pl.ds(0, 2)], partner))
    wo_pair.append(wire.go(wo.at[:, step(y, 2), c, pl.ds(2, 2)], partner))
    for copy in wo_pair:
        copy.wait_recv()
    out = pltpu.make_async_copy(wo, wo_ref, local_sem.at[0])
    out.start()
    wire.drain()

    @pl.when(x == 3)
    def _():
        for copy in halos[0]:
            copy.wait_send()

    @pl.when(x == 0)
    def _():
        for copy in halos[1]:
            copy.wait_send()

    out.wait()


COPIES = 80


def gather_and_project(tokens, gain, a, g, o):
    rows, width = tokens.shape
    return pl.pallas_call(
        project_kernel,
        out_shape=(
            jax.ShapeDtypeStruct((4 * rows + 2 * HALO, a.shape[1] - 128), jnp.bfloat16),
            jax.ShapeDtypeStruct((4 * rows, g.shape[1]), jnp.bfloat16),
            jax.ShapeDtypeStruct((4 * rows, 128), jnp.bfloat16),
            jax.ShapeDtypeStruct((4, 4, 2, 4, *o.shape), jnp.bfloat16),
        ),
        in_specs=[
            pl.BlockSpec(memory_space=pl.ANY),
            pl.BlockSpec(memory_space=pltpu.VMEM),
            pl.BlockSpec(memory_space=pl.ANY),
            pl.BlockSpec(memory_space=pl.ANY),
            pl.BlockSpec(memory_space=pl.ANY),
        ],
        out_specs=(
            pl.BlockSpec(memory_space=pltpu.VMEM),
            pl.BlockSpec(memory_space=pltpu.VMEM),
            pl.BlockSpec(memory_space=pltpu.VMEM),
            pl.BlockSpec(memory_space=pl.ANY),
        ),
        scratch_shapes=[
            pltpu.VMEM((4, rows, width), jnp.bfloat16),
            pltpu.VMEM((2, HALO, width), jnp.bfloat16),
            pltpu.VMEM((4 * rows + 2 * HALO, width), jnp.bfloat16),
            pltpu.VMEM((4, 4, 2, *a.shape), jnp.bfloat16),
            pltpu.VMEM((4, 4, 2, *g.shape), jnp.bfloat16),
            pltpu.VMEM((4, 4, 2, 4, *o.shape), jnp.bfloat16),
            pltpu.SemaphoreType.DMA((COPIES,)),
            pltpu.SemaphoreType.DMA((COPIES,)),
            pltpu.SemaphoreType.DMA((8,)),
            pltpu.SemaphoreType.DMA((2,)),
            pltpu.SemaphoreType.DMA((4,)),
        ],
        compiler_params=pltpu.CompilerParams(
            collective_id=0, has_side_effects=True, vmem_limit_bytes=60 * 2**20
        ),
        name="gather_project",
    )(tokens, gain.reshape(1, -1), a, g, o)


LOG2E = 1.4426950408889634


def dot_nt(a, b):
    return lax.dot_general(a, b, (((1,), (1,)), ((), ())), preferred_element_type=jnp.float32)


def dot_tn(a, b):
    return lax.dot_general(a, b, (((0,), (0,)), ((), ())), preferred_element_type=jnp.float32)


def dot(a, b, precision=None):
    return lax.dot_general(
        a, b, (((1,), (0,)), ((), ())), precision=precision, preferred_element_type=jnp.float32
    )


def iota(shape, dim):
    return lax.broadcasted_iota(jnp.int32, shape, dim)


def silu(v):
    return v / (1.0 + jnp.exp(-v))


def mixer_kernel(
    shift,
    mixed_ref,
    gate_ref,
    raw_ref,
    taps_ref,
    heads_ref,
    gain_ref,
    wo_hbm,
    out_ref,
    signal,
    inward,
    outward,
    column,
    rowwise,
    reading,
    states,
    decays,
    before,
    inner,
    totals,
    arrived,
    onward,
    incoming,
    mixed,
    shards,
    wo,
    send,
    recv,
    local_sem,
):
    z, y, c, x = place()
    me = z * 8 + y * 2 + c
    blocks = gate_ref.shape[0] // BLOCK
    half = signal.shape[1]
    wide = 2 * half
    groups = inward.shape[1] // STATE
    ratio = half // HEAD_DIM // groups
    heads = groups * ratio
    span = ratio * HEAD_DIM

    def stretch(n):
        return {"z": n // 8, "y": lax.rem(n // 2, 4), "c": lax.rem(n, 2)}

    barrier = pltpu.get_barrier_semaphore()

    @pl.loop(1, 32)
    def _(k):
        pl.semaphore_signal(
            barrier, inc=1, device_id=stretch(lax.rem(me + k, 32)), device_id_type=MESH
        )

    for k in range(1, 4):
        pl.semaphore_signal(barrier, inc=1, device_id={"x": step(x, k)}, device_id_type=MESH)
    load_wo = pltpu.make_async_copy(wo_hbm, wo, local_sem)
    load_wo.start()

    row, col = iota((BLOCK, BLOCK), 0), iota((BLOCK, BLOCK), 1)
    lower = row >= col
    triangle = jnp.where(lower, 1.0, 0.0)
    spread = jnp.where(
        iota((128, wide), 1) // HEAD_DIM == iota((128, wide), 0), 1.0, 0.0
    ).astype(jnp.bfloat16)
    forward_lane = iota((BLOCK, 128), 1) < heads

    def rows_of(k):
        return pl.ds(pl.multiple_of(k * BLOCK, BLOCK), BLOCK)

    @pl.loop(0, blocks)
    def _(k):
        window = pl.ds(pl.multiple_of(k * BLOCK, BLOCK), BLOCK + 2 * HALO)
        for at in range(0, mixed_ref.shape[1], 128):
            cells = mixed_ref[window, at : at + 128].astype(jnp.float32)
            tap = taps_ref[:, at : at + 128]
            total = (
                tap[0:1] * pltpu.roll(cells, 1, 0)
                + tap[1:2] * cells
                + tap[2:3] * pltpu.roll(cells, BLOCK + 2 * HALO - 1, 0)
            )[HALO : HALO + BLOCK]
            done = silu(total).astype(jnp.bfloat16)
            if at < half:
                signal[rows_of(k), at : at + 128] = done
            elif at < half + inward.shape[1]:
                inward[rows_of(k), at - half : at - half + 128] = done
            else:
                begin = at - half - inward.shape[1]
                outward[rows_of(k), begin : begin + 128] = done

        size = jax.nn.softplus(
            raw_ref[rows_of(k), :].astype(jnp.float32) + heads_ref[0:1, :] - shift
        )
        logs = size * heads_ref[1:2, :]
        through = dot(triangle, logs, lax.Precision.HIGHEST)
        until = through - logs
        whole = through[BLOCK - 1 : BLOCK, :]
        logsize = jnp.log(size)
        column[rows_of(k), :] = jnp.where(forward_lane, through, -until) * LOG2E
        across = jnp.where(forward_lane, logsize - through, logsize + until) * LOG2E
        turned = across.T
        sizes = size.T
        rowwise[k, 0 : 2 * heads, :] = turned[0 : 2 * heads]
        rowwise[k, 2 * heads : 3 * heads, :] = sizes[0:heads] + sizes[heads : 2 * heads]
        reading[rows_of(k), :] = jnp.exp(
            jnp.where(forward_lane, through, whole - until)
        ).astype(jnp.bfloat16)
        weight = size * jnp.exp(jnp.where(forward_lane, whole - through, until))
        decays[k] = dot(
            jnp.broadcast_to(jnp.exp(whole), (8, 128)),
            spread.astype(jnp.float32),
            lax.Precision.HIGHEST,
        )
        weights = dot(weight.astype(jnp.bfloat16), spread)
        for way in range(2):
            for g in range(groups):
                lanes = slice(g * span, (g + 1) * span)
                placed = slice(way * half + g * span, way * half + (g + 1) * span)
                content = (
                    signal[rows_of(k), lanes].astype(jnp.float32) * weights[:, placed]
                ).astype(jnp.bfloat16)
                states[k, :, placed] = dot_tn(
                    inward[rows_of(k), g * STATE : (g + 1) * STATE], content
                )

    @pl.loop(0, wide // 128)
    def _(j):
        lanes = pl.ds(pl.multiple_of(j * 128, 128), 128)
        backward = j >= half // 128
        total = jnp.zeros((STATE, 128), jnp.float32)
        decay = jnp.ones((1, 128), jnp.float32)
        for k in range(blocks):
            at = jnp.where(backward, blocks - 1 - k, k)
            part = decays[at, 0:1, lanes]
            total = total * part + states[at, :, lanes]
            decay = decay * part
        high = decay.astype(jnp.bfloat16).astype(jnp.float32)
        middle = (decay - high).astype(jnp.bfloat16).astype(jnp.float32)
        low = decay - high - middle
        place_row = iota((16, 128), 0)
        tail = jnp.where(place_row == 0, high, jnp.where(place_row == 1, middle, low))
        for q in range(4):
            totals[4 * j + q, 0:32, :] = total[32 * q : 32 * q + 32].astype(jnp.bfloat16)
            totals[4 * j + q, 32:48, :] = tail.astype(jnp.bfloat16)

    pl.semaphore_wait(barrier, 34)

    def outgoing(box, inbox, bank, k):
        to = lax.rem(me + k, 32)
        return pltpu.make_async_remote_copy(
            src_ref=box.at[to],
            dst_ref=inbox.at[me],
            send_sem=send.at[bank, k],
            recv_sem=recv.at[bank, me],
            device_id=stretch(to),
            device_id_type=MESH,
        )

    def expected(box, inbox, bank, k):
        source = lax.rem(me + k, 32)
        return pltpu.make_async_remote_copy(
            src_ref=box.at[me],
            dst_ref=inbox.at[source],
            send_sem=send.at[bank, k],
            recv_sem=recv.at[bank, source],
            device_id=stretch(source),
            device_id_type=MESH,
        )

    @pl.loop(1, 32)
    def _(k):
        outgoing(totals, arrived, 0, k).start()

    arrived[me] = totals[me]

    def within(k):
        for g in range(groups):
            inner_product = dot_nt(
                outward[rows_of(k), g * STATE : (g + 1) * STATE],
                inward[rows_of(k), g * STATE : (g + 1) * STATE],
            )
            cells = signal[rows_of(k), g * span : (g + 1) * span]
            head_of = iota((BLOCK, span), 1) // HEAD_DIM
            weights, content = [], []
            for r in range(ratio):
                h = g * ratio + r
                below = column[rows_of(k), h : h + 1] + rowwise[k, h : h + 1, :]
                above = (
                    column[rows_of(k), heads + h : heads + h + 1]
                    + rowwise[k, heads + h : heads + h + 1, :]
                )
                decay = jnp.exp2(jnp.where(lower, below, above))
                both = jnp.where(
                    row == col, rowwise[k, 2 * heads + h : 2 * heads + h + 1, :], decay
                )
                weights.append((inner_product * both).astype(jnp.bfloat16))
                content.append(jnp.where(head_of == r, cells, jnp.zeros_like(cells)))
            inner[rows_of(k), g * span : (g + 1) * span] = dot(
                jnp.concatenate(weights, axis=1), jnp.concatenate(content, axis=0)
            )

    @pl.loop(0, blocks // 2)
    def _(k):
        within(k)

    @pl.loop(1, 32)
    def _(k):
        expected(totals, arrived, 0, k).wait_recv()

    flip = me >= 16

    def hop(k, state):
        at = jnp.where(flip, 31 - k, k)
        onward[at] = state.astype(jnp.bfloat16)
        message = arrived[at].astype(jnp.float32)
        decay = message[32:33] + message[33:34] + message[34:35]
        return state * decay + message[0:32]

    lax.fori_loop(0, 32, hop, jnp.zeros((32, 128), jnp.float32))

    @pl.loop(1, 32)
    def _(k):
        outgoing(onward, incoming, 1, k).start()

    incoming[me] = onward[me]

    @pl.loop(blocks // 2, blocks)
    def _(k):
        within(k)

    @pl.loop(1, 32)
    def _(k):
        expected(onward, incoming, 1, k).wait_recv()

    @pl.loop(0, wide // 128)
    def _(j):
        lanes = pl.ds(pl.multiple_of(j * 128, 128), 128)
        backward = j >= half // 128
        state = jnp.concatenate([incoming[4 * j + q] for q in range(4)], axis=0).astype(jnp.float32)
        for k in range(blocks):
            at = jnp.where(backward, blocks - 1 - k, k)
            before[at, :, lanes] = state.astype(jnp.bfloat16)
            state = state * decays[at, 0:1, lanes] + states[at, :, lanes]

    def finish(k):
        scale = dot(reading[rows_of(k), :], spread)
        for g in range(groups):
            lanes = slice(g * span, (g + 1) * span)
            read = outward[rows_of(k), g * STATE : (g + 1) * STATE]
            total = inner[rows_of(k), lanes]
            for way in range(2):
                placed = slice(way * half + g * span, way * half + (g + 1) * span)
                total = total + dot(read, before[k, :, placed]) * scale[:, placed]
            gated = total * silu(gate_ref[rows_of(k), lanes].astype(jnp.float32))
            level = lax.rsqrt(jnp.mean(gated * gated, axis=-1, keepdims=True) + EPSILON)
            mixed[rows_of(k), lanes] = (gated * level * gain_ref[:, lanes]).astype(jnp.bfloat16)

    shard_rows = shards.shape[1]

    def hand_over(k):
        return pltpu.make_async_remote_copy(
            src_ref=mixed.at[pl.ds(pl.multiple_of(step(x, k) * shard_rows, shard_rows), shard_rows)],
            dst_ref=shards.at[x],
            send_sem=send.at[2, k],
            recv_sem=recv.at[2, x],
            device_id={"x": step(x, k)},
            device_id_type=MESH,
        )

    for k in (2, 1, 3, 0):

        @pl.loop(0, 2)
        def _(b):
            finish(2 * step(x, k) + b)

        if k:
            hand_over(k).start()

    shards[x] = mixed[pl.ds(pl.multiple_of(x * shard_rows, shard_rows), shard_rows), :]
    load_wo.wait()
    for k in (1, 3, 2):
        source = step(x, k)
        pltpu.make_async_remote_copy(
            src_ref=mixed.at[pl.ds(0, shard_rows)],
            dst_ref=shards.at[source],
            send_sem=send.at[2, k],
            recv_sem=recv.at[2, source],
            device_id={"x": source},
            device_id_type=MESH,
        ).wait_recv()

    @pl.loop(0, 8)
    def _(k):
        total = None
        for at in range(4):
            part = dot_nt(shards[at], wo[pl.ds(4 * k, 4), at].reshape(256, -1))
            total = part if total is None else total + part
        out_ref[:, pl.ds(pl.multiple_of(k * 256, 256), 256)] = total.astype(jnp.bfloat16)

    @pl.loop(1, 32)
    def _(k):
        outgoing(totals, arrived, 0, k).wait_send()
        outgoing(onward, incoming, 1, k).wait_send()

    for k in (1, 2, 3):
        hand_over(k).wait_send()


def mix(mixed_in, gate, raw, taps, head_rows, out_gain, wo, shift):
    rows, half = gate.shape
    states = (mixed_in.shape[1] - half) // 2
    blocks = rows // BLOCK
    vmem = pl.BlockSpec(memory_space=pltpu.VMEM)
    bf16, f32 = jnp.bfloat16, jnp.float32
    return pl.pallas_call(
        functools.partial(mixer_kernel, shift),
        out_shape=jax.ShapeDtypeStruct((rows // 4, wo.shape[0] * wo.shape[2]), bf16),
        in_specs=[vmem] * 6 + [pl.BlockSpec(memory_space=pl.ANY)],
        out_specs=vmem,
        scratch_shapes=[
            pltpu.VMEM((rows, half), bf16),
            pltpu.VMEM((rows, states), bf16),
            pltpu.VMEM((rows, states), bf16),
            pltpu.VMEM((rows, 128), f32),
            pltpu.VMEM((blocks, 24, 128), f32),
            pltpu.VMEM((rows, 128), bf16),
            pltpu.VMEM((blocks, STATE, 2 * half), f32),
            pltpu.VMEM((blocks, 8, 2 * half), f32),
            pltpu.VMEM((blocks, STATE, 2 * half), bf16),
            pltpu.VMEM((rows, half), f32),
            pltpu.VMEM((32, 48, 128), bf16),
            pltpu.VMEM((32, 48, 128), bf16),
            pltpu.VMEM((32, 32, 128), bf16),
            pltpu.VMEM((32, 32, 128), bf16),
            pltpu.VMEM((rows, half), bf16),
            pltpu.VMEM((4, rows // 4, half), bf16),
            pltpu.VMEM(wo.shape, bf16),
            pltpu.SemaphoreType.DMA((3, 32)),
            pltpu.SemaphoreType.DMA((3, 32)),
            pltpu.SemaphoreType.DMA,
        ],
        compiler_params=pltpu.CompilerParams(
            collective_id=1, has_side_effects=True, vmem_limit_bytes=60 * 2**20
        ),
        name="mixer",
    )(mixed_in, gate, raw, taps, head_rows, out_gain, wo)


def local(
    input_activations,
    norm_gain,
    w_gate,
    w_value,
    w_state_in,
    w_state_out,
    w_step_forward,
    w_step_backward,
    step_offset,
    fading_speed,
    conv_value,
    conv_state_in,
    conv_state_out,
    out_gain,
    w_out,
):
    heads_local = w_step_forward.shape[1]
    a = jnp.concatenate(
        [
            w_value,
            w_state_in,
            w_state_out,
            w_step_forward,
            w_step_backward,
            jnp.zeros((w_value.shape[0], 128 - 2 * heads_local), jnp.bfloat16),
        ],
        axis=1,
    )
    taps = jnp.concatenate([conv_value, conv_state_in, conv_state_out], axis=1)
    head_rows = jnp.pad(
        jnp.stack([step_offset.reshape(-1), -fading_speed.reshape(-1)]),
        ((0, 0), (0, 128 - 2 * heads_local)),
    )
    mixed_in, gate, raw, wo = gather_and_project(input_activations, norm_gain, a, w_gate, w_out.T)
    shift = math.log(gate.shape[0] * lax.axis_size(SP))
    return mix(
        mixed_in,
        gate,
        raw,
        taps,
        head_rows,
        out_gain.reshape(1, -1),
        wo.reshape(-1, *wo.shape[3:]),
        shift,
    )


def solution(mesh):
    torus = Mesh(mesh.devices.reshape(4, 4, 2, 4), SP_TP)
    return jax.shard_map(
        local,
        mesh=torus,
        in_specs=(
            P(SP_TP, None),
            P(),
            P(SP, "x"),
            P(SP, "x"),
            P(SP, "x"),
            P(SP, "x"),
            P(SP, "x"),
            P(SP, "x"),
            P(None, "x"),
            P(None, "x"),
            P(None, "x"),
            P(None, "x"),
            P(None, "x"),
            P("x"),
            P("x", SP),
        ),
        out_specs=P(SP_TP, None),
        check_vma=False,
    )
```

```python
import functools
import math

import jax
import jax.numpy as jnp
from jax import lax
from jax.experimental import pallas as pl
from jax.experimental.pallas import tpu as pltpu
from jax.sharding import Mesh
from jax.sharding import PartitionSpec as P

HEAD_DIM = 64
STATE = 128
BLOCK = 128
SP = ("z", "y", "c")
SP_TP = ("z", "y", "c", "x")
EPSILON = 1e-06
MESH = pl.DeviceIdType.MESH
HALO = 16


def place():
    return [lax.axis_index(name) for name in ("z", "y", "c", "x")]


def step(at, by):
    return lax.rem(at + by + 4, 4)


def stretch_at(z, y, c, by):
    n = lax.rem(z * 8 + y * 2 + c + by + 32, 32)
    return {"z": n // 8, "y": lax.rem(n // 2, 4), "c": lax.rem(n, 2)}


class Wire:
    def __init__(self, send, recv):
        self.send, self.recv, self.count, self.sent = send, recv, 0, []

    def describe(self, source, target, to):
        k = self.count
        self.count += 1
        return pltpu.make_async_remote_copy(
            src_ref=source,
            dst_ref=target,
            send_sem=self.send.at[k],
            recv_sem=self.recv.at[k],
            device_id=to,
            device_id_type=MESH,
        )

    def go(self, source, to, target=None):
        copy = self.describe(source, source if target is None else target, to)
        copy.start()
        self.sent.append(copy)
        return copy

    def drain(self):
        for copy in self.sent:
            copy.wait_send()


class Ring:
    def __init__(self, wire, axis, at, block, low, high):
        self.wire, self.at = wire, at
        self.up, self.down = {axis: step(at, 1)}, {axis: step(at, 3)}
        self.block, self.low, self.high = block, low, high

    def start(self):
        self.a = self.wire.go(self.block(self.at), self.up)
        self.b = self.wire.go(self.block(self.at), self.down)

    def forward(self):
        self.a.wait_recv()
        self.c = self.wire.go(self.low(step(self.at, 3)), self.up)
        self.b.wait_recv()
        self.d = self.wire.go(self.high(step(self.at, 1)), self.down)

    def finish(self):
        self.c.wait_recv()
        self.d.wait_recv()


LOG2E = 1.4426950408889634


def dot_nt(a, b):
    return lax.dot_general(a, b, (((1,), (1,)), ((), ())), preferred_element_type=jnp.float32)


def dot_tn(a, b):
    return lax.dot_general(a, b, (((0,), (0,)), ((), ())), preferred_element_type=jnp.float32)


def dot(a, b, precision=None):
    return lax.dot_general(
        a, b, (((1,), (0,)), ((), ())), precision=precision, preferred_element_type=jnp.float32
    )


def iota(shape, dim):
    return lax.broadcasted_iota(jnp.int32, shape, dim)


def silu(v):
    return v / (1.0 + jnp.exp(-v))


def mixer_kernel(
    shift,
    tokens_hbm,
    norm_gain_ref,
    value_hbm,
    state_in_hbm,
    state_out_hbm,
    step_forward_ref,
    step_backward_ref,
    gate_hbm,
    w_out_hbm,
    tap_value_ref,
    tap_in_ref,
    tap_out_ref,
    heads_ref,
    gain_ref,
    out_ref,
    tokens,
    edges,
    normed,
    wv,
    ws,
    wg,
    wo,
    projected,
    gates,
    raw,
    signal,
    inward,
    outward,
    column,
    rowwise,
    reading,
    states,
    decays,
    before,
    inner,
    totals,
    arrived,
    onward,
    incoming,
    mixed,
    shards,
    relay,
    summed,
    send,
    recv,
    halo_send,
    halo_recv,
    state_send,
    state_recv,
    local_sem,
):
    z, y, c, x = place()
    me = z * 8 + y * 2 + c
    wire = Wire(send, recv)
    rows = tokens.shape[1]
    middle = rows // 2
    count = 4 * rows
    blocks = count // BLOCK
    half = signal.shape[1]
    wide = 2 * half
    groups = inward.shape[1] // STATE
    ratio = half // HEAD_DIM // groups
    heads = groups * ratio
    span = ratio * HEAD_DIM
    lead = inward.shape[1]
    partner = {"c": 1 - c}

    def stretch(n):
        return {"z": n // 8, "y": lax.rem(n // 2, 4), "c": lax.rem(n, 2)}

    own = [
        pltpu.make_async_copy(tokens_hbm, tokens.at[x], local_sem.at[0]),
        pltpu.make_async_copy(value_hbm, wv.at[z, y, c], local_sem.at[1]),
        pltpu.make_async_copy(state_in_hbm, ws.at[z, y, c, :, pl.ds(0, lead)], local_sem.at[2]),
        pltpu.make_async_copy(state_out_hbm, ws.at[z, y, c, :, pl.ds(lead, lead)], local_sem.at[3]),
        pltpu.make_async_copy(gate_hbm, wg.at[z, y, c], local_sem.at[4]),
        pltpu.make_async_copy(w_out_hbm, wo.at[z, y, c, x], local_sem.at[5]),
    ]
    for copy in own:
        copy.start()
    depth = step_forward_ref.shape[1]
    steps = jnp.concatenate(
        [
            step_forward_ref[...].astype(jnp.float32),
            step_backward_ref[...].astype(jnp.float32),
            jnp.zeros((128 - 2 * heads, depth), jnp.float32),
        ],
        axis=0,
    )
    steps = jnp.concatenate([steps, jnp.zeros((128, 128 - depth), jnp.float32)], axis=1).T
    ws[z, y, c, :, 2 * lead :] = steps[0:depth].astype(jnp.bfloat16)

    barrier = pltpu.get_barrier_semaphore()

    @pl.loop(1, 32)
    def _(k):
        pl.semaphore_signal(
            barrier, inc=1, device_id=stretch(lax.rem(me + k, 32)), device_id_type=MESH
        )

    for k in range(1, 4):
        others = [{"x": step(x, k)}]
        others += [dict(stretch_at(z, y, c, by), x=step(x, k)) for by in (1, 31)]
        for other in others:
            pl.semaphore_signal(barrier, inc=1, device_id=other, device_id_type=MESH)
    for copy in own:
        copy.wait()
    pl.semaphore_wait(barrier, 40)

    low, high = pl.ds(0, middle), pl.ds(middle, middle)
    up, down = {"x": step(x, 1)}, {"x": step(x, 3)}
    up_low = wire.go(tokens.at[x, low], up)
    down_high = wire.go(tokens.at[x, high], down)
    up_high = wire.go(tokens.at[x, high], up)
    down_low = wire.go(tokens.at[x, low], down)

    halos = [
        [
            pltpu.make_async_remote_copy(
                src_ref=tokens.at[x, pl.ds(offset, HALO)],
                dst_ref=edges.at[slot],
                send_sem=halo_send.at[4 * slot + k],
                recv_sem=halo_recv.at[slot],
                device_id=dict(stretch_at(z, y, c, by), x=k),
                device_id_type=MESH,
            )
            for k in range(4)
        ]
        for slot, (by, offset) in enumerate(((1, rows - HALO), (31, 0)))
    ]

    def first(buffer, axis, keep=()):
        def at(n, part):
            spot = (z, n, c) if axis == "y" else (n, y, c)
            if keep:
                start, size = keep
                return buffer.at[(*spot, pl.ds(start, size) if part is None else start + part)]
            return buffer.at[spot] if part is None else buffer.at[(*spot, pl.ds(32 * part, 32))]

        here = y if axis == "y" else z
        return Ring(
            wire, axis, here, lambda n: at(n, None), lambda n: at(n, 0), lambda n: at(n, 1)
        )

    def group(buffer, axis, n, part, keep):
        some = pl.ds(0, 4) if part is None else pl.ds(2 * part, 2)
        spot = (n, some, c) if axis == "z" else (some, n, c)
        return buffer.at[(*spot, pl.ds(*keep))] if keep else buffer.at[spot]

    def second(buffer, axis, keep=()):
        here = y if axis == "y" else z
        return Ring(
            wire,
            axis,
            here,
            lambda n: group(buffer, axis, n, None, keep),
            lambda n: group(buffer, axis, n, 0, keep),
            lambda n: group(buffer, axis, n, 1, keep),
        )

    pairs = {}

    def across(name, buffer, axis, by, keep=()):
        here = y if axis == "y" else z
        copy = wire.go(group(buffer, axis, step(here, by), None, keep), partner)
        pairs.setdefault(name, []).append(copy)

    v_first, s_first = first(wv, "y"), first(ws, "z")
    v_first.start()
    s_first.start()

    @pl.when(x == 3)
    def _():
        for copy in halos[0]:
            copy.start()

    @pl.when(x == 0)
    def _():
        for copy in halos[1]:
            copy.start()

    wo_x = Ring(
        wire,
        "x",
        x,
        lambda at: wo.at[z, y, c, at],
        lambda at: wo.at[z, y, c, at, pl.ds(0, 32)],
        lambda at: wo.at[z, y, c, at, pl.ds(32, 32)],
    )
    wo_x.start()

    def main_row(shard):
        return HALO + shard * rows

    def normalize(ref, size, to):
        @pl.loop(0, size // 16)
        def _(k):
            start = pl.multiple_of(k * 16, 16)
            cells = ref[pl.ds(start, 16), :].astype(jnp.float32)
            scale = lax.rsqrt(jnp.mean(cells * cells, axis=-1, keepdims=True) + EPSILON)
            normed[pl.ds(pl.multiple_of(to + start, 16), 16), :] = (
                cells * scale * norm_gain_ref[...]
            ).astype(jnp.bfloat16)

    def project(start, size):
        taken = pl.ds(start, size)

        @pl.loop(0, half // 256)
        def _(k):
            columns = pl.ds(pl.multiple_of(k * 256, 256), 256)
            projected[taken, columns] = dot(
                normed[taken, :], wv[:, :, :, :, columns].reshape(-1, 256)
            ).astype(jnp.bfloat16)

        @pl.loop(0, 2 * lead // 256)
        def _(k):
            columns = pl.ds(pl.multiple_of(k * 256, 256), 256)
            projected[taken, pl.ds(pl.multiple_of(half + k * 256, 256), 256)] = dot(
                normed[taken, :], ws[:, :, :, :, columns].reshape(-1, 256)
            ).astype(jnp.bfloat16)

    def project_shard(shard):
        project(pl.multiple_of(main_row(shard), 16), rows)
        raw[pl.ds(pl.multiple_of(shard * rows, rows), rows), :] = dot(
            normed[pl.ds(pl.multiple_of(main_row(shard), 16), rows), :],
            ws[:, :, :, :, 2 * lead :].reshape(-1, 128),
        ).astype(jnp.bfloat16)

    def project_gate(shard):
        @pl.loop(0, half // 256)
        def _(k):
            columns = pl.ds(pl.multiple_of(k * 256, 256), 256)
            gates[pl.ds(pl.multiple_of(shard * rows, rows), rows), columns] = silu(
                dot(
                    normed[pl.ds(pl.multiple_of(main_row(shard), 16), rows), :],
                    wg[:, :, :, :, columns].reshape(-1, 256),
                )
                .astype(jnp.bfloat16)
                .astype(jnp.float32)
            ).astype(jnp.bfloat16)

    normalize(tokens.at[x], rows, main_row(x))

    v_first.forward()
    s_first.forward()
    v_first.finish()
    v_second = second(wv, "z")
    v_second.start()
    across("v", wv, "z", 0)
    s_first.finish()
    s_second = second(ws, "y")
    s_second.start()
    across("s", ws, "y", 0)
    g_first = first(wg, "z")
    g_first.start()

    for slot in range(2):
        halos[slot][0].wait_recv()
    normalize(edges.at[0], HALO, 0)
    normalize(edges.at[1], HALO, main_row(4))

    up_low.wait_recv()
    far_low = wire.go(tokens.at[step(x, 3), low], up)
    down_high.wait_recv()
    far_high = wire.go(tokens.at[step(x, 1), high], down)
    normalize(tokens.at[step(x, 3), low], middle, main_row(step(x, 3)))
    normalize(tokens.at[step(x, 1), high], middle, main_row(step(x, 1)) + middle)

    v_second.forward()
    s_second.forward()
    for by in (3, 1):
        across("v", wv, "z", by)
        across("s", ws, "y", by)
    g_first.forward()
    v_second.finish()
    across("v", wv, "z", 2)
    s_second.finish()
    across("s", ws, "y", 2)
    g_first.finish()
    g_second = second(wg, "y")
    g_second.start()
    across("g", wg, "y", 0)
    for copy in pairs["v"] + pairs["s"]:
        copy.wait_recv()
    project_shard(x)

    up_high.wait_recv()
    down_low.wait_recv()
    wo_x.forward()
    normalize(tokens.at[step(x, 3), high], middle, main_row(step(x, 3)) + middle)
    normalize(tokens.at[step(x, 1), low], middle, main_row(step(x, 1)))
    wo_x.finish()
    lo_first, hi_first = first(wo, "y", (0, 2)), first(wo, "z", (2, 2))
    lo_first.start()
    hi_first.start()
    project_shard(step(x, 3))
    g_second.forward()
    across("g", wg, "y", 3)
    across("g", wg, "y", 1)
    project_shard(step(x, 1))

    @pl.when(me > 0)
    def _():
        project(0, HALO)

    @pl.when(me == 0)
    def _():
        projected[0:HALO, :] = jnp.zeros((HALO, wide), jnp.bfloat16)

    @pl.when(me < 31)
    def _():
        project(main_row(4), HALO)

    @pl.when(me == 31)
    def _():
        projected[main_row(4) :, :] = jnp.zeros((HALO, wide), jnp.bfloat16)

    lo_first.forward()
    hi_first.forward()

    row, col = iota((BLOCK, BLOCK), 0), iota((BLOCK, BLOCK), 1)
    lower = row >= col
    triangle = jnp.where(lower, 1.0, 0.0)
    spread = jnp.where(
        iota((128, wide), 1) // HEAD_DIM == iota((128, wide), 0), 1.0, 0.0
    ).astype(jnp.bfloat16)
    forward_lane = iota((BLOCK, 128), 1) < heads

    def rows_of(k):
        return pl.ds(pl.multiple_of(k * BLOCK, BLOCK), BLOCK)

    def prepare(k):
        window = pl.ds(pl.multiple_of(k * BLOCK, BLOCK), BLOCK + 2 * HALO)
        for at in range(0, wide, 128):
            if at < half:
                tap_ref, target, begin = tap_value_ref, signal, at
            elif at < half + lead:
                tap_ref, target, begin = tap_in_ref, inward, at - half
            else:
                tap_ref, target, begin = tap_out_ref, outward, at - half - lead
            cells = projected[window, at : at + 128].astype(jnp.float32)
            tap = tap_ref[:, begin : begin + 128]
            total = (
                tap[0:1] * pltpu.roll(cells, 1, 0)
                + tap[1:2] * cells
                + tap[2:3] * pltpu.roll(cells, BLOCK + 2 * HALO - 1, 0)
            )[HALO : HALO + BLOCK]
            target[rows_of(k), begin : begin + 128] = silu(total).astype(jnp.bfloat16)

        size = jax.nn.softplus(
            raw[rows_of(k), :].astype(jnp.float32) + heads_ref[0:1, :] - shift
        )
        logs = size * heads_ref[1:2, :]
        through = dot(triangle, logs, lax.Precision.HIGHEST)
        until = through - logs
        whole = through[BLOCK - 1 : BLOCK, :]
        logsize = jnp.log(size)
        column[rows_of(k), :] = jnp.where(forward_lane, through, -until) * LOG2E
        turned = (jnp.where(forward_lane, logsize - through, logsize + until) * LOG2E).T
        sizes = size.T
        rowwise[k, 0 : 2 * heads, :] = turned[0 : 2 * heads]
        rowwise[k, 2 * heads : 3 * heads, :] = sizes[0:heads] + sizes[heads : 2 * heads]
        reading[rows_of(k), :] = jnp.exp(
            jnp.where(forward_lane, through, whole - until)
        ).astype(jnp.bfloat16)
        weight = size * jnp.exp(jnp.where(forward_lane, whole - through, until))
        decays[k] = dot(
            jnp.broadcast_to(jnp.exp(whole), (8, 128)),
            spread.astype(jnp.float32),
            lax.Precision.HIGHEST,
        )
        weights = dot(weight.astype(jnp.bfloat16), spread)
        for way in range(2):
            for g in range(groups):
                lanes = slice(g * span, (g + 1) * span)
                placed = slice(way * half + g * span, way * half + (g + 1) * span)
                content = (
                    signal[rows_of(k), lanes].astype(jnp.float32) * weights[:, placed]
                ).astype(jnp.bfloat16)
                states[k, :, placed] = dot_tn(
                    inward[rows_of(k), g * STATE : (g + 1) * STATE], content
                )

    far = 2 * step(x, 2)

    @pl.loop(0, 4)
    def _(k):
        prepare(lax.rem(far + 3 + k, blocks))

    lo_first.finish()
    lo_second = second(wo, "z", (0, 2))
    lo_second.start()
    across("o", wo, "z", 0, (0, 2))
    hi_first.finish()
    hi_second = second(wo, "y", (2, 2))
    hi_second.start()
    across("o", wo, "y", 0, (2, 2))

    g_second.finish()
    across("g", wg, "y", 2)
    for copy in pairs["g"]:
        copy.wait_recv()
    project_gate(x)
    project_gate(step(x, 3))
    project_gate(step(x, 1))

    far_low.wait_recv()
    far_high.wait_recv()
    normalize(tokens.at[step(x, 2)], rows, main_row(step(x, 2)))
    project_shard(step(x, 2))

    @pl.loop(0, 4)
    def _(k):
        prepare(lax.rem(far + 7 + k, blocks))

    @pl.loop(0, wide // 128)
    def _(j):
        lanes = pl.ds(pl.multiple_of(j * 128, 128), 128)
        backward = j >= half // 128
        total = jnp.zeros((STATE, 128), jnp.float32)
        decay = jnp.ones((1, 128), jnp.float32)
        for k in range(blocks):
            at = jnp.where(backward, blocks - 1 - k, k)
            part = decays[at, 0:1, lanes]
            total = total * part + states[at, :, lanes]
            decay = decay * part
        upper = decay.astype(jnp.bfloat16).astype(jnp.float32)
        centre = (decay - upper).astype(jnp.bfloat16).astype(jnp.float32)
        rest = decay - upper - centre
        place_row = iota((16, 128), 0)
        tail = jnp.where(place_row == 0, upper, jnp.where(place_row == 1, centre, rest))
        for q in range(4):
            totals[4 * j + q, 0:32, :] = total[32 * q : 32 * q + 32].astype(jnp.bfloat16)
            totals[4 * j + q, 32:48, :] = tail.astype(jnp.bfloat16)

    def outgoing(box, inbox, bank, k):
        to = lax.rem(me + k, 32)
        return pltpu.make_async_remote_copy(
            src_ref=box.at[to],
            dst_ref=inbox.at[me],
            send_sem=state_send.at[bank, k],
            recv_sem=state_recv.at[bank, me],
            device_id=stretch(to),
            device_id_type=MESH,
        )

    def expected(box, inbox, bank, k):
        source = lax.rem(me + k, 32)
        return pltpu.make_async_remote_copy(
            src_ref=box.at[me],
            dst_ref=inbox.at[source],
            send_sem=state_send.at[bank, k],
            recv_sem=state_recv.at[bank, source],
            device_id=stretch(source),
            device_id_type=MESH,
        )

    @pl.loop(1, 32)
    def _(k):
        outgoing(totals, arrived, 0, k).start()

    arrived[me] = totals[me]

    lo_second.forward()
    hi_second.forward()
    for by in (3, 1):
        across("o", wo, "z", by, (0, 2))
        across("o", wo, "y", by, (2, 2))

    def within(k):
        for g in range(groups):
            inner_product = dot_nt(
                outward[rows_of(k), g * STATE : (g + 1) * STATE],
                inward[rows_of(k), g * STATE : (g + 1) * STATE],
            )
            cells = signal[rows_of(k), g * span : (g + 1) * span]
            head_of = iota((BLOCK, span), 1) // HEAD_DIM
            weights, content = [], []
            for r in range(ratio):
                h = g * ratio + r
                below = column[rows_of(k), h : h + 1] + rowwise[k, h : h + 1, :]
                above = (
                    column[rows_of(k), heads + h : heads + h + 1]
                    + rowwise[k, heads + h : heads + h + 1, :]
                )
                decay = jnp.exp2(jnp.where(lower, below, above))
                both = jnp.where(
                    row == col, rowwise[k, 2 * heads + h : 2 * heads + h + 1, :], decay
                )
                weights.append((inner_product * both).astype(jnp.bfloat16))
                content.append(jnp.where(head_of == r, cells, jnp.zeros_like(cells)))
            inner[rows_of(k), g * span : (g + 1) * span] = dot(
                jnp.concatenate(weights, axis=1), jnp.concatenate(content, axis=0)
            )

    project_gate(step(x, 2))

    @pl.loop(0, blocks // 2)
    def _(k):
        within(k)

    @pl.loop(1, 32)
    def _(k):
        expected(totals, arrived, 0, k).wait_recv()

    flip = me >= 16

    def hop(k, state):
        at = jnp.where(flip, 31 - k, k)
        onward[at] = state.astype(jnp.bfloat16)
        message = arrived[at].astype(jnp.float32)
        decay = message[32:33] + message[33:34] + message[34:35]
        return state * decay + message[0:32]

    lax.fori_loop(0, 32, hop, jnp.zeros((32, 128), jnp.float32))

    @pl.loop(1, 32)
    def _(k):
        outgoing(onward, incoming, 1, k).start()

    incoming[me] = onward[me]

    @pl.loop(blocks // 2, blocks)
    def _(k):
        within(k)

    @pl.loop(1, 32)
    def _(k):
        expected(onward, incoming, 1, k).wait_recv()

    @pl.loop(0, wide // 128)
    def _(j):
        lanes = pl.ds(pl.multiple_of(j * 128, 128), 128)
        backward = j >= half // 128
        state = jnp.concatenate([incoming[4 * j + q] for q in range(4)], axis=0).astype(jnp.float32)
        for k in range(blocks):
            at = jnp.where(backward, blocks - 1 - k, k)
            before[at, :, lanes] = state.astype(jnp.bfloat16)
            state = state * decays[at, 0:1, lanes] + states[at, :, lanes]

    def finish(k):
        scale = dot(reading[rows_of(k), :], spread)
        for g in range(groups):
            lanes = slice(g * span, (g + 1) * span)
            read = outward[rows_of(k), g * STATE : (g + 1) * STATE]
            total = inner[rows_of(k), lanes]
            for way in range(2):
                placed = slice(way * half + g * span, way * half + (g + 1) * span)
                total = total + dot(read, before[k, :, placed]) * scale[:, placed]
            gated = total * gates[rows_of(k), lanes].astype(jnp.float32)
            level = lax.rsqrt(jnp.mean(gated * gated, axis=-1, keepdims=True) + EPSILON)
            mixed[rows_of(k), lanes] = (gated * level * gain_ref[:, lanes]).astype(jnp.bfloat16)

    def finish_shard(shard):
        @pl.loop(0, 2)
        def _(b):
            finish(2 * shard + b)

    def part(shard, some):
        start, size = some
        return mixed.at[pl.ds(pl.multiple_of(shard * rows + start, middle), size)]

    finish_shard(step(x, 2))
    relay_up = wire.go(part(step(x, 2), (0, middle)), up, relay.at[0])
    relay_down = wire.go(part(step(x, 2), (middle, middle)), down, relay.at[1])
    finish_shard(step(x, 1))
    near_up = wire.go(part(step(x, 1), (0, rows)), up, shards.at[x])
    finish_shard(step(x, 3))
    near_down = wire.go(part(step(x, 3), (0, rows)), down, shards.at[x])
    lo_second.finish()
    across("o", wo, "z", 2, (0, 2))
    hi_second.finish()
    across("o", wo, "y", 2, (2, 2))
    finish_shard(x)
    shards[x] = mixed[pl.ds(pl.multiple_of(x * rows, rows), rows), :]
    relay_up.wait_recv()
    far_up = wire.go(relay.at[0], up, shards.at[step(x, 3), low])
    relay_down.wait_recv()
    far_down = wire.go(relay.at[1], down, shards.at[step(x, 1), high])
    for copy in pairs["o"]:
        copy.wait_recv()

    def contribute(at, begin, end):
        @pl.loop(0, 8)
        def _(k):
            columns = pl.ds(pl.multiple_of(k * 256, 256), 256)
            weight = wo[k // 2, pl.ds(2 * lax.rem(k, 2), 2), :, at].reshape(256, -1)
            total = dot_nt(shards[at], weight)
            if not begin:
                total = total + summed[:, columns]
            if end:
                out_ref[:, columns] = total.astype(out_ref.dtype)
            else:
                summed[:, columns] = total

    contribute(x, True, False)
    near_up.wait_recv()
    contribute(step(x, 3), False, False)
    near_down.wait_recv()
    contribute(step(x, 1), False, False)
    far_up.wait_recv()
    far_down.wait_recv()
    contribute(step(x, 2), False, True)

    wire.drain()

    @pl.loop(1, 32)
    def _(k):
        outgoing(totals, arrived, 0, k).wait_send()
        outgoing(onward, incoming, 1, k).wait_send()

    @pl.when(x == 3)
    def _():
        for copy in halos[0]:
            copy.wait_send()

    @pl.when(x == 0)
    def _():
        for copy in halos[1]:
            copy.wait_send()


COPIES = 80


def mix(
    tokens,
    norm_gain,
    w_gate,
    w_value,
    w_state_in,
    w_state_out,
    w_step_forward,
    w_step_backward,
    head_rows,
    conv_value,
    conv_state_in,
    conv_state_out,
    out_gain,
    w_out,
):
    rows, width = tokens.shape
    depth, half = w_value.shape
    states = w_state_in.shape[1]
    blocks = 4 * rows // BLOCK
    vmem, anywhere = pl.BlockSpec(memory_space=pltpu.VMEM), pl.BlockSpec(memory_space=pl.ANY)
    bf16, f32 = jnp.bfloat16, jnp.float32
    return pl.pallas_call(
        functools.partial(mixer_kernel, math.log(4 * rows * lax.axis_size(SP))),
        out_shape=jax.ShapeDtypeStruct((rows, width), OUT_TYPE),
        in_specs=[anywhere, vmem] + [anywhere] * 3 + [vmem] * 2 + [anywhere] * 2 + [vmem] * 5,
        out_specs=vmem,
        scratch_shapes=[
            pltpu.VMEM((4, rows, width), bf16),
            pltpu.VMEM((2, HALO, width), bf16),
            pltpu.VMEM((4 * rows + 2 * HALO, width), bf16),
            pltpu.VMEM((4, 4, 2, depth, half), bf16),
            pltpu.VMEM((4, 4, 2, depth, 2 * states + 128), bf16),
            pltpu.VMEM((4, 4, 2, depth, half), bf16),
            pltpu.VMEM((4, 4, 2, 4, depth, half), bf16),
            pltpu.VMEM((4 * rows + 2 * HALO, 2 * half), bf16),
            pltpu.VMEM((4 * rows, half), bf16),
            pltpu.VMEM((4 * rows, 128), bf16),
            pltpu.VMEM((4 * rows, half), bf16),
            pltpu.VMEM((4 * rows, states), bf16),
            pltpu.VMEM((4 * rows, states), bf16),
            pltpu.VMEM((4 * rows, 128), f32),
            pltpu.VMEM((blocks, 24, 128), f32),
            pltpu.VMEM((4 * rows, 128), bf16),
            pltpu.VMEM((blocks, STATE, 2 * half), f32),
            pltpu.VMEM((blocks, 8, 2 * half), f32),
            pltpu.VMEM((blocks, STATE, 2 * half), bf16),
            pltpu.VMEM((4 * rows, half), f32),
            pltpu.VMEM((32, 48, 128), bf16),
            pltpu.VMEM((32, 48, 128), bf16),
            pltpu.VMEM((32, 32, 128), bf16),
            pltpu.VMEM((32, 32, 128), bf16),
            pltpu.VMEM((4 * rows, half), bf16),
            pltpu.VMEM((4, rows, half), bf16),
            pltpu.VMEM((2, rows // 2, half), bf16),
            pltpu.VMEM((rows, width), f32),
            pltpu.SemaphoreType.DMA((COPIES,)),
            pltpu.SemaphoreType.DMA((COPIES,)),
            pltpu.SemaphoreType.DMA((8,)),
            pltpu.SemaphoreType.DMA((2,)),
            pltpu.SemaphoreType.DMA((2, 32)),
            pltpu.SemaphoreType.DMA((2, 32)),
            pltpu.SemaphoreType.DMA((6,)),
        ],
        compiler_params=pltpu.CompilerParams(
            collective_id=0, has_side_effects=True, vmem_limit_bytes=60 * 2**20
        ),
        name="mixer",
    )(
        tokens,
        norm_gain.reshape(1, -1),
        w_value,
        w_state_in,
        w_state_out,
        w_step_forward.T,
        w_step_backward.T,
        w_gate,
        w_out.T,
        conv_value,
        conv_state_in,
        conv_state_out,
        head_rows,
        out_gain.reshape(1, -1),
    )


OUT_TYPE = jnp.bfloat16


def local(
    input_activations,
    norm_gain,
    w_gate,
    w_value,
    w_state_in,
    w_state_out,
    w_step_forward,
    w_step_backward,
    step_offset,
    fading_speed,
    conv_value,
    conv_state_in,
    conv_state_out,
    out_gain,
    w_out,
):
    head_rows = jnp.pad(
        jnp.stack([step_offset.reshape(-1), -fading_speed.reshape(-1)]),
        ((0, 0), (0, 128 - step_offset.size)),
    )
    return mix(
        input_activations,
        norm_gain,
        w_gate,
        w_value,
        w_state_in,
        w_state_out,
        w_step_forward,
        w_step_backward,
        head_rows,
        conv_value,
        conv_state_in,
        conv_state_out,
        out_gain,
        w_out,
    )


def solution(mesh):
    torus = Mesh(mesh.devices.reshape(4, 4, 2, 4), SP_TP)
    return jax.shard_map(
        local,
        mesh=torus,
        in_specs=(
            P(SP_TP, None),
            P(),
            P(SP, "x"),
            P(SP, "x"),
            P(SP, "x"),
            P(SP, "x"),
            P(SP, "x"),
            P(SP, "x"),
            P(None, "x"),
            P(None, "x"),
            P(None, "x"),
            P(None, "x"),
            P(None, "x"),
            P("x"),
            P("x", SP),
        ),
        out_specs=P(SP_TP, None),
        check_vma=False,
    )
```

```python
import functools
import math

import jax
import jax.numpy as jnp
from jax import lax
from jax.experimental import pallas as pl
from jax.experimental.pallas import tpu as pltpu
from jax.sharding import Mesh
from jax.sharding import PartitionSpec as P

HEAD_DIM = 64
STATE = 128
BLOCK = 128
SP = ("z", "y", "c")
SP_TP = ("z", "y", "c", "x")
EPSILON = 1e-06
MESH = pl.DeviceIdType.MESH
HALO = 16


def place():
    return [lax.axis_index(name) for name in ("z", "y", "c", "x")]


def step(at, by):
    return lax.rem(at + by + 4, 4)


def stretch_at(z, y, c, by):
    n = lax.rem(z * 8 + y * 2 + c + by + 32, 32)
    return {"z": n // 8, "y": lax.rem(n // 2, 4), "c": lax.rem(n, 2)}


class Wire:
    def __init__(self, send, recv):
        self.send, self.recv, self.count, self.sent = send, recv, 0, []

    def describe(self, source, target, to):
        k = self.count
        self.count += 1
        return pltpu.make_async_remote_copy(
            src_ref=source,
            dst_ref=target,
            send_sem=self.send.at[k],
            recv_sem=self.recv.at[k],
            device_id=to,
            device_id_type=MESH,
        )

    def go(self, source, to, target=None):
        copy = self.describe(source, source if target is None else target, to)
        copy.start()
        self.sent.append(copy)
        return copy

    def drain(self):
        for copy in self.sent:
            copy.wait_send()


class Ring:
    def __init__(self, wire, axis, at, block, low, high):
        self.wire, self.at = wire, at
        self.up, self.down = {axis: step(at, 1)}, {axis: step(at, 3)}
        self.block, self.low, self.high = block, low, high

    def start(self):
        self.a = self.wire.go(self.block(self.at), self.up)
        self.b = self.wire.go(self.block(self.at), self.down)

    def forward(self):
        self.a.wait_recv()
        self.c = self.wire.go(self.low(step(self.at, 3)), self.up)
        self.b.wait_recv()
        self.d = self.wire.go(self.high(step(self.at, 1)), self.down)

    def finish(self):
        self.c.wait_recv()
        self.d.wait_recv()


LOG2E = 1.4426950408889634


def dot_nt(a, b):
    return lax.dot_general(a, b, (((1,), (1,)), ((), ())), preferred_element_type=jnp.float32)


def dot_tn(a, b):
    return lax.dot_general(a, b, (((0,), (0,)), ((), ())), preferred_element_type=jnp.float32)


def dot(a, b, precision=None):
    return lax.dot_general(
        a, b, (((1,), (0,)), ((), ())), precision=precision, preferred_element_type=jnp.float32
    )


def iota(shape, dim):
    return lax.broadcasted_iota(jnp.int32, shape, dim)


def silu(v):
    part = 0.5 * v
    return part + part * jnp.tanh(part)


def mixer_kernel(
    shift,
    tokens_hbm,
    value_hbm,
    state_in_hbm,
    state_out_hbm,
    gate_hbm,
    w_out_hbm,
    norm_gain_hbm,
    step_forward_hbm,
    step_backward_hbm,
    tap_value_hbm,
    tap_in_hbm,
    tap_out_hbm,
    offset_hbm,
    speed_hbm,
    gain_hbm,
    out_ref,
    norm_gain_ref,
    step_forward_ref,
    step_backward_ref,
    tap_value_ref,
    tap_in_ref,
    tap_out_ref,
    offset_ref,
    speed_ref,
    gain_ref,
    heads_ref,
    squares,
    fades,
    tokens,
    edges,
    normed,
    wv,
    ws,
    wg,
    wo,
    projected,
    gates,
    raw,
    signal,
    inward,
    outward,
    column,
    rowwise,
    states,
    decays,
    before,
    inner,
    totals,
    arrived,
    onward,
    incoming,
    mixed,
    shards,
    relay,
    summed,
    send,
    recv,
    state_send,
    state_recv,
    local_sem,
):
    z, y, c, x = place()
    me = z * 8 + y * 2 + c
    wire = Wire(send, recv)
    rows = tokens.shape[1]
    middle = rows // 2
    count = 4 * rows
    blocks = count // BLOCK
    half = signal.shape[1]
    wide = 2 * half
    groups = inward.shape[1] // STATE
    ratio = half // HEAD_DIM // groups
    heads = groups * ratio
    span = ratio * HEAD_DIM
    lead = inward.shape[1]
    partner = {"c": 1 - c}

    def stretch(n):
        return {"z": n // 8, "y": lax.rem(n // 2, 4), "c": lax.rem(n, 2)}

    own = [
        pltpu.make_async_copy(tokens_hbm, tokens.at[x], local_sem.at[0]),
        pltpu.make_async_copy(value_hbm, wv.at[z, y, c], local_sem.at[1]),
        pltpu.make_async_copy(state_in_hbm, ws.at[z, y, c, :, pl.ds(0, lead)], local_sem.at[2]),
        pltpu.make_async_copy(state_out_hbm, ws.at[z, y, c, :, pl.ds(lead, lead)], local_sem.at[3]),
        pltpu.make_async_copy(gate_hbm, wg.at[z, y, c], local_sem.at[4]),
        pltpu.make_async_copy(w_out_hbm, wo.at[z, y, c, x], local_sem.at[5]),
    ]
    small = (
        (step_forward_hbm, step_forward_ref),
        (step_backward_hbm, step_backward_ref),
        (offset_hbm, offset_ref),
        (speed_hbm, speed_ref),
        (norm_gain_hbm, norm_gain_ref),
        (tap_value_hbm, tap_value_ref),
        (tap_in_hbm, tap_in_ref),
        (tap_out_hbm, tap_out_ref),
        (gain_hbm, gain_ref),
    )
    own += [
        pltpu.make_async_copy(source, target, local_sem.at[6 + k])
        for k, (source, target) in enumerate(small)
    ]
    for copy in own:
        copy.start()
    barrier = pltpu.get_barrier_semaphore()

    near = [{axis: step(at, by)} for axis, at in (("x", x), ("y", y), ("z", z)) for by in (1, 3)]
    for other in near + [partner]:
        pl.semaphore_signal(barrier, inc=1, device_id=other, device_id_type=MESH)
    for copy in own:
        copy.wait()
    depth = step_forward_ref.shape[1]
    steps = jnp.concatenate(
        [
            step_forward_ref[...].astype(jnp.float32),
            step_backward_ref[...].astype(jnp.float32),
            jnp.zeros((128 - 2 * heads, depth), jnp.float32),
        ],
        axis=0,
    )
    steps = jnp.concatenate([steps, jnp.zeros((128, 128 - depth), jnp.float32)], axis=1).T
    ws[z, y, c, :, 2 * lead :] = steps[0:depth].astype(jnp.bfloat16)
    lines = jnp.concatenate(
        [
            jnp.concatenate([ref[w : w + 1, :] * sign for w in range(2)], axis=1)
            for ref, sign in ((offset_ref, 1.0), (speed_ref, -1.0))
        ],
        axis=0,
    )
    lines = jnp.concatenate([lines, jnp.zeros((2, 128 - 2 * heads), jnp.float32)], axis=1)
    heads_ref[...] = jnp.concatenate([lines, jnp.zeros((126, 128), jnp.float32)], axis=0).T[
        0 : 2 * heads
    ]
    pl.semaphore_wait(barrier, 7)

    wo_x = Ring(
        wire,
        "x",
        x,
        lambda at: wo.at[z, y, c, at],
        lambda at: wo.at[z, y, c, at, pl.ds(0, 32)],
        lambda at: wo.at[z, y, c, at, pl.ds(32, 32)],
    )
    wo_x.start()

    low, high = pl.ds(0, middle), pl.ds(middle, middle)
    up, down = {"x": step(x, 1)}, {"x": step(x, 3)}
    up_low = wire.go(tokens.at[x, low], up)
    down_high = wire.go(tokens.at[x, high], down)
    up_high = wire.go(tokens.at[x, high], up)
    down_low = wire.go(tokens.at[x, low], down)

    def first(buffer, axis, keep=()):
        def at(n, part):
            spot = (z, n, c) if axis == "y" else (n, y, c)
            if keep:
                start, size = keep
                return buffer.at[(*spot, pl.ds(start, size) if part is None else start + part)]
            return buffer.at[spot] if part is None else buffer.at[(*spot, pl.ds(32 * part, 32))]

        here = y if axis == "y" else z
        return Ring(
            wire, axis, here, lambda n: at(n, None), lambda n: at(n, 0), lambda n: at(n, 1)
        )

    def group(buffer, axis, n, part, keep):
        some = pl.ds(0, 4) if part is None else pl.ds(2 * part, 2)
        spot = (n, some, c) if axis == "z" else (some, n, c)
        return buffer.at[(*spot, pl.ds(*keep))] if keep else buffer.at[spot]

    def second(buffer, axis, keep=()):
        here = y if axis == "y" else z
        return Ring(
            wire,
            axis,
            here,
            lambda n: group(buffer, axis, n, None, keep),
            lambda n: group(buffer, axis, n, 0, keep),
            lambda n: group(buffer, axis, n, 1, keep),
        )

    pairs = {}

    def across(name, buffer, axis, by, keep=()):
        here = y if axis == "y" else z
        copy = wire.go(group(buffer, axis, step(here, by), None, keep), partner)
        pairs.setdefault(name, []).append(copy)

    v_first, s_first = first(wv, "y"), first(ws, "z")
    v_first.start()
    s_first.start()

    def main_row(shard):
        return HALO + shard * rows

    def normalize(ref, size, to):
        width = ref.shape[-1]

        @pl.loop(0, size // 16)
        def _(k):
            taken = pl.ds(pl.multiple_of(k * 16, 16), 16)
            cells = ref[taken, :].astype(jnp.float32)
            total = cells[:, 0:128] * cells[:, 0:128]
            for at in range(128, width, 128):
                total = total + cells[:, at : at + 128] * cells[:, at : at + 128]
            squares[taken, :] = total

        level = lax.rsqrt(
            jnp.sum(squares[0:size, :], axis=-1, keepdims=True) * (1.0 / width) + EPSILON
        )
        squares[0:size, :] = jnp.broadcast_to(level, (size, 128))

        @pl.loop(0, size // 16)
        def _(k):
            taken = pl.ds(pl.multiple_of(k * 16, 16), 16)
            scale = squares[taken, :]
            cells = ref[taken, :].astype(jnp.float32)
            placed = pl.ds(pl.multiple_of(to + k * 16, 16), 16)
            for at in range(0, width, 128):
                normed[placed, at : at + 128] = (
                    cells[:, at : at + 128] * scale * norm_gain_ref[:, at : at + 128]
                ).astype(jnp.bfloat16)

    shard_in = (x, step(x, 3), step(x, 1), step(x, 2))

    def project(slots):
        edge = not slots
        begin, size = (slots[0] * rows, len(slots) * rows) if slots else (4 * rows, 2 * HALO)
        taken = pl.ds(begin, size)

        def put(values, columns):
            for k, slot in enumerate(slots):
                placed = pl.ds(pl.multiple_of(main_row(shard_in[slot]), 16), rows)
                projected[placed, columns] = values[k * rows : (k + 1) * rows]
            if edge:
                projected[0:HALO, columns] = jnp.where(me > 0, values[0:HALO], 0).astype(
                    values.dtype
                )
                projected[main_row(4) : main_row(4) + HALO, columns] = jnp.where(
                    me < 31, values[HALO:], 0
                ).astype(values.dtype)

        for weights, total, start in ((wv, half, 0), (ws, 2 * lead, half)):

            @pl.loop(0, total // 256)
            def _(k):
                columns = pl.ds(pl.multiple_of(k * 256, 256), 256)
                put(
                    dot(normed[taken, :], weights[:, :, :, :, columns].reshape(-1, 256)).astype(
                        jnp.bfloat16
                    ),
                    pl.ds(pl.multiple_of(start + k * 256, 256), 256),
                )

        if edge:
            return
        values = dot(normed[taken, :], ws[:, :, :, :, 2 * lead :].reshape(-1, 128)).astype(
            jnp.bfloat16
        )
        for k, slot in enumerate(slots):
            placed = pl.ds(pl.multiple_of(shard_in[slot] * rows, rows), rows)
            raw[placed, :] = values[k * rows : (k + 1) * rows]

    def project_gate(slots):
        taken = pl.ds(slots[0] * rows, len(slots) * rows)

        @pl.loop(0, half // 256)
        def _(k):
            columns = pl.ds(pl.multiple_of(k * 256, 256), 256)
            values = dot(normed[taken, :], wg[:, :, :, :, columns].reshape(-1, 256))
            values = silu(values.astype(jnp.bfloat16).astype(jnp.float32)).astype(jnp.bfloat16)
            for k, slot in enumerate(slots):
                placed = pl.ds(pl.multiple_of(shard_in[slot] * rows, rows), rows)
                gates[placed, columns] = values[k * rows : (k + 1) * rows]

    normalize(tokens.at[x], rows, 0)

    v_first.forward()
    s_first.forward()
    wo_x.forward()
    v_first.finish()
    v_second = second(wv, "z")
    v_second.start()
    across("v", wv, "z", 0)
    s_first.finish()
    s_second = second(ws, "y")
    s_second.start()
    across("s", ws, "y", 0)
    g_first = first(wg, "z")
    g_first.start()

    up_low.wait_recv()
    down_high.wait_recv()
    far = [
        wire.go(tokens.at[step(x, by), pl.ds(*some)], to)
        for by, some, to in (
            (3, (0, HALO), up),
            (1, (rows - HALO, HALO), down),
            (3, (HALO, middle - HALO), up),
            (1, (middle, middle - HALO), down),
        )
    ]
    normalize(tokens.at[step(x, 3), low], middle, rows)
    normalize(tokens.at[step(x, 1), high], middle, 2 * rows + middle)

    v_second.forward()
    s_second.forward()
    for by in (3, 1):
        across("v", wv, "z", by)
        across("s", ws, "y", by)
    g_first.forward()
    v_second.finish()
    across("v", wv, "z", 2)
    s_second.finish()
    across("s", ws, "y", 2)
    g_first.finish()
    g_second = second(wg, "y")
    g_second.start()
    across("g", wg, "y", 0)
    for copy in pairs["v"] + pairs["s"]:
        copy.wait_recv()
    project((0,))

    up_high.wait_recv()
    down_low.wait_recv()
    wo_x.finish()
    normalize(tokens.at[step(x, 3), high], middle, rows + middle)
    normalize(tokens.at[step(x, 1), low], middle, 2 * rows)
    lo_first, hi_first = first(wo, "y", (0, 2)), first(wo, "z", (2, 2))
    lo_first.start()
    hi_first.start()
    far[0].wait_recv()
    far[1].wait_recv()
    edge_in = [
        wire.go(
            tokens.at[shard, pl.ds(offset, HALO)],
            stretch_at(z, y, c, by),
            edges.at[pl.ds(slot * HALO, HALO)],
        )
        for slot, (shard, offset, by) in enumerate(((3, rows - HALO, 1), (0, 0, 31)))
    ]
    project((1, 2))
    g_second.forward()
    across("g", wg, "y", 3)
    across("g", wg, "y", 1)
    lo_first.forward()
    hi_first.forward()
    for copy in edge_in:
        copy.wait_recv()
    normalize(edges, 2 * HALO, 4 * rows)
    project(())

    row, col = iota((BLOCK, BLOCK), 0), iota((BLOCK, BLOCK), 1)
    lower = row >= col
    triangle = jnp.where(row <= col, 1.0, 0.0)
    forward_row = iota((2 * heads, BLOCK), 0) < heads

    def spread(kind):
        place_of = iota((128, wide), 1) // HEAD_DIM + 2 * heads * kind
        return jnp.where(place_of == iota((128, wide), 0), 1.0, 0.0)

    spread_weight = spread(2).astype(jnp.bfloat16)

    def rows_of(k):
        return pl.ds(pl.multiple_of(k * BLOCK, BLOCK), BLOCK)

    def prepare(k):
        window = pl.ds(pl.multiple_of(k * BLOCK, BLOCK), BLOCK + 2 * HALO)
        for at in range(0, wide, 128):
            if at < half:
                tap_ref, target, begin = tap_value_ref, signal, at
            elif at < half + lead:
                tap_ref, target, begin = tap_in_ref, inward, at - half
            else:
                tap_ref, target, begin = tap_out_ref, outward, at - half - lead
            cells = projected[window, at : at + 128].astype(jnp.float32)
            tap = tap_ref[:, begin : begin + 128]
            here = slice(HALO, HALO + BLOCK)
            total = (
                tap[0:1] * pltpu.roll(cells, 1, 0)[here]
                + tap[1:2] * cells[here]
                + tap[2:3] * pltpu.roll(cells, BLOCK + 2 * HALO - 1, 0)[here]
            )
            target[rows_of(k), begin : begin + 128] = silu(total).astype(jnp.bfloat16)

        size = jax.nn.softplus(
            raw[rows_of(k), :].astype(jnp.float32).T[0 : 2 * heads] + heads_ref[:, 0:1] - shift
        )
        logs = size * heads_ref[:, 1:2]
        through = dot(logs, triangle, lax.Precision.HIGHEST)
        until = through - logs
        whole = through[:, BLOCK - 1 : BLOCK]
        logsize = jnp.log(size)
        rowwise[k, 0 : 2 * heads, :] = (
            jnp.where(forward_row, logsize - through, logsize + until) * LOG2E
        )
        rowwise[k, 2 * heads : 3 * heads, :] = size[0:heads] + size[heads : 2 * heads]
        turned = jnp.concatenate(
            [
                jnp.where(forward_row, through, -until) * LOG2E,
                jnp.exp(jnp.where(forward_row, through, whole - until)),
                size * jnp.exp(jnp.where(forward_row, whole - through, until)),
                jnp.broadcast_to(jnp.exp(whole), (2 * heads, BLOCK)),
                jnp.zeros((128 - 8 * heads, BLOCK), jnp.float32),
            ],
            axis=0,
        ).T
        column[rows_of(k), :] = turned
        fades[k] = turned[0:8]
        weights = dot(turned.astype(jnp.bfloat16), spread_weight)
        for way in range(2):
            for g in range(groups):
                lanes = slice(g * span, (g + 1) * span)
                placed = slice(way * half + g * span, way * half + (g + 1) * span)
                content = (
                    signal[rows_of(k), lanes].astype(jnp.float32) * weights[:, placed]
                ).astype(jnp.bfloat16)
                states[k, :, placed] = dot_tn(
                    inward[rows_of(k), g * STATE : (g + 1) * STATE], content
                )

    away = 2 * step(x, 2)

    @pl.loop(0, 4)
    def _(k):
        prepare(lax.rem(away + 3 + k, blocks))

    lo_first.finish()
    lo_second = second(wo, "z", (0, 2))
    lo_second.start()
    across("o", wo, "z", 0, (0, 2))
    hi_first.finish()
    hi_second = second(wo, "y", (2, 2))
    hi_second.start()
    across("o", wo, "y", 0, (2, 2))

    g_second.finish()
    across("g", wg, "y", 2)
    for copy in pairs["g"]:
        copy.wait_recv()
    project_gate((0, 1, 2))

    far[2].wait_recv()
    far[3].wait_recv()
    normalize(tokens.at[step(x, 2)], rows, 3 * rows)
    project((3,))

    @pl.loop(0, 4)
    def _(k):
        prepare(lax.rem(away + 7 + k, blocks))

    over = dot(
        jnp.concatenate([fades[k, 0:1, :] for k in range(blocks)], axis=0),
        spread(3),
        lax.Precision.HIGHEST,
    )
    for k in range(blocks):
        decays[k] = jnp.broadcast_to(over[k : k + 1], (8, wide))

    @pl.loop(0, wide // 128)
    def _(j):
        lanes = pl.ds(pl.multiple_of(j * 128, 128), 128)
        backward = j >= half // 128
        total = jnp.zeros((STATE, 128), jnp.float32)
        decay = jnp.ones((1, 128), jnp.float32)
        for k in range(blocks):
            at = jnp.where(backward, blocks - 1 - k, k)
            part = decays[at, 0:1, lanes]
            total = total * part + states[at, :, lanes]
            decay = decay * part
        upper = decay.astype(jnp.bfloat16).astype(jnp.float32)
        centre = (decay - upper).astype(jnp.bfloat16).astype(jnp.float32)
        rest = decay - upper - centre
        place_row = iota((16, 128), 0)
        tail = jnp.where(place_row == 0, upper, jnp.where(place_row == 1, centre, rest))
        for q in range(4):
            totals[4 * j + q, 0:32, :] = total[32 * q : 32 * q + 32].astype(jnp.bfloat16)
            totals[4 * j + q, 32:48, :] = tail.astype(jnp.bfloat16)

    def outgoing(box, inbox, bank, k):
        to = lax.rem(me + k, 32)
        return pltpu.make_async_remote_copy(
            src_ref=box.at[to],
            dst_ref=inbox.at[me],
            send_sem=state_send.at[bank, k],
            recv_sem=state_recv.at[bank, me],
            device_id=stretch(to),
            device_id_type=MESH,
        )

    def expected(box, inbox, bank, k):
        source = lax.rem(me + k, 32)
        return pltpu.make_async_remote_copy(
            src_ref=box.at[me],
            dst_ref=inbox.at[source],
            send_sem=state_send.at[bank, k],
            recv_sem=state_recv.at[bank, source],
            device_id=stretch(source),
            device_id_type=MESH,
        )

    @pl.loop(1, 32)
    def _(k):
        outgoing(totals, arrived, 0, k).start()

    arrived[me] = totals[me]

    lo_second.forward()
    hi_second.forward()
    for by in (3, 1):
        across("o", wo, "z", by, (0, 2))
        across("o", wo, "y", by, (2, 2))

    def within(k):
        for g in range(groups):
            inner_product = dot_nt(
                outward[rows_of(k), g * STATE : (g + 1) * STATE],
                inward[rows_of(k), g * STATE : (g + 1) * STATE],
            )
            cells = signal[rows_of(k), g * span : (g + 1) * span]
            head_of = iota((BLOCK, span), 1) // HEAD_DIM
            weights, content = [], []
            for r in range(ratio):
                h = g * ratio + r
                below = column[rows_of(k), h : h + 1] + rowwise[k, h : h + 1, :]
                above = (
                    column[rows_of(k), heads + h : heads + h + 1]
                    + rowwise[k, heads + h : heads + h + 1, :]
                )
                decay = jnp.exp2(jnp.where(lower, below, above))
                both = jnp.where(
                    row == col, rowwise[k, 2 * heads + h : 2 * heads + h + 1, :], decay
                )
                weights.append((inner_product * both).astype(jnp.bfloat16))
                content.append(jnp.where(head_of == r, cells, jnp.zeros_like(cells)))
            inner[rows_of(k), g * span : (g + 1) * span] = dot(
                jnp.concatenate(weights, axis=1), jnp.concatenate(content, axis=0)
            )

    project_gate((3,))

    @pl.loop(0, blocks // 2)
    def _(k):
        within(k)

    @pl.loop(1, 32)
    def _(k):
        expected(totals, arrived, 0, k).wait_recv()

    flip = me >= 16

    def hop(k, state):
        at = jnp.where(flip, 31 - k, k)
        onward[at] = state.astype(jnp.bfloat16)
        message = arrived[at].astype(jnp.float32)
        decay = message[32:33] + message[33:34] + message[34:35]
        return state * decay + message[0:32]

    lax.fori_loop(0, 32, hop, jnp.zeros((32, 128), jnp.float32))

    @pl.loop(1, 32)
    def _(k):
        outgoing(onward, incoming, 1, k).start()

    incoming[me] = onward[me]

    @pl.loop(blocks // 2, blocks)
    def _(k):
        within(k)

    @pl.loop(1, 32)
    def _(k):
        expected(onward, incoming, 1, k).wait_recv()

    @pl.loop(0, wide // 128)
    def _(j):
        lanes = pl.ds(pl.multiple_of(j * 128, 128), 128)
        backward = j >= half // 128
        state = jnp.concatenate([incoming[4 * j + q] for q in range(4)], axis=0).astype(jnp.float32)
        for k in range(blocks):
            at = jnp.where(backward, blocks - 1 - k, k)
            before[at, :, lanes] = state.astype(jnp.bfloat16)
            state = state * decays[at, 0:1, lanes] + states[at, :, lanes]

    spread_read = spread(1).astype(jnp.bfloat16)

    def finish(k):
        scale = dot(column[rows_of(k), :].astype(jnp.bfloat16), spread_read)
        for g in range(groups):
            lanes = slice(g * span, (g + 1) * span)
            read = outward[rows_of(k), g * STATE : (g + 1) * STATE]
            total = inner[rows_of(k), lanes]
            for way in range(2):
                placed = slice(way * half + g * span, way * half + (g + 1) * span)
                total = total + dot(read, before[k, :, placed]) * scale[:, placed]
            gated = total * gates[rows_of(k), lanes].astype(jnp.float32)
            level = lax.rsqrt(jnp.mean(gated * gated, axis=-1, keepdims=True) + EPSILON)
            mixed[rows_of(k), lanes] = (gated * level * gain_ref[:, lanes]).astype(jnp.bfloat16)

    def finish_shard(shard):
        @pl.loop(0, 2)
        def _(b):
            finish(2 * shard + b)

    def part(shard, some):
        start, size = some
        return mixed.at[pl.ds(pl.multiple_of(shard * rows + start, middle), size)]

    finish_shard(step(x, 2))
    relay_up = wire.go(part(step(x, 2), (0, middle)), up, relay.at[0])
    relay_down = wire.go(part(step(x, 2), (middle, middle)), down, relay.at[1])
    finish_shard(step(x, 1))
    near_up = wire.go(part(step(x, 1), (0, rows)), up, shards.at[x])
    finish_shard(step(x, 3))
    near_down = wire.go(part(step(x, 3), (0, rows)), down, shards.at[x])
    lo_second.finish()
    across("o", wo, "z", 2, (0, 2))
    hi_second.finish()
    across("o", wo, "y", 2, (2, 2))
    finish_shard(x)
    shards[x] = mixed[pl.ds(pl.multiple_of(x * rows, rows), rows), :]
    relay_up.wait_recv()
    far_up = wire.go(relay.at[0], up, shards.at[step(x, 3), low])
    relay_down.wait_recv()
    far_down = wire.go(relay.at[1], down, shards.at[step(x, 1), high])
    for copy in pairs["o"]:
        copy.wait_recv()

    def contribute(at, begin, end):
        @pl.loop(0, 4)
        def _(k):
            lines = pl.ds(pl.multiple_of(k * 512, 512), 512)
            total = dot_nt(wo[k, :, :, at].reshape(512, -1), shards[at])
            if not begin:
                total = total + summed[lines, :]
            if end:
                out_ref[:, lines] = total.T.astype(out_ref.dtype)
            else:
                summed[lines, :] = total

    contribute(x, True, False)
    near_up.wait_recv()
    contribute(step(x, 3), False, False)
    near_down.wait_recv()
    contribute(step(x, 1), False, False)
    far_up.wait_recv()
    far_down.wait_recv()
    contribute(step(x, 2), False, True)

    wire.drain()

    @pl.loop(1, 32)
    def _(k):
        outgoing(totals, arrived, 0, k).wait_send()
        outgoing(onward, incoming, 1, k).wait_send()


COPIES = 80


def mix(
    tokens,
    norm_gain,
    w_gate,
    w_value,
    w_state_in,
    w_state_out,
    w_step_forward,
    w_step_backward,
    step_offset,
    fading_speed,
    conv_value,
    conv_state_in,
    conv_state_out,
    out_gain,
    w_out,
):
    rows, width = tokens.shape
    depth, half = w_value.shape
    states = w_state_in.shape[1]
    blocks = 4 * rows // BLOCK
    vmem, anywhere = pl.BlockSpec(memory_space=pltpu.VMEM), pl.BlockSpec(memory_space=pl.ANY)
    bf16, f32 = jnp.bfloat16, jnp.float32
    return pl.pallas_call(
        functools.partial(mixer_kernel, math.log(4 * rows * lax.axis_size(SP))),
        out_shape=jax.ShapeDtypeStruct((rows, width), OUT_TYPE),
        in_specs=[anywhere] * 15,
        out_specs=vmem,
        scratch_shapes=[
            pltpu.VMEM((1, width), f32),
            pltpu.VMEM(w_step_forward.shape[::-1], bf16),
            pltpu.VMEM(w_step_backward.shape[::-1], bf16),
            pltpu.VMEM(conv_value.shape, f32),
            pltpu.VMEM(conv_state_in.shape, f32),
            pltpu.VMEM(conv_state_out.shape, f32),
            pltpu.VMEM(step_offset.shape, f32),
            pltpu.VMEM(fading_speed.shape, f32),
            pltpu.VMEM((1, half), f32),
            pltpu.VMEM((16, 128), f32),
            pltpu.VMEM((rows, 128), f32),
            pltpu.VMEM((blocks, 8, 128), f32),
            pltpu.VMEM((4, rows, width), bf16),
            pltpu.VMEM((2 * HALO, width), bf16),
            pltpu.VMEM((4 * rows + 2 * HALO, width), bf16),
            pltpu.VMEM((4, 4, 2, depth, half), bf16),
            pltpu.VMEM((4, 4, 2, depth, 2 * states + 128), bf16),
            pltpu.VMEM((4, 4, 2, depth, half), bf16),
            pltpu.VMEM((4, 4, 2, 4, depth, half), bf16),
            pltpu.VMEM((4 * rows + 2 * HALO, 2 * half), bf16),
            pltpu.VMEM((4 * rows, half), bf16),
            pltpu.VMEM((4 * rows, 128), bf16),
            pltpu.VMEM((4 * rows, half), bf16),
            pltpu.VMEM((4 * rows, states), bf16),
            pltpu.VMEM((4 * rows, states), bf16),
            pltpu.VMEM((4 * rows, 128), f32),
            pltpu.VMEM((blocks, 24, 128), f32),
            pltpu.VMEM((blocks, STATE, 2 * half), f32),
            pltpu.VMEM((blocks, 8, 2 * half), f32),
            pltpu.VMEM((blocks, STATE, 2 * half), bf16),
            pltpu.VMEM((4 * rows, half), f32),
            pltpu.VMEM((32, 48, 128), bf16),
            pltpu.VMEM((32, 48, 128), bf16),
            pltpu.VMEM((32, 32, 128), bf16),
            pltpu.VMEM((32, 32, 128), bf16),
            pltpu.VMEM((4 * rows, half), bf16),
            pltpu.VMEM((4, rows, half), bf16),
            pltpu.VMEM((2, rows // 2, half), bf16),
            pltpu.VMEM((width, rows), f32),
            pltpu.SemaphoreType.DMA((COPIES,)),
            pltpu.SemaphoreType.DMA((COPIES,)),
            pltpu.SemaphoreType.DMA((2, 32)),
            pltpu.SemaphoreType.DMA((2, 32)),
            pltpu.SemaphoreType.DMA((15,)),
        ],
        compiler_params=pltpu.CompilerParams(
            collective_id=0, has_side_effects=True, vmem_limit_bytes=60 * 2**20
        ),
        name="mixer",
    )(
        tokens,
        w_value,
        w_state_in,
        w_state_out,
        w_gate,
        w_out.T,
        norm_gain.reshape(1, -1),
        w_step_forward.T,
        w_step_backward.T,
        conv_value,
        conv_state_in,
        conv_state_out,
        step_offset,
        fading_speed,
        out_gain.reshape(1, -1),
    )


OUT_TYPE = jnp.bfloat16


def local(
    input_activations,
    norm_gain,
    w_gate,
    w_value,
    w_state_in,
    w_state_out,
    w_step_forward,
    w_step_backward,
    step_offset,
    fading_speed,
    conv_value,
    conv_state_in,
    conv_state_out,
    out_gain,
    w_out,
):
    return mix(
        input_activations,
        norm_gain,
        w_gate,
        w_value,
        w_state_in,
        w_state_out,
        w_step_forward,
        w_step_backward,
        step_offset,
        fading_speed,
        conv_value,
        conv_state_in,
        conv_state_out,
        out_gain,
        w_out,
    )


def solution(mesh):
    torus = Mesh(mesh.devices.reshape(4, 4, 2, 4), SP_TP)
    return jax.shard_map(
        local,
        mesh=torus,
        in_specs=(
            P(SP_TP, None),
            P(),
            P(SP, "x"),
            P(SP, "x"),
            P(SP, "x"),
            P(SP, "x"),
            P(SP, "x"),
            P(SP, "x"),
            P(None, "x"),
            P(None, "x"),
            P(None, "x"),
            P(None, "x"),
            P(None, "x"),
            P("x"),
            P("x", SP),
        ),
        out_specs=P(SP_TP, None),
        check_vma=False,
    )
```

```python
import functools
import math

import jax
import jax.numpy as jnp
from jax import lax
from jax.experimental import pallas as pl
from jax.experimental.pallas import tpu as pltpu
from jax.sharding import Mesh
from jax.sharding import PartitionSpec as P

HEAD_DIM = 64
STATE = 128
BLOCK = 128
SP = ("z", "y", "c")
SP_TP = ("z", "y", "c", "x")
EPSILON = 1e-06
MESH = pl.DeviceIdType.MESH
VALUE, INWARD, OUTWARD, STEPS = range(4)
HALO = 16


def place():
    return [lax.axis_index(name) for name in ("z", "y", "c", "x")]


def step(at, by):
    return lax.rem(at + by + 4, 4)


def stretch_at(z, y, c, by):
    n = lax.rem(z * 8 + y * 2 + c + by + 32, 32)
    return {"z": n // 8, "y": lax.rem(n // 2, 4), "c": lax.rem(n, 2)}


class Wire:
    def __init__(self, send, recv):
        self.send, self.recv, self.count, self.sent = send, recv, 0, []

    def describe(self, source, target, to):
        k = self.count
        self.count += 1
        return pltpu.make_async_remote_copy(
            src_ref=source,
            dst_ref=target,
            send_sem=self.send.at[k],
            recv_sem=self.recv.at[k],
            device_id=to,
            device_id_type=MESH,
        )

    def go(self, source, to, target=None):
        copy = self.describe(source, source if target is None else target, to)
        copy.start()
        self.sent.append(copy)
        return copy

    def drain(self):
        for copy in self.sent:
            copy.wait_send()


class Ring:
    def __init__(self, wire, axis, at, block, low, high):
        self.wire, self.at = wire, at
        self.up, self.down = {axis: step(at, 1)}, {axis: step(at, 3)}
        self.block, self.low, self.high = block, low, high

    def start(self):
        self.a = self.wire.go(self.block(self.at), self.up)
        self.b = self.wire.go(self.block(self.at), self.down)

    def forward(self):
        self.a.wait_recv()
        self.c = self.wire.go(self.low(step(self.at, 3)), self.up)
        self.b.wait_recv()
        self.d = self.wire.go(self.high(step(self.at, 1)), self.down)

    def finish(self):
        self.c.wait_recv()
        self.d.wait_recv()


LOG2E = 1.4426950408889634


def dot_nt(a, b):
    return lax.dot_general(a, b, (((1,), (1,)), ((), ())), preferred_element_type=jnp.float32)


def dot_tn(a, b):
    return lax.dot_general(a, b, (((0,), (0,)), ((), ())), preferred_element_type=jnp.float32)


def dot(a, b, precision=None):
    return lax.dot_general(
        a, b, (((1,), (0,)), ((), ())), precision=precision, preferred_element_type=jnp.float32
    )


def iota(shape, dim):
    return lax.broadcasted_iota(jnp.int32, shape, dim)


def silu(v):
    part = 0.5 * v
    return part + part * jnp.tanh(part)


def mixer_kernel(
    shift,
    tokens_hbm,
    value_hbm,
    state_in_hbm,
    state_out_hbm,
    gate_hbm,
    w_out_hbm,
    norm_gain_hbm,
    step_forward_hbm,
    step_backward_hbm,
    tap_value_hbm,
    tap_in_hbm,
    tap_out_hbm,
    offset_hbm,
    speed_hbm,
    gain_hbm,
    out_hbm,
    norm_gain_ref,
    step_forward_ref,
    step_backward_ref,
    tap_value_ref,
    tap_in_ref,
    tap_out_ref,
    offset_ref,
    speed_ref,
    gain_ref,
    heads_ref,
    squares,
    fades,
    out_ref,
    tokens,
    edges,
    normed,
    wv,
    ws,
    wg,
    wo,
    projected,
    gates,
    raw,
    signal,
    inward,
    outward,
    column,
    rowwise,
    states,
    decays,
    before,
    inner,
    totals,
    arrived,
    onward,
    incoming,
    mixed,
    shards,
    relay,
    summed,
    send,
    recv,
    state_send,
    state_recv,
    local_sem,
):
    z, y, c, x = place()
    me = z * 8 + y * 2 + c
    wire = Wire(send, recv)
    rows = tokens.shape[1]
    middle = rows // 2
    count = 4 * rows
    blocks = count // BLOCK
    half = signal.shape[1]
    wide = 2 * half
    groups = inward.shape[1] // STATE
    ratio = half // HEAD_DIM // groups
    heads = groups * ratio
    span = ratio * HEAD_DIM
    lead = inward.shape[1]
    partner = {"c": 1 - c}

    def stretch(n):
        return {"z": n // 8, "y": lax.rem(n // 2, 4), "c": lax.rem(n, 2)}

    own = [
        pltpu.make_async_copy(tokens_hbm, tokens.at[x], local_sem.at[0]),
        pltpu.make_async_copy(value_hbm, wv.at[z, y, c], local_sem.at[1]),
        pltpu.make_async_copy(state_in_hbm, ws.at[z, y, c, :, pl.ds(0, lead)], local_sem.at[2]),
        pltpu.make_async_copy(state_out_hbm, ws.at[z, y, c, :, pl.ds(lead, lead)], local_sem.at[3]),
        pltpu.make_async_copy(gate_hbm, wg.at[z, y, c], local_sem.at[4]),
        pltpu.make_async_copy(w_out_hbm, wo.at[z, y, c, x], local_sem.at[5]),
    ]
    small = (
        (step_forward_hbm, step_forward_ref),
        (step_backward_hbm, step_backward_ref),
        (offset_hbm, offset_ref),
        (speed_hbm, speed_ref),
        (norm_gain_hbm, norm_gain_ref),
        (tap_value_hbm, tap_value_ref),
        (tap_in_hbm, tap_in_ref),
        (tap_out_hbm, tap_out_ref),
        (gain_hbm, gain_ref),
    )
    own += [
        pltpu.make_async_copy(source, target, local_sem.at[6 + k])
        for k, (source, target) in enumerate(small)
    ]
    for copy in own:
        copy.start()
    barrier = pltpu.get_barrier_semaphore()

    near = [{axis: step(at, by)} for axis, at in (("x", x), ("y", y), ("z", z)) for by in (1, 3)]
    for other in near + [partner]:
        pl.semaphore_signal(barrier, inc=1, device_id=other, device_id_type=MESH)
    for copy in own:
        copy.wait()
    depth = step_forward_ref.shape[1]
    steps = jnp.concatenate(
        [
            step_forward_ref[...].astype(jnp.float32),
            step_backward_ref[...].astype(jnp.float32),
            jnp.zeros((128 - 2 * heads, depth), jnp.float32),
        ],
        axis=0,
    )
    steps = jnp.concatenate([steps, jnp.zeros((128, 128 - depth), jnp.float32)], axis=1).T
    ws[z, y, c, :, 2 * lead :] = steps[0:depth].astype(jnp.bfloat16)
    lines = jnp.concatenate(
        [
            jnp.concatenate([ref[w : w + 1, :] * sign for w in range(2)], axis=1)
            for ref, sign in ((offset_ref, 1.0), (speed_ref, -1.0))
        ],
        axis=0,
    )
    lines = jnp.concatenate([lines, jnp.zeros((2, 128 - 2 * heads), jnp.float32)], axis=1)
    heads_ref[...] = jnp.concatenate([lines, jnp.zeros((126, 128), jnp.float32)], axis=0).T[
        0 : 2 * heads
    ]
    pl.semaphore_wait(barrier, 7)

    wo_x = Ring(
        wire,
        "x",
        x,
        lambda at: wo.at[z, y, c, at],
        lambda at: wo.at[z, y, c, at, pl.ds(0, 32)],
        lambda at: wo.at[z, y, c, at, pl.ds(32, 32)],
    )
    wo_x.start()

    low, high = pl.ds(0, middle), pl.ds(middle, middle)
    up, down = {"x": step(x, 1)}, {"x": step(x, 3)}
    up_low = wire.go(tokens.at[x, low], up)
    down_high = wire.go(tokens.at[x, high], down)

    def first(buffer, axis, keep=()):
        def at(n, part):
            spot = (z, n, c) if axis == "y" else (n, y, c)
            if keep:
                start, size = keep
                return buffer.at[(*spot, pl.ds(start, size) if part is None else start + part)]
            return buffer.at[spot] if part is None else buffer.at[(*spot, pl.ds(32 * part, 32))]

        here = y if axis == "y" else z
        return Ring(
            wire, axis, here, lambda n: at(n, None), lambda n: at(n, 0), lambda n: at(n, 1)
        )

    def group(buffer, axis, n, part, keep):
        some = pl.ds(0, 4) if part is None else pl.ds(2 * part, 2)
        spot = (n, some, c) if axis == "z" else (some, n, c)
        return buffer.at[(*spot, pl.ds(*keep))] if keep else buffer.at[spot]

    def second(buffer, axis, keep=()):
        here = y if axis == "y" else z
        return Ring(
            wire,
            axis,
            here,
            lambda n: group(buffer, axis, n, None, keep),
            lambda n: group(buffer, axis, n, 0, keep),
            lambda n: group(buffer, axis, n, 1, keep),
        )

    pairs = {}

    def across(name, buffer, axis, by, keep=()):
        here = y if axis == "y" else z
        copy = wire.go(group(buffer, axis, step(here, by), None, keep), partner)
        pairs.setdefault(name, []).append(copy)

    v_first, s_first = first(wv, "y"), first(ws, "z")
    v_first.start()
    s_first.start()

    def main_row(shard):
        return HALO + shard * rows

    def normalize(ref, size, to):
        width = ref.shape[-1]

        @pl.loop(0, size // 16)
        def _(k):
            taken = pl.ds(pl.multiple_of(k * 16, 16), 16)
            cells = ref[taken, :].astype(jnp.float32)
            total = cells[:, 0:128] * cells[:, 0:128]
            for at in range(128, width, 128):
                total = total + cells[:, at : at + 128] * cells[:, at : at + 128]
            squares[taken, :] = total

        level = lax.rsqrt(
            jnp.sum(squares[0:size, :], axis=-1, keepdims=True) * (1.0 / width) + EPSILON
        )
        squares[0:size, :] = jnp.broadcast_to(level, (size, 128))

        @pl.loop(0, size // 16)
        def _(k):
            taken = pl.ds(pl.multiple_of(k * 16, 16), 16)
            scale = squares[taken, :]
            cells = ref[taken, :].astype(jnp.float32)
            placed = pl.ds(pl.multiple_of(to + k * 16, 16), 16)
            for at in range(0, width, 128):
                normed[placed, at : at + 128] = (
                    cells[:, at : at + 128] * scale * norm_gain_ref[:, at : at + 128]
                ).astype(jnp.bfloat16)

    shard_in = (x, step(x, 3), step(x, 1), step(x, 2))

    def project(slots, parts):
        edge = not slots
        begin, size = (slots[0] * rows, len(slots) * rows) if slots else (4 * rows, 2 * HALO)
        taken = pl.ds(begin, size)

        def put(values, columns):
            for k, slot in enumerate(slots):
                placed = pl.ds(pl.multiple_of(main_row(shard_in[slot]), 16), rows)
                projected[placed, columns] = values[k * rows : (k + 1) * rows]
            if edge:
                projected[0:HALO, columns] = jnp.where(me > 0, values[0:HALO], 0).astype(
                    values.dtype
                )
                projected[main_row(4) : main_row(4) + HALO, columns] = jnp.where(
                    me < 31, values[HALO:], 0
                ).astype(values.dtype)

        def product(weights, columns):
            return dot(normed[taken, :], weights[:, :, :, :, columns].reshape(-1, 256)).astype(
                jnp.bfloat16
            )

        if VALUE in parts:

            @pl.loop(0, half // 256)
            def _(k):
                columns = pl.ds(pl.multiple_of(k * 256, 256), 256)
                put(product(wv, columns), columns)

        if INWARD in parts:
            put(product(ws, slice(0, lead)), slice(half, half + lead))
        if OUTWARD in parts:
            put(product(ws, slice(lead, 2 * lead)), slice(half + lead, wide))
        if STEPS in parts:
            values = dot(normed[taken, :], ws[:, :, :, :, 2 * lead :].reshape(-1, 128)).astype(
                jnp.bfloat16
            )
            for k, slot in enumerate(slots):
                placed = pl.ds(pl.multiple_of(shard_in[slot] * rows, rows), rows)
                raw[placed, :] = values[k * rows : (k + 1) * rows]

    def project_gate(slots):
        taken = pl.ds(slots[0] * rows, len(slots) * rows)

        @pl.loop(0, half // 256)
        def _(k):
            columns = pl.ds(pl.multiple_of(k * 256, 256), 256)
            values = dot(normed[taken, :], wg[:, :, :, :, columns].reshape(-1, 256))
            values = silu(values.astype(jnp.bfloat16).astype(jnp.float32)).astype(jnp.bfloat16)
            for k, slot in enumerate(slots):
                placed = pl.ds(pl.multiple_of(shard_in[slot] * rows, rows), rows)
                gates[placed, columns] = values[k * rows : (k + 1) * rows]

    normalize(tokens.at[x], rows, 0)

    v_first.forward()
    wo_x.forward()
    up_high = wire.go(tokens.at[x, high], up)
    down_low = wire.go(tokens.at[x, low], down)
    s_first.forward()
    v_first.finish()
    v_second = second(wv, "z")
    v_second.start()
    across("v", wv, "z", 0)
    s_first.finish()
    s_second = second(ws, "y")
    s_second.start()
    across("s", ws, "y", 0)
    g_first = first(wg, "z")
    g_first.start()

    up_low.wait_recv()
    down_high.wait_recv()
    far = [
        wire.go(tokens.at[step(x, by), pl.ds(*some)], to)
        for by, some, to in (
            (3, (0, HALO), up),
            (1, (rows - HALO, HALO), down),
            (3, (HALO, middle - HALO), up),
            (1, (middle, middle - HALO), down),
        )
    ]
    wo_x.finish()
    lo_first, hi_first = first(wo, "y", (0, 2)), first(wo, "z", (2, 2))
    lo_first.start()
    hi_first.start()
    normalize(tokens.at[step(x, 3), low], middle, rows)
    normalize(tokens.at[step(x, 1), high], middle, 2 * rows + middle)

    v_second.forward()
    s_second.forward()
    for by in (3, 1):
        across("v", wv, "z", by)
        across("s", ws, "y", by)
    g_first.forward()
    v_second.finish()
    across("v", wv, "z", 2)
    s_second.finish()
    across("s", ws, "y", 2)
    g_first.finish()
    g_second = second(wg, "y")
    g_second.start()
    across("g", wg, "y", 0)
    lo_first.forward()
    hi_first.forward()
    for copy in pairs["v"] + pairs["s"]:
        copy.wait_recv()
    project((0,), (VALUE, INWARD, OUTWARD, STEPS))

    up_high.wait_recv()
    down_low.wait_recv()
    normalize(tokens.at[step(x, 3), high], middle, rows + middle)
    normalize(tokens.at[step(x, 1), low], middle, 2 * rows)
    far[0].wait_recv()
    far[1].wait_recv()
    edge_in = [
        wire.go(
            tokens.at[shard, pl.ds(offset, HALO)],
            stretch_at(z, y, c, by),
            edges.at[pl.ds(slot * HALO, HALO)],
        )
        for slot, (shard, offset, by) in enumerate(((3, rows - HALO, 1), (0, 0, 31)))
    ]
    lo_first.finish()
    lo_second = second(wo, "z", (0, 2))
    lo_second.start()
    across("o", wo, "z", 0, (0, 2))
    hi_first.finish()
    hi_second = second(wo, "y", (2, 2))
    hi_second.start()
    across("o", wo, "y", 0, (2, 2))
    project((1, 2), (VALUE, INWARD, OUTWARD, STEPS))
    g_second.forward()
    across("g", wg, "y", 3)
    across("g", wg, "y", 1)
    for copy in edge_in:
        copy.wait_recv()
    normalize(edges, 2 * HALO, 4 * rows)
    project((), (VALUE, INWARD, OUTWARD))

    row, col = iota((BLOCK, BLOCK), 0), iota((BLOCK, BLOCK), 1)
    lower = row >= col
    triangle = jnp.where(row <= col, 1.0, 0.0)

    def spread(kind):
        place_of = iota((128, wide), 1) // HEAD_DIM + 2 * heads * kind
        return jnp.where(place_of == iota((128, wide), 0), 1.0, 0.0)

    spread_weight = spread(2).astype(jnp.bfloat16)

    def rows_of(k):
        return pl.ds(pl.multiple_of(k * BLOCK, BLOCK), BLOCK)

    def filtered(k, begin, end):
        window = pl.ds(pl.multiple_of(k * BLOCK, BLOCK), BLOCK + 2 * HALO)
        for at in range(begin, end, 128):
            if at < half:
                tap_ref, target, start = tap_value_ref, signal, at
            elif at < half + lead:
                tap_ref, target, start = tap_in_ref, inward, at - half
            else:
                tap_ref, target, start = tap_out_ref, outward, at - half - lead
            cells = projected[window, at : at + 128].astype(jnp.float32)
            tap = tap_ref[:, start : start + 128]
            here = slice(HALO, HALO + BLOCK)
            total = (
                tap[0:1] * pltpu.roll(cells, 1, 0)[here]
                + tap[1:2] * cells[here]
                + tap[2:3] * pltpu.roll(cells, BLOCK + 2 * HALO - 1, 0)[here]
            )
            target[rows_of(k), start : start + 128] = silu(total).astype(jnp.bfloat16)

    def prepare(first_block):
        some = [lax.rem(first_block + n, blocks) for n in range(4)]
        both = 2 * heads
        forward_row = lax.rem(iota((4 * both, BLOCK), 0), both) < heads
        size = jax.nn.softplus(
            jnp.concatenate(
                [raw[rows_of(k), :].astype(jnp.float32).T[0:both] for k in some], axis=0
            )
            + jnp.concatenate([heads_ref[:, 0:1]] * 4, axis=0)
            - shift
        )
        logs = size * jnp.concatenate([heads_ref[:, 1:2]] * 4, axis=0)
        through = dot(logs, triangle, lax.Precision.HIGHEST)
        until = through - logs
        whole = through[:, BLOCK - 1 : BLOCK]
        logsize = jnp.log(size)
        lines = jnp.where(forward_row, logsize - through, logsize + until) * LOG2E
        kinds = (
            jnp.where(forward_row, through, -until) * LOG2E,
            jnp.exp(jnp.where(forward_row, through, whole - until)),
            size * jnp.exp(jnp.where(forward_row, whole - through, until)),
            jnp.broadcast_to(jnp.exp(whole), (4 * both, BLOCK)),
        )
        turned = []
        for n, k in enumerate(some):
            own_rows = slice(n * both, (n + 1) * both)
            rowwise[k, 0:both, :] = lines[own_rows]
            rowwise[k, both : both + heads, :] = (
                size[n * both : n * both + heads] + size[n * both + heads : (n + 1) * both]
            )
            block = jnp.concatenate(
                [kind[own_rows] for kind in kinds]
                + [jnp.zeros((128 - 4 * both, BLOCK), jnp.float32)],
                axis=0,
            ).T
            column[rows_of(k), :] = block
            fades[k] = block[0:8]
            turned.append(block.astype(jnp.bfloat16))
        turned = jnp.concatenate(turned, axis=0)
        for g in range(groups):
            across_in = [
                inward[rows_of(k), g * STATE : (g + 1) * STATE].astype(jnp.float32).T.astype(
                    jnp.bfloat16
                )
                for k in some
            ]
            cells = jnp.concatenate(
                [signal[rows_of(k), g * span : (g + 1) * span] for k in some], axis=0
            )
            for way in range(2):
                placed = slice(way * half + g * span, way * half + (g + 1) * span)
                content = (
                    cells.astype(jnp.float32) * dot(turned, spread_weight[:, placed])
                ).astype(jnp.bfloat16)
                for n, k in enumerate(some):
                    states[k, :, placed] = dot(
                        across_in[n], content[n * BLOCK : (n + 1) * BLOCK]
                    )

    away = 2 * step(x, 2)

    @pl.loop(0, 4)
    def _(k):
        filtered(lax.rem(away + 3 + k, blocks), 0, wide)

    prepare(away + 3)

    far[2].wait_recv()
    far[3].wait_recv()
    normalize(tokens.at[step(x, 2)], rows, 3 * rows)
    project((3,), (VALUE, INWARD, STEPS))

    @pl.loop(0, 4)
    def _(k):
        filtered(lax.rem(away + 7 + k, blocks), 0, half + lead)

    prepare(away + 7)

    over = dot(
        jnp.concatenate([fades[k, 0:1, :] for k in range(blocks)], axis=0),
        spread(3),
        lax.Precision.HIGHEST,
    )
    for k in range(blocks):
        decays[k] = jnp.broadcast_to(over[k : k + 1], (8, wide))

    @pl.loop(0, wide // 128)
    def _(j):
        lanes = pl.ds(pl.multiple_of(j * 128, 128), 128)
        backward = j >= half // 128
        total = jnp.zeros((STATE, 128), jnp.float32)
        decay = jnp.ones((1, 128), jnp.float32)
        for k in range(blocks):
            at = jnp.where(backward, blocks - 1 - k, k)
            part = decays[at, 0:1, lanes]
            total = total * part + states[at, :, lanes]
            decay = decay * part
        upper = decay.astype(jnp.bfloat16).astype(jnp.float32)
        centre = (decay - upper).astype(jnp.bfloat16).astype(jnp.float32)
        rest = decay - upper - centre
        place_row = iota((16, 128), 0)
        tail = jnp.where(place_row == 0, upper, jnp.where(place_row == 1, centre, rest))
        for q in range(4):
            totals[4 * j + q, 0:32, :] = total[32 * q : 32 * q + 32].astype(jnp.bfloat16)
            totals[4 * j + q, 32:48, :] = tail.astype(jnp.bfloat16)

    def outgoing(box, inbox, bank, k):
        to = lax.rem(me + k, 32)
        return pltpu.make_async_remote_copy(
            src_ref=box.at[to],
            dst_ref=inbox.at[me],
            send_sem=state_send.at[bank, k],
            recv_sem=state_recv.at[bank, me],
            device_id=stretch(to),
            device_id_type=MESH,
        )

    def expected(box, inbox, bank, k):
        source = lax.rem(me + k, 32)
        return pltpu.make_async_remote_copy(
            src_ref=box.at[me],
            dst_ref=inbox.at[source],
            send_sem=state_send.at[bank, k],
            recv_sem=state_recv.at[bank, source],
            device_id=stretch(source),
            device_id_type=MESH,
        )

    @pl.loop(1, 32)
    def _(k):
        outgoing(totals, arrived, 0, k).start()

    arrived[me] = totals[me]

    g_second.finish()
    across("g", wg, "y", 2)

    def within(k):
        for g in range(groups):
            inner_product = dot_nt(
                outward[rows_of(k), g * STATE : (g + 1) * STATE],
                inward[rows_of(k), g * STATE : (g + 1) * STATE],
            )
            cells = signal[rows_of(k), g * span : (g + 1) * span]
            head_of = iota((BLOCK, span), 1) // HEAD_DIM
            weights, content = [], []
            for r in range(ratio):
                h = g * ratio + r
                below = column[rows_of(k), h : h + 1] + rowwise[k, h : h + 1, :]
                above = (
                    column[rows_of(k), heads + h : heads + h + 1]
                    + rowwise[k, heads + h : heads + h + 1, :]
                )
                decay = jnp.exp2(jnp.where(lower, below, above))
                both = jnp.where(
                    row == col, rowwise[k, 2 * heads + h : 2 * heads + h + 1, :], decay
                )
                weights.append((inner_product * both).astype(jnp.bfloat16))
                content.append(jnp.where(head_of == r, cells, jnp.zeros_like(cells)))
            inner[rows_of(k), g * span : (g + 1) * span] = dot(
                jnp.concatenate(weights, axis=1), jnp.concatenate(content, axis=0)
            )

    lo_second.forward()
    hi_second.forward()
    for by in (3, 1):
        across("o", wo, "z", by, (0, 2))
        across("o", wo, "y", by, (2, 2))

    project((3,), (OUTWARD,))

    @pl.loop(0, 4)
    def _(k):
        filtered(lax.rem(away + 7 + k, blocks), half + lead, wide)

    for copy in pairs["g"]:
        copy.wait_recv()
    project_gate((0, 1, 2))
    project_gate((3,))

    @pl.loop(0, blocks // 2)
    def _(k):
        within(k)

    @pl.loop(1, 32)
    def _(k):
        expected(totals, arrived, 0, k).wait_recv()

    flip = me >= 16

    def hop(k, state):
        at = jnp.where(flip, 31 - k, k)
        onward[at] = state.astype(jnp.bfloat16)
        message = arrived[at].astype(jnp.float32)
        decay = message[32:33] + message[33:34] + message[34:35]
        return state * decay + message[0:32]

    lax.fori_loop(0, 32, hop, jnp.zeros((32, 128), jnp.float32))

    @pl.loop(1, 32)
    def _(k):
        outgoing(onward, incoming, 1, k).start()

    incoming[me] = onward[me]

    @pl.loop(blocks // 2, blocks)
    def _(k):
        within(k)

    @pl.loop(1, 32)
    def _(k):
        expected(onward, incoming, 1, k).wait_recv()

    @pl.loop(0, wide // 128)
    def _(j):
        lanes = pl.ds(pl.multiple_of(j * 128, 128), 128)
        backward = j >= half // 128
        state = jnp.concatenate([incoming[4 * j + q] for q in range(4)], axis=0).astype(jnp.float32)
        for k in range(blocks):
            at = jnp.where(backward, blocks - 1 - k, k)
            before[at, :, lanes] = state.astype(jnp.bfloat16)
            state = state * decays[at, 0:1, lanes] + states[at, :, lanes]

    spread_read = spread(1).astype(jnp.bfloat16)

    def finish(k):
        scale = dot(column[rows_of(k), :].astype(jnp.bfloat16), spread_read)
        for g in range(groups):
            lanes = slice(g * span, (g + 1) * span)
            read = outward[rows_of(k), g * STATE : (g + 1) * STATE]
            total = inner[rows_of(k), lanes]
            for way in range(2):
                placed = slice(way * half + g * span, way * half + (g + 1) * span)
                total = total + dot(read, before[k, :, placed]) * scale[:, placed]
            gated = total * gates[rows_of(k), lanes].astype(jnp.float32)
            level = lax.rsqrt(jnp.mean(gated * gated, axis=-1, keepdims=True) + EPSILON)
            mixed[rows_of(k), lanes] = (gated * level * gain_ref[:, lanes]).astype(jnp.bfloat16)

    def finish_shard(shard):
        @pl.loop(0, 2)
        def _(b):
            finish(2 * shard + b)

    def part(shard, some):
        start, size = some
        return mixed.at[pl.ds(pl.multiple_of(shard * rows + start, middle), size)]

    finish_shard(step(x, 2))
    relay_up = wire.go(part(step(x, 2), (0, middle)), up, relay.at[0])
    relay_down = wire.go(part(step(x, 2), (middle, middle)), down, relay.at[1])
    finish_shard(step(x, 1))
    near_up = wire.go(part(step(x, 1), (0, rows)), up, shards.at[x])
    finish_shard(step(x, 3))
    near_down = wire.go(part(step(x, 3), (0, rows)), down, shards.at[x])
    lo_second.finish()
    across("o", wo, "z", 2, (0, 2))
    hi_second.finish()
    across("o", wo, "y", 2, (2, 2))
    finish_shard(x)
    shards[x] = mixed[pl.ds(pl.multiple_of(x * rows, rows), rows), :]
    relay_up.wait_recv()
    far_up = wire.go(relay.at[0], up, shards.at[step(x, 3), low])
    relay_down.wait_recv()
    far_down = wire.go(relay.at[1], down, shards.at[step(x, 1), high])
    for copy in pairs["o"]:
        copy.wait_recv()

    def leaving(k):
        lines = pl.ds(pl.multiple_of(k * 512, 512), 512)
        return pltpu.make_async_copy(out_ref.at[:, lines], out_hbm.at[:, lines], local_sem.at[k])

    def contribute(at, begin, end):
        @pl.loop(0, 4)
        def _(k):
            lines = pl.ds(pl.multiple_of(k * 512, 512), 512)
            total = dot_nt(wo[k, :, :, at].reshape(512, -1), shards[at])
            if not begin:
                total = total + summed[lines, :]
            if end:
                out_ref[:, lines] = total.T.astype(out_ref.dtype)
                leaving(k).start()
            else:
                summed[lines, :] = total

    contribute(x, True, False)
    near_up.wait_recv()
    contribute(step(x, 3), False, False)
    near_down.wait_recv()
    contribute(step(x, 1), False, False)
    far_up.wait_recv()
    far_down.wait_recv()
    contribute(step(x, 2), False, True)

    wire.drain()

    @pl.loop(1, 32)
    def _(k):
        outgoing(totals, arrived, 0, k).wait_send()
        outgoing(onward, incoming, 1, k).wait_send()

    @pl.loop(0, 4)
    def _(k):
        leaving(k).wait()


COPIES = 80


def mix(
    tokens,
    norm_gain,
    w_gate,
    w_value,
    w_state_in,
    w_state_out,
    w_step_forward,
    w_step_backward,
    step_offset,
    fading_speed,
    conv_value,
    conv_state_in,
    conv_state_out,
    out_gain,
    w_out,
):
    rows, width = tokens.shape
    depth, half = w_value.shape
    states = w_state_in.shape[1]
    blocks = 4 * rows // BLOCK
    anywhere = pl.BlockSpec(memory_space=pl.ANY)
    bf16, f32 = jnp.bfloat16, jnp.float32
    return pl.pallas_call(
        functools.partial(mixer_kernel, math.log(4 * rows * lax.axis_size(SP))),
        out_shape=jax.ShapeDtypeStruct((rows, width), OUT_TYPE),
        in_specs=[anywhere] * 15,
        out_specs=pl.BlockSpec(memory_space=pltpu.HBM),
        scratch_shapes=[
            pltpu.VMEM((1, width), f32),
            pltpu.VMEM(w_step_forward.shape[::-1], bf16),
            pltpu.VMEM(w_step_backward.shape[::-1], bf16),
            pltpu.VMEM(conv_value.shape, f32),
            pltpu.VMEM(conv_state_in.shape, f32),
            pltpu.VMEM(conv_state_out.shape, f32),
            pltpu.VMEM(step_offset.shape, f32),
            pltpu.VMEM(fading_speed.shape, f32),
            pltpu.VMEM((1, half), f32),
            pltpu.VMEM((16, 128), f32),
            pltpu.VMEM((rows, 128), f32),
            pltpu.VMEM((blocks, 8, 128), f32),
            pltpu.VMEM((rows, width), OUT_TYPE),
            pltpu.VMEM((4, rows, width), bf16),
            pltpu.VMEM((2 * HALO, width), bf16),
            pltpu.VMEM((4 * rows + 2 * HALO, width), bf16),
            pltpu.VMEM((4, 4, 2, depth, half), bf16),
            pltpu.VMEM((4, 4, 2, depth, 2 * states + 128), bf16),
            pltpu.VMEM((4, 4, 2, depth, half), bf16),
            pltpu.VMEM((4, 4, 2, 4, depth, half), bf16),
            pltpu.VMEM((4 * rows + 2 * HALO, 2 * half), bf16),
            pltpu.VMEM((4 * rows, half), bf16),
            pltpu.VMEM((4 * rows, 128), bf16),
            pltpu.VMEM((4 * rows, half), bf16),
            pltpu.VMEM((4 * rows, states), bf16),
            pltpu.VMEM((4 * rows, states), bf16),
            pltpu.VMEM((4 * rows, 128), f32),
            pltpu.VMEM((blocks, 24, 128), f32),
            pltpu.VMEM((blocks, STATE, 2 * half), f32),
            pltpu.VMEM((blocks, 8, 2 * half), f32),
            pltpu.VMEM((blocks, STATE, 2 * half), bf16),
            pltpu.VMEM((4 * rows, half), f32),
            pltpu.VMEM((32, 48, 128), bf16),
            pltpu.VMEM((32, 48, 128), bf16),
            pltpu.VMEM((32, 32, 128), bf16),
            pltpu.VMEM((32, 32, 128), bf16),
            pltpu.VMEM((4 * rows, half), bf16),
            pltpu.VMEM((4, rows, half), bf16),
            pltpu.VMEM((2, rows // 2, half), bf16),
            pltpu.VMEM((width, rows), f32),
            pltpu.SemaphoreType.DMA((COPIES,)),
            pltpu.SemaphoreType.DMA((COPIES,)),
            pltpu.SemaphoreType.DMA((2, 32)),
            pltpu.SemaphoreType.DMA((2, 32)),
            pltpu.SemaphoreType.DMA((15,)),
        ],
        compiler_params=pltpu.CompilerParams(
            collective_id=0, has_side_effects=True, vmem_limit_bytes=60 * 2**20
        ),
        name="mixer",
    )(
        tokens,
        w_value,
        w_state_in,
        w_state_out,
        w_gate,
        w_out.T,
        norm_gain.reshape(1, -1),
        w_step_forward.T,
        w_step_backward.T,
        conv_value,
        conv_state_in,
        conv_state_out,
        step_offset,
        fading_speed,
        out_gain.reshape(1, -1),
    )


OUT_TYPE = jnp.bfloat16


def local(
    input_activations,
    norm_gain,
    w_gate,
    w_value,
    w_state_in,
    w_state_out,
    w_step_forward,
    w_step_backward,
    step_offset,
    fading_speed,
    conv_value,
    conv_state_in,
    conv_state_out,
    out_gain,
    w_out,
):
    return mix(
        input_activations,
        norm_gain,
        w_gate,
        w_value,
        w_state_in,
        w_state_out,
        w_step_forward,
        w_step_backward,
        step_offset,
        fading_speed,
        conv_value,
        conv_state_in,
        conv_state_out,
        out_gain,
        w_out,
    )


def solution(mesh):
    torus = Mesh(mesh.devices.reshape(4, 4, 2, 4), SP_TP)
    return jax.shard_map(
        local,
        mesh=torus,
        in_specs=(
            P(SP_TP, None),
            P(),
            P(SP, "x"),
            P(SP, "x"),
            P(SP, "x"),
            P(SP, "x"),
            P(SP, "x"),
            P(SP, "x"),
            P(None, "x"),
            P(None, "x"),
            P(None, "x"),
            P(None, "x"),
            P(None, "x"),
            P("x"),
            P("x", SP),
        ),
        out_specs=P(SP_TP, None),
        check_vma=False,
    )
```

```python
import functools
import math

import jax
import jax.numpy as jnp
from jax import lax
from jax.experimental import pallas as pl
from jax.experimental.pallas import tpu as pltpu
from jax.sharding import Mesh
from jax.sharding import PartitionSpec as P

HEAD_DIM = 64
STATE = 128
BLOCK = 128
SP = ("z", "y", "c")
SP_TP = ("z", "y", "c", "x")
EPSILON = 1e-06
MESH = pl.DeviceIdType.MESH
VALUE, INWARD, OUTWARD, STEPS = range(4)
HALO = 16


def place():
    return [lax.axis_index(name) for name in ("z", "y", "c", "x")]


def step(at, by):
    return lax.rem(at + by + 4, 4)


def stretch_at(z, y, c, by):
    n = lax.rem(z * 8 + y * 2 + c + by + 32, 32)
    return {"z": n // 8, "y": lax.rem(n // 2, 4), "c": lax.rem(n, 2)}


class Wire:
    def __init__(self, flags, self_free):
        self.flags, self.count, self.to, self.sent = flags, 0, self_free, []

    def flag(self):
        self.count += 1
        return self.flags.at[self.count - 1]

    def go(self, source, to, send, recv, target=None):
        pltpu.make_async_remote_copy(
            src_ref=source,
            dst_ref=source if target is None else target,
            send_sem=send,
            recv_sem=recv,
            device_id=to,
            device_id_type=MESH,
        ).start()

    def span(self, ref, flag):
        return pltpu.make_async_remote_copy(
            src_ref=ref,
            dst_ref=ref,
            send_sem=flag,
            recv_sem=flag,
            device_id=self.to,
            device_id_type=MESH,
        )

    def landed(self, ref, flag):
        self.span(ref, flag).wait_recv()

    def drain(self):
        for ref, flag in self.sent:
            self.span(ref, flag).wait_send()


class Ring:
    def __init__(self, wire, axis, at, block, low, high, many):
        self.wire, self.at = wire, at
        self.up, self.down = {axis: step(at, 1)}, {axis: step(at, 3)}
        self.block, self.low, self.high, self.many = block, low, high, many
        self.out, self.near, self.away = wire.flag(), wire.flag(), wire.flag()
        wire.sent.append((many(3), self.out))

    def start(self):
        self.wire.go(self.block(self.at), self.up, self.out, self.near)
        self.wire.go(self.block(self.at), self.down, self.out, self.near)

    def forward(self):
        self.wire.landed(self.many(2), self.near)
        self.wire.go(self.low(step(self.at, 3)), self.up, self.out, self.away)
        self.wire.go(self.high(step(self.at, 1)), self.down, self.out, self.away)

    def finish(self):
        self.wire.landed(self.many(1), self.away)


LOG2E = 1.4426950408889634


def dot_nt(a, b):
    return lax.dot_general(a, b, (((1,), (1,)), ((), ())), preferred_element_type=jnp.float32)


def dot_tn(a, b):
    return lax.dot_general(a, b, (((0,), (0,)), ((), ())), preferred_element_type=jnp.float32)


def dot(a, b, precision=None):
    return lax.dot_general(
        a, b, (((1,), (0,)), ((), ())), precision=precision, preferred_element_type=jnp.float32
    )


def iota(shape, dim):
    return lax.broadcasted_iota(jnp.int32, shape, dim)


def silu(v):
    part = 0.5 * v
    return part + part * jnp.tanh(part)


def mixer_kernel(
    shift,
    tokens_hbm,
    value_hbm,
    state_in_hbm,
    state_out_hbm,
    gate_hbm,
    w_out_hbm,
    norm_gain_hbm,
    step_forward_hbm,
    step_backward_hbm,
    tap_value_hbm,
    tap_in_hbm,
    tap_out_hbm,
    offset_hbm,
    speed_hbm,
    gain_hbm,
    out_hbm,
    norm_gain_ref,
    step_forward_ref,
    step_backward_ref,
    tap_value_ref,
    tap_in_ref,
    tap_out_ref,
    offset_ref,
    speed_ref,
    gain_ref,
    heads_ref,
    squares,
    fades,
    out_ref,
    tokens,
    edges,
    normed,
    wv,
    ws,
    wg,
    wo,
    projected,
    gates,
    raw,
    signal,
    inward,
    outward,
    column,
    rowwise,
    states,
    decays,
    before,
    inner,
    totals,
    arrived,
    onward,
    incoming,
    mixed,
    shards,
    relay,
    summed,
    flags,
    local_sem,
):
    z, y, c, x = place()
    me = z * 8 + y * 2 + c
    wire = Wire(flags, {"c": 1 - c})
    rows = tokens.shape[1]
    middle = rows // 2
    count = 4 * rows
    blocks = count // BLOCK
    half = signal.shape[1]
    wide = 2 * half
    groups = inward.shape[1] // STATE
    ratio = half // HEAD_DIM // groups
    heads = groups * ratio
    span = ratio * HEAD_DIM
    lead = inward.shape[1]
    partner = {"c": 1 - c}

    def stretch(n):
        return {"z": n // 8, "y": lax.rem(n // 2, 4), "c": lax.rem(n, 2)}

    own = [
        pltpu.make_async_copy(tokens_hbm, tokens.at[x], local_sem.at[0]),
        pltpu.make_async_copy(value_hbm, wv.at[z, y, c], local_sem.at[1]),
        pltpu.make_async_copy(state_in_hbm, ws.at[z, y, c, :, pl.ds(0, lead)], local_sem.at[2]),
        pltpu.make_async_copy(state_out_hbm, ws.at[z, y, c, :, pl.ds(lead, lead)], local_sem.at[3]),
        pltpu.make_async_copy(gate_hbm, wg.at[z, y, c], local_sem.at[4]),
        pltpu.make_async_copy(w_out_hbm, wo.at[z, y, c, x], local_sem.at[5]),
    ]
    small = (
        (step_forward_hbm, step_forward_ref),
        (step_backward_hbm, step_backward_ref),
        (offset_hbm, offset_ref),
        (speed_hbm, speed_ref),
        (norm_gain_hbm, norm_gain_ref),
        (tap_value_hbm, tap_value_ref),
        (tap_in_hbm, tap_in_ref),
        (tap_out_hbm, tap_out_ref),
        (gain_hbm, gain_ref),
    )
    own += [
        pltpu.make_async_copy(source, target, local_sem.at[6 + k])
        for k, (source, target) in enumerate(small)
    ]
    for copy in own:
        copy.start()
    barrier = pltpu.get_barrier_semaphore()

    near = [{axis: step(at, by)} for axis, at in (("x", x), ("y", y), ("z", z)) for by in (1, 3)]
    for other in near + [partner]:
        pl.semaphore_signal(barrier, inc=1, device_id=other, device_id_type=MESH)
    for copy in own:
        copy.wait()
    depth = step_forward_ref.shape[1]
    steps = jnp.concatenate(
        [
            step_forward_ref[...].astype(jnp.float32),
            step_backward_ref[...].astype(jnp.float32),
            jnp.zeros((128 - 2 * heads, depth), jnp.float32),
        ],
        axis=0,
    )
    steps = jnp.concatenate([steps, jnp.zeros((128, 128 - depth), jnp.float32)], axis=1).T
    ws[z, y, c, :, 2 * lead :] = steps[0:depth].astype(jnp.bfloat16)
    lines = jnp.concatenate(
        [
            jnp.concatenate([ref[w : w + 1, :] * sign for w in range(2)], axis=1)
            for ref, sign in ((offset_ref, 1.0), (speed_ref, -1.0))
        ],
        axis=0,
    )
    lines = jnp.concatenate([lines, jnp.zeros((2, 128 - 2 * heads), jnp.float32)], axis=1)
    heads_ref[...] = jnp.concatenate([lines, jnp.zeros((126, 128), jnp.float32)], axis=0).T[
        0 : 2 * heads
    ]
    pl.semaphore_wait(barrier, 7)

    wo_x = Ring(
        wire,
        "x",
        x,
        lambda at: wo.at[z, y, c, at],
        lambda at: wo.at[z, y, c, at, pl.ds(0, 32)],
        lambda at: wo.at[z, y, c, at, pl.ds(32, 32)],
        lambda n: wo.at[z, y, c, pl.ds(0, n)],
    )
    wo_x.start()

    low, high = pl.ds(0, middle), pl.ds(middle, middle)
    up, down = {"x": step(x, 1)}, {"x": step(x, 3)}
    tokens_out, first_half, second_half = wire.flag(), wire.flag(), wire.flag()
    far_ends, far_rest = wire.flag(), wire.flag()
    wire.sent.append((tokens.at[pl.ds(0, 3)], tokens_out))
    wire.go(tokens.at[x, low], up, tokens_out, first_half)
    wire.go(tokens.at[x, high], down, tokens_out, first_half)

    def first(buffer, axis, keep=()):
        def at(n, part):
            spot = (z, n, c) if axis == "y" else (n, y, c)
            if keep:
                start, size = keep
                return buffer.at[(*spot, pl.ds(start, size) if part is None else start + part)]
            return buffer.at[spot] if part is None else buffer.at[(*spot, pl.ds(32 * part, 32))]

        here = y if axis == "y" else z

        def many(n):
            spot = (z, pl.ds(0, n), c) if axis == "y" else (pl.ds(0, n), y, c)
            return buffer.at[(*spot, pl.ds(*keep))] if keep else buffer.at[spot]

        return Ring(
            wire, axis, here, lambda n: at(n, None), lambda n: at(n, 0), lambda n: at(n, 1), many
        )

    def group(buffer, axis, n, part, keep):
        some = pl.ds(0, 4) if part is None else pl.ds(2 * part, 2)
        spot = (n, some, c) if axis == "z" else (some, n, c)
        return buffer.at[(*spot, pl.ds(*keep))] if keep else buffer.at[spot]

    def second(buffer, axis, keep=()):
        here = y if axis == "y" else z
        return Ring(
            wire,
            axis,
            here,
            lambda n: group(buffer, axis, n, None, keep),
            lambda n: group(buffer, axis, n, 0, keep),
            lambda n: group(buffer, axis, n, 1, keep),
            lambda n: group(buffer, axis, pl.ds(0, n), None, keep),
        )

    pairs = {}
    for name, buffer in (("v", wv), ("s", ws), ("g", wg), ("o", wo)):
        pairs[name] = wire.flag(), wire.flag()
        wire.sent.append((buffer.at[:, :, 1 - c], pairs[name][0]))

    def across(name, buffer, axis, by, keep=()):
        here = y if axis == "y" else z
        wire.go(group(buffer, axis, step(here, by), None, keep), partner, *pairs[name])

    def crossed(name, buffer):
        wire.landed(buffer.at[:, :, 1 - c], pairs[name][1])

    v_first, s_first = first(wv, "y"), first(ws, "z")
    v_first.start()
    s_first.start()

    def main_row(shard):
        return HALO + shard * rows

    def normalize(ref, size, to):
        width = ref.shape[-1]

        @pl.loop(0, size // 16)
        def _(k):
            taken = pl.ds(pl.multiple_of(k * 16, 16), 16)
            cells = ref[taken, :].astype(jnp.float32)
            total = cells[:, 0:128] * cells[:, 0:128]
            for at in range(128, width, 128):
                total = total + cells[:, at : at + 128] * cells[:, at : at + 128]
            squares[taken, :] = total

        level = lax.rsqrt(
            jnp.sum(squares[0:size, :], axis=-1, keepdims=True) * (1.0 / width) + EPSILON
        )
        squares[0:size, :] = jnp.broadcast_to(level, (size, 128))

        @pl.loop(0, size // 16)
        def _(k):
            taken = pl.ds(pl.multiple_of(k * 16, 16), 16)
            scale = squares[taken, :]
            cells = ref[taken, :].astype(jnp.float32)
            placed = pl.ds(pl.multiple_of(to + k * 16, 16), 16)
            for at in range(0, width, 128):
                normed[placed, at : at + 128] = (
                    cells[:, at : at + 128] * scale * norm_gain_ref[:, at : at + 128]
                ).astype(jnp.bfloat16)

    shard_in = (x, step(x, 3), step(x, 1), step(x, 2))

    def project(slots, parts):
        edge = not slots
        begin, size = (slots[0] * rows, len(slots) * rows) if slots else (4 * rows, 2 * HALO)
        taken = pl.ds(begin, size)

        def put(values, columns):
            for k, slot in enumerate(slots):
                placed = pl.ds(pl.multiple_of(main_row(shard_in[slot]), 16), rows)
                projected[placed, columns] = values[k * rows : (k + 1) * rows]
            if edge:
                projected[0:HALO, columns] = jnp.where(me > 0, values[0:HALO], 0).astype(
                    values.dtype
                )
                projected[main_row(4) : main_row(4) + HALO, columns] = jnp.where(
                    me < 31, values[HALO:], 0
                ).astype(values.dtype)

        def product(weights, columns):
            return dot(normed[taken, :], weights[:, :, :, :, columns].reshape(-1, 256)).astype(
                jnp.bfloat16
            )

        if VALUE in parts:

            @pl.loop(0, half // 256)
            def _(k):
                columns = pl.ds(pl.multiple_of(k * 256, 256), 256)
                put(product(wv, columns), columns)

        if INWARD in parts:
            put(product(ws, slice(0, lead)), slice(half, half + lead))
        if OUTWARD in parts:
            put(product(ws, slice(lead, 2 * lead)), slice(half + lead, wide))
        if STEPS in parts:
            values = dot(normed[taken, :], ws[:, :, :, :, 2 * lead :].reshape(-1, 128)).astype(
                jnp.bfloat16
            )
            for k, slot in enumerate(slots):
                placed = pl.ds(pl.multiple_of(shard_in[slot] * rows, rows), rows)
                raw[placed, :] = values[k * rows : (k + 1) * rows]

    def project_gate(slots):
        taken = pl.ds(slots[0] * rows, len(slots) * rows)

        @pl.loop(0, half // 256)
        def _(k):
            columns = pl.ds(pl.multiple_of(k * 256, 256), 256)
            values = dot(normed[taken, :], wg[:, :, :, :, columns].reshape(-1, 256))
            values = silu(values.astype(jnp.bfloat16).astype(jnp.float32)).astype(jnp.bfloat16)
            for k, slot in enumerate(slots):
                placed = pl.ds(pl.multiple_of(shard_in[slot] * rows, rows), rows)
                gates[placed, columns] = values[k * rows : (k + 1) * rows]

    normalize(tokens.at[x], rows, 0)

    v_first.forward()
    wo_x.forward()
    wire.go(tokens.at[x, high], up, tokens_out, second_half)
    wire.go(tokens.at[x, low], down, tokens_out, second_half)
    s_first.forward()
    v_first.finish()
    v_second = second(wv, "z")
    v_second.start()
    across("v", wv, "z", 0)
    s_first.finish()
    s_second = second(ws, "y")
    s_second.start()
    across("s", ws, "y", 0)
    g_first = first(wg, "z")
    g_first.start()

    wire.landed(tokens.at[0], first_half)
    for by, start, to, flag in (
        (3, (0, HALO), up, far_ends),
        (1, (rows - HALO, HALO), down, far_ends),
        (3, (HALO, middle - HALO), up, far_rest),
        (1, (middle, middle - HALO), down, far_rest),
    ):
        wire.go(tokens.at[step(x, by), pl.ds(*start)], to, tokens_out, flag)
    wo_x.finish()
    lo_first, hi_first = first(wo, "y", (0, 2)), first(wo, "z", (2, 2))
    lo_first.start()
    hi_first.start()
    normalize(tokens.at[step(x, 3), low], middle, rows)
    normalize(tokens.at[step(x, 1), high], middle, 2 * rows + middle)

    v_second.forward()
    s_second.forward()
    for by in (3, 1):
        across("v", wv, "z", by)
        across("s", ws, "y", by)
    g_first.forward()
    v_second.finish()
    across("v", wv, "z", 2)
    s_second.finish()
    across("s", ws, "y", 2)
    g_first.finish()
    g_second = second(wg, "y")
    g_second.start()
    across("g", wg, "y", 0)
    lo_first.forward()
    hi_first.forward()
    crossed("v", wv)
    crossed("s", ws)
    project((0,), (VALUE, INWARD, OUTWARD, STEPS))

    wire.landed(tokens.at[0], second_half)
    normalize(tokens.at[step(x, 3), high], middle, rows + middle)
    normalize(tokens.at[step(x, 1), low], middle, 2 * rows)
    wire.landed(edges, far_ends)
    edge_out, edge_in = wire.flag(), wire.flag()
    wire.sent.append((edges, edge_out))
    for slot, (shard, offset, by) in enumerate(((3, rows - HALO, 1), (0, 0, 31))):
        wire.go(
            tokens.at[shard, pl.ds(offset, HALO)],
            stretch_at(z, y, c, by),
            edge_out,
            edge_in,
            edges.at[pl.ds(slot * HALO, HALO)],
        )
    lo_first.finish()
    lo_second = second(wo, "z", (0, 2))
    lo_second.start()
    across("o", wo, "z", 0, (0, 2))
    hi_first.finish()
    hi_second = second(wo, "y", (2, 2))
    hi_second.start()
    across("o", wo, "y", 0, (2, 2))
    project((1, 2), (VALUE, INWARD, OUTWARD, STEPS))
    g_second.forward()
    across("g", wg, "y", 3)
    across("g", wg, "y", 1)
    wire.landed(edges, edge_in)
    normalize(edges, 2 * HALO, 4 * rows)
    project((), (VALUE, INWARD, OUTWARD))

    row, col = iota((BLOCK, BLOCK), 0), iota((BLOCK, BLOCK), 1)
    lower = row >= col
    triangle = jnp.where(row <= col, 1.0, 0.0)

    def spread(kind):
        place_of = iota((128, wide), 1) // HEAD_DIM + 2 * heads * kind
        return jnp.where(place_of == iota((128, wide), 0), 1.0, 0.0)

    spread_weight = spread(2).astype(jnp.bfloat16)

    def rows_of(k):
        return pl.ds(pl.multiple_of(k * BLOCK, BLOCK), BLOCK)

    def filtered(k, begin, end):
        window = pl.ds(pl.multiple_of(k * BLOCK, BLOCK), BLOCK + 2 * HALO)
        for at in range(begin, end, 128):
            if at < half:
                tap_ref, target, start = tap_value_ref, signal, at
            elif at < half + lead:
                tap_ref, target, start = tap_in_ref, inward, at - half
            else:
                tap_ref, target, start = tap_out_ref, outward, at - half - lead
            cells = projected[window, at : at + 128].astype(jnp.float32)
            tap = tap_ref[:, start : start + 128]
            here = slice(HALO, HALO + BLOCK)
            total = (
                tap[0:1] * pltpu.roll(cells, 1, 0)[here]
                + tap[1:2] * cells[here]
                + tap[2:3] * pltpu.roll(cells, BLOCK + 2 * HALO - 1, 0)[here]
            )
            target[rows_of(k), start : start + 128] = silu(total).astype(jnp.bfloat16)

    def prepare(first_block):
        some = [lax.rem(first_block + n, blocks) for n in range(4)]
        both = 2 * heads
        forward_row = lax.rem(iota((4 * both, BLOCK), 0), both) < heads
        size = jax.nn.softplus(
            jnp.concatenate(
                [raw[rows_of(k), :].astype(jnp.float32).T[0:both] for k in some], axis=0
            )
            + jnp.concatenate([heads_ref[:, 0:1]] * 4, axis=0)
            - shift
        )
        logs = size * jnp.concatenate([heads_ref[:, 1:2]] * 4, axis=0)
        through = dot(logs, triangle, lax.Precision.HIGHEST)
        until = through - logs
        whole = through[:, BLOCK - 1 : BLOCK]
        logsize = jnp.log(size)
        lines = jnp.where(forward_row, logsize - through, logsize + until) * LOG2E
        kinds = (
            jnp.where(forward_row, through, -until) * LOG2E,
            jnp.exp(jnp.where(forward_row, through, whole - until)),
            size * jnp.exp(jnp.where(forward_row, whole - through, until)),
            jnp.broadcast_to(jnp.exp(whole), (4 * both, BLOCK)),
        )
        turned = []
        for n, k in enumerate(some):
            own_rows = slice(n * both, (n + 1) * both)
            rowwise[k, 0:both, :] = lines[own_rows]
            rowwise[k, both : both + heads, :] = (
                size[n * both : n * both + heads] + size[n * both + heads : (n + 1) * both]
            )
            block = jnp.concatenate(
                [kind[own_rows] for kind in kinds]
                + [jnp.zeros((128 - 4 * both, BLOCK), jnp.float32)],
                axis=0,
            ).T
            column[rows_of(k), :] = block
            fades[k] = block[0:8]
            turned.append(block.astype(jnp.bfloat16))
        turned = jnp.concatenate(turned, axis=0)
        for g in range(groups):
            across_in = [
                inward[rows_of(k), g * STATE : (g + 1) * STATE].astype(jnp.float32).T.astype(
                    jnp.bfloat16
                )
                for k in some
            ]
            cells = jnp.concatenate(
                [signal[rows_of(k), g * span : (g + 1) * span] for k in some], axis=0
            )
            for way in range(2):
                placed = slice(way * half + g * span, way * half + (g + 1) * span)
                content = (
                    cells.astype(jnp.float32) * dot(turned, spread_weight[:, placed])
                ).astype(jnp.bfloat16)
                for n, k in enumerate(some):
                    states[k, :, placed] = dot(
                        across_in[n], content[n * BLOCK : (n + 1) * BLOCK]
                    )

    away = 2 * step(x, 2)

    @pl.loop(0, 4)
    def _(k):
        filtered(lax.rem(away + 3 + k, blocks), 0, wide)

    prepare(away + 3)

    wire.landed(tokens.at[0, pl.ds(0, rows - 2 * HALO)], far_rest)
    normalize(tokens.at[step(x, 2)], rows, 3 * rows)
    project((3,), (VALUE, INWARD, STEPS))

    @pl.loop(0, 4)
    def _(k):
        filtered(lax.rem(away + 7 + k, blocks), 0, half + lead)

    prepare(away + 7)

    over = dot(
        jnp.concatenate([fades[k, 0:1, :] for k in range(blocks)], axis=0),
        spread(3),
        lax.Precision.HIGHEST,
    )
    for k in range(blocks):
        decays[k] = jnp.broadcast_to(over[k : k + 1], (8, wide))

    @pl.loop(0, wide // 128)
    def _(j):
        lanes = pl.ds(pl.multiple_of(j * 128, 128), 128)
        backward = j >= half // 128
        total = jnp.zeros((STATE, 128), jnp.float32)
        decay = jnp.ones((1, 128), jnp.float32)
        for k in range(blocks):
            at = jnp.where(backward, blocks - 1 - k, k)
            part = decays[at, 0:1, lanes]
            total = total * part + states[at, :, lanes]
            decay = decay * part
        upper = decay.astype(jnp.bfloat16).astype(jnp.float32)
        centre = (decay - upper).astype(jnp.bfloat16).astype(jnp.float32)
        rest = decay - upper - centre
        place_row = iota((16, 128), 0)
        tail = jnp.where(place_row == 0, upper, jnp.where(place_row == 1, centre, rest))
        for q in range(4):
            totals[4 * j + q, 0:32, :] = total[32 * q : 32 * q + 32].astype(jnp.bfloat16)
            totals[4 * j + q, 32:48, :] = tail.astype(jnp.bfloat16)

    state_flags = [wire.flag() for _ in range(4)]
    wire.sent.append((totals.at[pl.ds(0, 31)], state_flags[0]))
    wire.sent.append((onward.at[pl.ds(0, 31)], state_flags[2]))

    def disperse(box, inbox, send, recv):
        @pl.loop(0, 31)
        def _(k):
            to = lax.rem(me + lax.rem(k + 15, 31) + 1, 32)
            wire.go(box.at[to], stretch(to), send, recv, inbox.at[me])

    disperse(totals, arrived, *state_flags[:2])

    arrived[me] = totals[me]

    g_second.finish()
    across("g", wg, "y", 2)

    def within(k):
        for g in range(groups):
            inner_product = dot_nt(
                outward[rows_of(k), g * STATE : (g + 1) * STATE],
                inward[rows_of(k), g * STATE : (g + 1) * STATE],
            )
            cells = signal[rows_of(k), g * span : (g + 1) * span]
            head_of = iota((BLOCK, span), 1) // HEAD_DIM
            weights, content = [], []
            for r in range(ratio):
                h = g * ratio + r
                below = column[rows_of(k), h : h + 1] + rowwise[k, h : h + 1, :]
                above = (
                    column[rows_of(k), heads + h : heads + h + 1]
                    + rowwise[k, heads + h : heads + h + 1, :]
                )
                decay = jnp.exp2(jnp.where(lower, below, above))
                both = jnp.where(
                    row == col, rowwise[k, 2 * heads + h : 2 * heads + h + 1, :], decay
                )
                weights.append((inner_product * both).astype(jnp.bfloat16))
                content.append(jnp.where(head_of == r, cells, jnp.zeros_like(cells)))
            inner[rows_of(k), g * span : (g + 1) * span] = dot(
                jnp.concatenate(weights, axis=1), jnp.concatenate(content, axis=0)
            )

    lo_second.forward()
    hi_second.forward()
    for by in (3, 1):
        across("o", wo, "z", by, (0, 2))
        across("o", wo, "y", by, (2, 2))

    project((3,), (OUTWARD,))

    @pl.loop(0, 4)
    def _(k):
        filtered(lax.rem(away + 7 + k, blocks), half + lead, wide)


    @pl.loop(0, blocks // 2)
    def _(k):
        within(k)

    wire.landed(arrived.at[pl.ds(0, 31)], state_flags[1])

    flip = me >= 16

    def hop(k, state):
        at = jnp.where(flip, 31 - k, k)
        onward[at] = state.astype(jnp.bfloat16)
        message = arrived[at].astype(jnp.float32)
        decay = message[32:33] + message[33:34] + message[34:35]
        return state * decay + message[0:32]

    lax.fori_loop(0, 32, hop, jnp.zeros((32, 128), jnp.float32))

    disperse(onward, incoming, *state_flags[2:])

    incoming[me] = onward[me]

    crossed("g", wg)
    project_gate((0, 1, 2))
    project_gate((3,))

    @pl.loop(blocks // 2, blocks)
    def _(k):
        within(k)

    wire.landed(incoming.at[pl.ds(0, 31)], state_flags[3])

    @pl.loop(0, wide // 128)
    def _(j):
        lanes = pl.ds(pl.multiple_of(j * 128, 128), 128)
        backward = j >= half // 128
        state = jnp.concatenate([incoming[4 * j + q] for q in range(4)], axis=0).astype(jnp.float32)
        for k in range(blocks):
            at = jnp.where(backward, blocks - 1 - k, k)
            before[at, :, lanes] = state.astype(jnp.bfloat16)
            state = state * decays[at, 0:1, lanes] + states[at, :, lanes]

    spread_read = spread(1).astype(jnp.bfloat16)

    def finish(k):
        scale = dot(column[rows_of(k), :].astype(jnp.bfloat16), spread_read)
        for g in range(groups):
            lanes = slice(g * span, (g + 1) * span)
            read = outward[rows_of(k), g * STATE : (g + 1) * STATE]
            total = inner[rows_of(k), lanes]
            for way in range(2):
                placed = slice(way * half + g * span, way * half + (g + 1) * span)
                total = total + dot(read, before[k, :, placed]) * scale[:, placed]
            gated = total * gates[rows_of(k), lanes].astype(jnp.float32)
            level = lax.rsqrt(jnp.mean(gated * gated, axis=-1, keepdims=True) + EPSILON)
            mixed[rows_of(k), lanes] = (gated * level * gain_ref[:, lanes]).astype(jnp.bfloat16)

    def finish_shard(shard):
        @pl.loop(0, 2)
        def _(b):
            finish(2 * shard + b)

    def part(shard, some):
        start, size = some
        return mixed.at[pl.ds(pl.multiple_of(shard * rows + start, middle), size)]

    mixed_out, relayed, from_below, from_above, from_far = [wire.flag() for _ in range(5)]
    wire.sent.append((shards, mixed_out))
    finish(2 * step(x, 2))
    wire.go(part(step(x, 2), (0, middle)), up, mixed_out, relayed, relay.at[0])
    finish(2 * step(x, 2) + 1)
    wire.go(part(step(x, 2), (middle, middle)), down, mixed_out, relayed, relay.at[1])
    finish_shard(step(x, 1))
    wire.go(part(step(x, 1), (0, rows)), up, mixed_out, from_below, shards.at[x])
    finish_shard(step(x, 3))
    wire.go(part(step(x, 3), (0, rows)), down, mixed_out, from_above, shards.at[x])
    lo_second.finish()
    across("o", wo, "z", 2, (0, 2))
    hi_second.finish()
    across("o", wo, "y", 2, (2, 2))
    finish_shard(x)
    shards[x] = mixed[pl.ds(pl.multiple_of(x * rows, rows), rows), :]
    wire.landed(relay, relayed)
    wire.go(relay.at[0], up, mixed_out, from_far, shards.at[step(x, 3), low])
    wire.go(relay.at[1], down, mixed_out, from_far, shards.at[step(x, 1), high])
    crossed("o", wo)

    def leaving(k):
        lines = pl.ds(pl.multiple_of(k * 512, 512), 512)
        return pltpu.make_async_copy(out_ref.at[:, lines], out_hbm.at[:, lines], local_sem.at[k])

    def contribute(at, begin, end):
        @pl.loop(0, 4)
        def _(k):
            lines = pl.ds(pl.multiple_of(k * 512, 512), 512)
            total = dot_nt(wo[k, :, :, at].reshape(512, -1), shards[at])
            if not begin:
                total = total + summed[lines, :]
            if end:
                out_ref[:, lines] = total.T.astype(out_ref.dtype)
                leaving(k).start()
            else:
                summed[lines, :] = total

    contribute(x, True, False)
    wire.landed(shards.at[0], from_below)
    contribute(step(x, 3), False, False)
    wire.landed(shards.at[0], from_above)
    contribute(step(x, 1), False, False)
    wire.landed(shards.at[0], from_far)
    contribute(step(x, 2), False, True)

    wire.drain()

    @pl.loop(0, 4)
    def _(k):
        leaving(k).wait()


FLAGS = 57


def mix(
    tokens,
    norm_gain,
    w_gate,
    w_value,
    w_state_in,
    w_state_out,
    w_step_forward,
    w_step_backward,
    step_offset,
    fading_speed,
    conv_value,
    conv_state_in,
    conv_state_out,
    out_gain,
    w_out,
):
    rows, width = tokens.shape
    depth, half = w_value.shape
    states = w_state_in.shape[1]
    blocks = 4 * rows // BLOCK
    anywhere = pl.BlockSpec(memory_space=pl.ANY)
    bf16, f32 = jnp.bfloat16, jnp.float32
    return pl.pallas_call(
        functools.partial(mixer_kernel, math.log(4 * rows * lax.axis_size(SP))),
        out_shape=jax.ShapeDtypeStruct((rows, width), OUT_TYPE),
        in_specs=[anywhere] * 15,
        out_specs=pl.BlockSpec(memory_space=pltpu.HBM),
        scratch_shapes=[
            pltpu.VMEM((1, width), f32),
            pltpu.VMEM(w_step_forward.shape[::-1], bf16),
            pltpu.VMEM(w_step_backward.shape[::-1], bf16),
            pltpu.VMEM(conv_value.shape, f32),
            pltpu.VMEM(conv_state_in.shape, f32),
            pltpu.VMEM(conv_state_out.shape, f32),
            pltpu.VMEM(step_offset.shape, f32),
            pltpu.VMEM(fading_speed.shape, f32),
            pltpu.VMEM((1, half), f32),
            pltpu.VMEM((16, 128), f32),
            pltpu.VMEM((rows, 128), f32),
            pltpu.VMEM((blocks, 8, 128), f32),
            pltpu.VMEM((rows, width), OUT_TYPE),
            pltpu.VMEM((4, rows, width), bf16),
            pltpu.VMEM((2 * HALO, width), bf16),
            pltpu.VMEM((4 * rows + 2 * HALO, width), bf16),
            pltpu.VMEM((4, 4, 2, depth, half), bf16),
            pltpu.VMEM((4, 4, 2, depth, 2 * states + 128), bf16),
            pltpu.VMEM((4, 4, 2, depth, half), bf16),
            pltpu.VMEM((4, 4, 2, 4, depth, half), bf16),
            pltpu.VMEM((4 * rows + 2 * HALO, 2 * half), bf16),
            pltpu.VMEM((4 * rows, half), bf16),
            pltpu.VMEM((4 * rows, 128), bf16),
            pltpu.VMEM((4 * rows, half), bf16),
            pltpu.VMEM((4 * rows, states), bf16),
            pltpu.VMEM((4 * rows, states), bf16),
            pltpu.VMEM((4 * rows, 128), f32),
            pltpu.VMEM((blocks, 24, 128), f32),
            pltpu.VMEM((blocks, STATE, 2 * half), f32),
            pltpu.VMEM((blocks, 8, 2 * half), f32),
            pltpu.VMEM((blocks, STATE, 2 * half), bf16),
            pltpu.VMEM((4 * rows, half), f32),
            pltpu.VMEM((32, 48, 128), bf16),
            pltpu.VMEM((32, 48, 128), bf16),
            pltpu.VMEM((32, 32, 128), bf16),
            pltpu.VMEM((32, 32, 128), bf16),
            pltpu.VMEM((4 * rows, half), bf16),
            pltpu.VMEM((4, rows, half), bf16),
            pltpu.VMEM((2, rows // 2, half), bf16),
            pltpu.VMEM((width, rows), f32),
            pltpu.SemaphoreType.DMA((FLAGS,)),
            pltpu.SemaphoreType.DMA((15,)),
        ],
        compiler_params=pltpu.CompilerParams(
            collective_id=0, has_side_effects=True, vmem_limit_bytes=60 * 2**20
        ),
        name="mixer",
    )(
        tokens,
        w_value,
        w_state_in,
        w_state_out,
        w_gate,
        w_out.T,
        norm_gain.reshape(1, -1),
        w_step_forward.T,
        w_step_backward.T,
        conv_value,
        conv_state_in,
        conv_state_out,
        step_offset,
        fading_speed,
        out_gain.reshape(1, -1),
    )


OUT_TYPE = jnp.bfloat16


def local(
    input_activations,
    norm_gain,
    w_gate,
    w_value,
    w_state_in,
    w_state_out,
    w_step_forward,
    w_step_backward,
    step_offset,
    fading_speed,
    conv_value,
    conv_state_in,
    conv_state_out,
    out_gain,
    w_out,
):
    return mix(
        input_activations,
        norm_gain,
        w_gate,
        w_value,
        w_state_in,
        w_state_out,
        w_step_forward,
        w_step_backward,
        step_offset,
        fading_speed,
        conv_value,
        conv_state_in,
        conv_state_out,
        out_gain,
        w_out,
    )


def solution(mesh):
    torus = Mesh(mesh.devices.reshape(4, 4, 2, 4), SP_TP)
    return jax.shard_map(
        local,
        mesh=torus,
        in_specs=(
            P(SP_TP, None),
            P(),
            P(SP, "x"),
            P(SP, "x"),
            P(SP, "x"),
            P(SP, "x"),
            P(SP, "x"),
            P(SP, "x"),
            P(None, "x"),
            P(None, "x"),
            P(None, "x"),
            P(None, "x"),
            P(None, "x"),
            P("x"),
            P("x", SP),
        ),
        out_specs=P(SP_TP, None),
        check_vma=False,
    )
```

```python
import functools
import math

import jax
import jax.numpy as jnp
from jax import lax
from jax.experimental import pallas as pl
from jax.experimental.pallas import tpu as pltpu
from jax.sharding import Mesh
from jax.sharding import PartitionSpec as P

HEAD_DIM = 64
STATE = 128
BLOCK = 128
SP = ("z", "y", "c")
SP_TP = ("z", "y", "c", "x")
EPSILON = 1e-06
MESH = pl.DeviceIdType.MESH
VALUE, INWARD, OUTWARD, STEPS = range(4)
HALO = 16


def place():
    return [lax.axis_index(name) for name in ("z", "y", "c", "x")]


def step(at, by):
    return lax.rem(at + by + 4, 4)


def stretch_at(z, y, c, by):
    n = lax.rem(z * 8 + y * 2 + c + by + 32, 32)
    return {"z": n // 8, "y": lax.rem(n // 2, 4), "c": lax.rem(n, 2)}


class Wire:
    def __init__(self, flags, self_free):
        self.flags, self.count, self.to, self.sent = flags, 0, self_free, []

    def flag(self):
        self.count += 1
        return self.flags.at[self.count - 1]

    def go(self, source, to, send, recv, target=None):
        pltpu.make_async_remote_copy(
            src_ref=source,
            dst_ref=source if target is None else target,
            send_sem=send,
            recv_sem=recv,
            device_id=to,
            device_id_type=MESH,
        ).start()

    def span(self, ref, flag):
        return pltpu.make_async_remote_copy(
            src_ref=ref,
            dst_ref=ref,
            send_sem=flag,
            recv_sem=flag,
            device_id=self.to,
            device_id_type=MESH,
        )

    def landed(self, ref, flag):
        self.span(ref, flag).wait_recv()

    def drain(self):
        for ref, flag in self.sent:
            self.span(ref, flag).wait_send()


class Ring:
    def __init__(self, wire, axis, at, block, low, high, many):
        self.wire, self.at = wire, at
        self.up, self.down = {axis: step(at, 1)}, {axis: step(at, 3)}
        self.block, self.low, self.high, self.many = block, low, high, many
        self.out, self.near, self.away = wire.flag(), wire.flag(), wire.flag()
        wire.sent.append((many(3), self.out))

    def start(self):
        self.wire.go(self.block(self.at), self.up, self.out, self.near)
        self.wire.go(self.block(self.at), self.down, self.out, self.near)

    def forward(self):
        self.wire.landed(self.many(2), self.near)
        self.wire.go(self.low(step(self.at, 3)), self.up, self.out, self.away)
        self.wire.go(self.high(step(self.at, 1)), self.down, self.out, self.away)

    def finish(self):
        self.wire.landed(self.many(1), self.away)


LOG2E = 1.4426950408889634


def dot_nt(a, b):
    return lax.dot_general(a, b, (((1,), (1,)), ((), ())), preferred_element_type=jnp.float32)


def dot_tn(a, b):
    return lax.dot_general(a, b, (((0,), (0,)), ((), ())), preferred_element_type=jnp.float32)


def dot(a, b, precision=None):
    return lax.dot_general(
        a, b, (((1,), (0,)), ((), ())), precision=precision, preferred_element_type=jnp.float32
    )


def iota(shape, dim):
    return lax.broadcasted_iota(jnp.int32, shape, dim)


def silu(v):
    part = 0.5 * v
    return part + part * jnp.tanh(part)


def mixer_kernel(
    shift,
    tokens_hbm,
    value_hbm,
    state_in_hbm,
    state_out_hbm,
    gate_hbm,
    w_out_hbm,
    norm_gain_hbm,
    step_forward_hbm,
    step_backward_hbm,
    tap_value_hbm,
    tap_in_hbm,
    tap_out_hbm,
    offset_hbm,
    speed_hbm,
    gain_hbm,
    out_ref,
    norm_gain_ref,
    step_forward_ref,
    step_backward_ref,
    tap_value_ref,
    tap_in_ref,
    tap_out_ref,
    offset_ref,
    speed_ref,
    gain_ref,
    heads_ref,
    squares,
    fades,
    tokens,
    edges,
    normed,
    wv,
    ws,
    wg,
    wo,
    projected,
    gates,
    raw,
    signal,
    inward,
    outward,
    column,
    rowwise,
    states,
    decays,
    before,
    inner,
    totals,
    arrived,
    onward,
    incoming,
    mixed,
    shards,
    relay,
    summed,
    flags,
    local_sem,
):
    z, y, c, x = place()
    me = z * 8 + y * 2 + c
    wire = Wire(flags, {"c": 1 - c})
    rows = tokens.shape[1]
    middle = rows // 2
    count = 4 * rows
    blocks = count // BLOCK
    half = signal.shape[1]
    wide = 2 * half
    groups = inward.shape[1] // STATE
    ratio = half // HEAD_DIM // groups
    heads = groups * ratio
    span = ratio * HEAD_DIM
    lead = inward.shape[1]
    partner = {"c": 1 - c}

    def stretch(n):
        return {"z": n // 8, "y": lax.rem(n // 2, 4), "c": lax.rem(n, 2)}

    own = [
        pltpu.make_async_copy(tokens_hbm, tokens.at[x], local_sem.at[0]),
        pltpu.make_async_copy(value_hbm, wv.at[z, y, c], local_sem.at[1]),
        pltpu.make_async_copy(state_in_hbm, ws.at[z, y, c, :, pl.ds(0, lead)], local_sem.at[2]),
        pltpu.make_async_copy(state_out_hbm, ws.at[z, y, c, :, pl.ds(lead, lead)], local_sem.at[3]),
        pltpu.make_async_copy(gate_hbm, wg.at[z, y, c], local_sem.at[4]),
        pltpu.make_async_copy(w_out_hbm, wo.at[z, y, c, x], local_sem.at[5]),
    ]
    small = (
        (step_forward_hbm, step_forward_ref),
        (step_backward_hbm, step_backward_ref),
        (offset_hbm, offset_ref),
        (speed_hbm, speed_ref),
        (norm_gain_hbm, norm_gain_ref),
        (tap_value_hbm, tap_value_ref),
        (tap_in_hbm, tap_in_ref),
        (tap_out_hbm, tap_out_ref),
        (gain_hbm, gain_ref),
    )
    own += [
        pltpu.make_async_copy(source, target, local_sem.at[6 + k])
        for k, (source, target) in enumerate(small)
    ]
    for copy in own:
        copy.start()
    barrier = pltpu.get_barrier_semaphore()

    near = [{axis: step(at, by)} for axis, at in (("x", x), ("y", y), ("z", z)) for by in (1, 3)]
    for other in near + [partner]:
        pl.semaphore_signal(barrier, inc=1, device_id=other, device_id_type=MESH)
    for copy in own:
        copy.wait()
    depth = step_forward_ref.shape[1]
    steps = jnp.concatenate(
        [
            step_forward_ref[...].astype(jnp.float32),
            step_backward_ref[...].astype(jnp.float32),
            jnp.zeros((128 - 2 * heads, depth), jnp.float32),
        ],
        axis=0,
    )
    steps = jnp.concatenate([steps, jnp.zeros((128, 128 - depth), jnp.float32)], axis=1).T
    ws[z, y, c, :, 2 * lead :] = steps[0:depth].astype(jnp.bfloat16)
    lines = jnp.concatenate(
        [
            jnp.concatenate([ref[w : w + 1, :] * sign for w in range(2)], axis=1)
            for ref, sign in ((offset_ref, 1.0), (speed_ref, -1.0))
        ],
        axis=0,
    )
    lines = jnp.concatenate([lines, jnp.zeros((2, 128 - 2 * heads), jnp.float32)], axis=1)
    heads_ref[...] = jnp.concatenate([lines, jnp.zeros((126, 128), jnp.float32)], axis=0).T[
        0 : 2 * heads
    ]
    pl.semaphore_wait(barrier, 7)

    wo_x = Ring(
        wire,
        "x",
        x,
        lambda at: wo.at[z, y, c, at],
        lambda at: wo.at[z, y, c, at, pl.ds(0, 32)],
        lambda at: wo.at[z, y, c, at, pl.ds(32, 32)],
        lambda n: wo.at[z, y, c, pl.ds(0, n)],
    )
    wo_x.start()

    low, high = pl.ds(0, middle), pl.ds(middle, middle)
    up, down = {"x": step(x, 1)}, {"x": step(x, 3)}
    tokens_out, first_half, second_half = wire.flag(), wire.flag(), wire.flag()
    far_ends, far_rest = wire.flag(), wire.flag()
    wire.sent.append((tokens.at[pl.ds(0, 3)], tokens_out))
    wire.go(tokens.at[x, low], up, tokens_out, first_half)
    wire.go(tokens.at[x, high], down, tokens_out, first_half)

    def first(buffer, axis, keep=()):
        def at(n, part):
            spot = (z, n, c) if axis == "y" else (n, y, c)
            if keep:
                start, size = keep
                return buffer.at[(*spot, pl.ds(start, size) if part is None else start + part)]
            return buffer.at[spot] if part is None else buffer.at[(*spot, pl.ds(32 * part, 32))]

        here = y if axis == "y" else z

        def many(n):
            spot = (z, pl.ds(0, n), c) if axis == "y" else (pl.ds(0, n), y, c)
            return buffer.at[(*spot, pl.ds(*keep))] if keep else buffer.at[spot]

        return Ring(
            wire, axis, here, lambda n: at(n, None), lambda n: at(n, 0), lambda n: at(n, 1), many
        )

    def group(buffer, axis, n, part, keep):
        some = pl.ds(0, 4) if part is None else pl.ds(2 * part, 2)
        spot = (n, some, c) if axis == "z" else (some, n, c)
        return buffer.at[(*spot, pl.ds(*keep))] if keep else buffer.at[spot]

    def second(buffer, axis, keep=()):
        here = y if axis == "y" else z
        return Ring(
            wire,
            axis,
            here,
            lambda n: group(buffer, axis, n, None, keep),
            lambda n: group(buffer, axis, n, 0, keep),
            lambda n: group(buffer, axis, n, 1, keep),
            lambda n: group(buffer, axis, pl.ds(0, n), None, keep),
        )

    pairs = {}
    for name, buffer in (("v", wv), ("s", ws), ("g", wg), ("o", wo)):
        pairs[name] = wire.flag(), wire.flag()
        wire.sent.append((buffer.at[:, :, 1 - c], pairs[name][0]))

    def across(name, buffer, axis, by, keep=()):
        here = y if axis == "y" else z
        wire.go(group(buffer, axis, step(here, by), None, keep), partner, *pairs[name])

    def crossed(name, buffer):
        wire.landed(buffer.at[:, :, 1 - c], pairs[name][1])

    v_first, s_first = first(wv, "y"), first(ws, "z")
    v_first.start()
    s_first.start()

    def main_row(shard):
        return HALO + shard * rows

    def normalize(ref, size, to):
        width = ref.shape[-1]

        @pl.loop(0, size // 32, unroll=2)
        def _(k):
            taken = pl.ds(pl.multiple_of(k * 32, 32), 32)
            cells = ref[taken, :].astype(jnp.float32)
            total = cells[:, 0:128] * cells[:, 0:128]
            for at in range(128, width, 128):
                total = total + cells[:, at : at + 128] * cells[:, at : at + 128]
            squares[taken, :] = total

        level = lax.rsqrt(
            jnp.sum(squares[0:size, :], axis=-1, keepdims=True) * (1.0 / width) + EPSILON
        )
        squares[0:size, :] = jnp.broadcast_to(level, (size, 128))

        @pl.loop(0, size // 32, unroll=2)
        def _(k):
            taken = pl.ds(pl.multiple_of(k * 32, 32), 32)
            scale = squares[taken, :]
            cells = ref[taken, :].astype(jnp.float32)
            placed = pl.ds(pl.multiple_of(to + k * 32, 16), 32)
            for at in range(0, width, 128):
                normed[placed, at : at + 128] = (
                    cells[:, at : at + 128] * scale * norm_gain_ref[:, at : at + 128]
                ).astype(jnp.bfloat16)

    shard_in = (x, step(x, 3), step(x, 1), step(x, 2))

    def project(slots, parts):
        edge = not slots
        begin, size = (slots[0] * rows, len(slots) * rows) if slots else (4 * rows, 2 * HALO)
        taken = pl.ds(begin, size)

        def put(values, columns):
            for k, slot in enumerate(slots):
                placed = pl.ds(pl.multiple_of(main_row(shard_in[slot]), 16), rows)
                projected[placed, columns] = values[k * rows : (k + 1) * rows]
            if edge:
                projected[0:HALO, columns] = jnp.where(me > 0, values[0:HALO], 0).astype(
                    values.dtype
                )
                projected[main_row(4) : main_row(4) + HALO, columns] = jnp.where(
                    me < 31, values[HALO:], 0
                ).astype(values.dtype)

        def product(weights, columns):
            return dot(normed[taken, :], weights[:, :, :, :, columns].reshape(-1, 256)).astype(
                jnp.bfloat16
            )

        if VALUE in parts:

            @pl.loop(0, half // 256)
            def _(k):
                columns = pl.ds(pl.multiple_of(k * 256, 256), 256)
                put(product(wv, columns), columns)

        if INWARD in parts:
            put(product(ws, slice(0, lead)), slice(half, half + lead))
        if OUTWARD in parts:
            put(product(ws, slice(lead, 2 * lead)), slice(half + lead, wide))
        if STEPS in parts:
            values = dot(normed[taken, :], ws[:, :, :, :, 2 * lead :].reshape(-1, 128)).astype(
                jnp.bfloat16
            )
            for k, slot in enumerate(slots):
                placed = pl.ds(pl.multiple_of(shard_in[slot] * rows, rows), rows)
                raw[placed, :] = values[k * rows : (k + 1) * rows]

    def project_gate(slots):
        taken = pl.ds(slots[0] * rows, len(slots) * rows)

        @pl.loop(0, half // 256)
        def _(k):
            columns = pl.ds(pl.multiple_of(k * 256, 256), 256)
            values = dot(normed[taken, :], wg[:, :, :, :, columns].reshape(-1, 256))
            values = silu(values.astype(jnp.bfloat16).astype(jnp.float32)).astype(jnp.bfloat16)
            for k, slot in enumerate(slots):
                placed = pl.ds(pl.multiple_of(shard_in[slot] * rows, rows), rows)
                gates[placed, columns] = values[k * rows : (k + 1) * rows]

    normalize(tokens.at[x], rows, 0)

    v_first.forward()
    wo_x.forward()
    wire.go(tokens.at[x, high], up, tokens_out, second_half)
    wire.go(tokens.at[x, low], down, tokens_out, second_half)
    s_first.forward()
    v_first.finish()
    v_second = second(wv, "z")
    v_second.start()
    across("v", wv, "z", 0)
    s_first.finish()
    s_second = second(ws, "y")
    s_second.start()
    across("s", ws, "y", 0)
    g_first = first(wg, "z")
    g_first.start()

    wire.landed(tokens.at[0], first_half)
    for by, start, to, flag in (
        (3, (0, HALO), up, far_ends),
        (1, (rows - HALO, HALO), down, far_ends),
        (3, (HALO, middle - HALO), up, far_rest),
        (1, (middle, middle - HALO), down, far_rest),
    ):
        wire.go(tokens.at[step(x, by), pl.ds(*start)], to, tokens_out, flag)
    wo_x.finish()
    lo_first, hi_first = first(wo, "y", (0, 2)), first(wo, "z", (2, 2))
    lo_first.start()
    hi_first.start()
    normalize(tokens.at[step(x, 3), low], middle, rows)
    normalize(tokens.at[step(x, 1), high], middle, 2 * rows + middle)

    v_second.forward()
    s_second.forward()
    for by in (3, 1):
        across("v", wv, "z", by)
        across("s", ws, "y", by)
    g_first.forward()
    v_second.finish()
    across("v", wv, "z", 2)
    s_second.finish()
    across("s", ws, "y", 2)
    g_first.finish()
    g_second = second(wg, "y")
    g_second.start()
    across("g", wg, "y", 0)
    lo_first.forward()
    hi_first.forward()
    crossed("v", wv)
    crossed("s", ws)
    project((0,), (VALUE, INWARD, OUTWARD, STEPS))

    wire.landed(tokens.at[0], second_half)
    normalize(tokens.at[step(x, 3), high], middle, rows + middle)
    normalize(tokens.at[step(x, 1), low], middle, 2 * rows)
    wire.landed(edges, far_ends)
    edge_out, edge_in = wire.flag(), wire.flag()
    wire.sent.append((edges, edge_out))
    for slot, (shard, offset, by) in enumerate(((3, rows - HALO, 1), (0, 0, 31))):
        wire.go(
            tokens.at[shard, pl.ds(offset, HALO)],
            stretch_at(z, y, c, by),
            edge_out,
            edge_in,
            edges.at[pl.ds(slot * HALO, HALO)],
        )
    lo_first.finish()
    lo_second = second(wo, "z", (0, 2))
    lo_second.start()
    across("o", wo, "z", 0, (0, 2))
    hi_first.finish()
    hi_second = second(wo, "y", (2, 2))
    hi_second.start()
    across("o", wo, "y", 0, (2, 2))
    project((1, 2), (VALUE, INWARD, OUTWARD, STEPS))
    g_second.forward()
    across("g", wg, "y", 3)
    across("g", wg, "y", 1)
    wire.landed(edges, edge_in)
    normalize(edges, 2 * HALO, 4 * rows)
    project((), (VALUE, INWARD, OUTWARD))

    row, col = iota((BLOCK, BLOCK), 0), iota((BLOCK, BLOCK), 1)
    lower = row >= col
    triangle = jnp.where(row <= col, 1.0, 0.0)

    def spread(kind):
        place_of = iota((128, wide), 1) // HEAD_DIM + 2 * heads * kind
        return jnp.where(place_of == iota((128, wide), 0), 1.0, 0.0)

    spread_weight = spread(2).astype(jnp.bfloat16)

    def rows_of(k):
        return pl.ds(pl.multiple_of(k * BLOCK, BLOCK), BLOCK)

    def filtered(k, begin, end):
        window = pl.ds(pl.multiple_of(k * BLOCK, BLOCK), BLOCK + 2 * HALO)
        for at in range(begin, end, 128):
            if at < half:
                tap_ref, target, start = tap_value_ref, signal, at
            elif at < half + lead:
                tap_ref, target, start = tap_in_ref, inward, at - half
            else:
                tap_ref, target, start = tap_out_ref, outward, at - half - lead
            cells = projected[window, at : at + 128].astype(jnp.float32)
            tap = tap_ref[:, start : start + 128]
            here = slice(HALO, HALO + BLOCK)
            total = (
                tap[0:1] * pltpu.roll(cells, 1, 0)[here]
                + tap[1:2] * cells[here]
                + tap[2:3] * pltpu.roll(cells, BLOCK + 2 * HALO - 1, 0)[here]
            )
            target[rows_of(k), start : start + 128] = silu(total).astype(jnp.bfloat16)

    def prepare(first_block):
        some = [lax.rem(first_block + n, blocks) for n in range(4)]
        both = 2 * heads
        forward_row = lax.rem(iota((4 * both, BLOCK), 0), both) < heads
        size = jax.nn.softplus(
            jnp.concatenate(
                [raw[rows_of(k), :].astype(jnp.float32).T[0:both] for k in some], axis=0
            )
            + jnp.concatenate([heads_ref[:, 0:1]] * 4, axis=0)
            - shift
        )
        logs = size * jnp.concatenate([heads_ref[:, 1:2]] * 4, axis=0)
        through = dot(logs, triangle, lax.Precision.HIGHEST)
        until = through - logs
        whole = through[:, BLOCK - 1 : BLOCK]
        logsize = jnp.log(size)
        lines = jnp.where(forward_row, logsize - through, logsize + until) * LOG2E
        kinds = (
            jnp.where(forward_row, through, -until) * LOG2E,
            jnp.exp(jnp.where(forward_row, through, whole - until)),
            size * jnp.exp(jnp.where(forward_row, whole - through, until)),
            jnp.broadcast_to(jnp.exp(whole), (4 * both, BLOCK)),
        )
        turned = []
        for n, k in enumerate(some):
            own_rows = slice(n * both, (n + 1) * both)
            rowwise[k, 0:both, :] = lines[own_rows]
            rowwise[k, both : both + heads, :] = (
                size[n * both : n * both + heads] + size[n * both + heads : (n + 1) * both]
            )
            block = jnp.concatenate(
                [kind[own_rows] for kind in kinds]
                + [jnp.zeros((128 - 4 * both, BLOCK), jnp.float32)],
                axis=0,
            ).T
            column[rows_of(k), :] = block
            fades[k] = block[0:8]
            turned.append(block.astype(jnp.bfloat16))
        turned = jnp.concatenate(turned, axis=0)
        for g in range(groups):
            across_in = [
                inward[rows_of(k), g * STATE : (g + 1) * STATE].astype(jnp.float32).T.astype(
                    jnp.bfloat16
                )
                for k in some
            ]
            cells = jnp.concatenate(
                [signal[rows_of(k), g * span : (g + 1) * span] for k in some], axis=0
            )
            for way in range(2):
                placed = slice(way * half + g * span, way * half + (g + 1) * span)
                content = (
                    cells.astype(jnp.float32) * dot(turned, spread_weight[:, placed])
                ).astype(jnp.bfloat16)
                for n, k in enumerate(some):
                    states[k, :, placed] = dot(
                        across_in[n], content[n * BLOCK : (n + 1) * BLOCK]
                    )

    away = 2 * step(x, 2)

    @pl.loop(0, 4)
    def _(k):
        filtered(lax.rem(away + 3 + k, blocks), 0, wide)

    prepare(away + 3)

    wire.landed(tokens.at[0, pl.ds(0, rows - 2 * HALO)], far_rest)
    normalize(tokens.at[step(x, 2)], rows, 3 * rows)
    project((3,), (VALUE, INWARD, STEPS))

    @pl.loop(0, 4)
    def _(k):
        filtered(lax.rem(away + 7 + k, blocks), 0, half + lead)

    prepare(away + 7)

    over = dot(
        jnp.concatenate([fades[k, 0:1, :] for k in range(blocks)], axis=0),
        spread(3),
        lax.Precision.HIGHEST,
    )
    for k in range(blocks):
        decays[k] = jnp.broadcast_to(over[k : k + 1], (8, wide))

    @pl.loop(0, wide // 128)
    def _(j):
        lanes = pl.ds(pl.multiple_of(j * 128, 128), 128)
        backward = j >= half // 128
        total = jnp.zeros((STATE, 128), jnp.float32)
        decay = jnp.ones((1, 128), jnp.float32)
        for k in range(blocks):
            at = jnp.where(backward, blocks - 1 - k, k)
            part = decays[at, 0:1, lanes]
            total = total * part + states[at, :, lanes]
            decay = decay * part
        upper = decay.astype(jnp.bfloat16).astype(jnp.float32)
        centre = (decay - upper).astype(jnp.bfloat16).astype(jnp.float32)
        rest = decay - upper - centre
        place_row = iota((16, 128), 0)
        tail = jnp.where(place_row == 0, upper, jnp.where(place_row == 1, centre, rest))
        for q in range(4):
            totals[4 * j + q, 0:32, :] = total[32 * q : 32 * q + 32].astype(jnp.bfloat16)
            totals[4 * j + q, 32:48, :] = tail.astype(jnp.bfloat16)

    state_flags = [wire.flag() for _ in range(4)]
    wire.sent.append((totals.at[pl.ds(0, 31)], state_flags[0]))
    wire.sent.append((onward.at[pl.ds(0, 31)], state_flags[2]))

    def disperse(box, inbox, send, recv):
        @pl.loop(0, 31)
        def _(k):
            to = lax.rem(me + lax.rem(k + 15, 31) + 1, 32)
            wire.go(box.at[to], stretch(to), send, recv, inbox.at[me])

    disperse(totals, arrived, *state_flags[:2])

    arrived[me] = totals[me]

    g_second.finish()
    across("g", wg, "y", 2)

    def within(k):
        for g in range(groups):
            inner_product = dot_nt(
                outward[rows_of(k), g * STATE : (g + 1) * STATE],
                inward[rows_of(k), g * STATE : (g + 1) * STATE],
            )
            cells = signal[rows_of(k), g * span : (g + 1) * span]
            head_of = iota((BLOCK, span), 1) // HEAD_DIM
            weights, content = [], []
            for r in range(ratio):
                h = g * ratio + r
                below = column[rows_of(k), h : h + 1] + rowwise[k, h : h + 1, :]
                above = (
                    column[rows_of(k), heads + h : heads + h + 1]
                    + rowwise[k, heads + h : heads + h + 1, :]
                )
                decay = jnp.exp2(jnp.where(lower, below, above))
                both = jnp.where(
                    row == col, rowwise[k, 2 * heads + h : 2 * heads + h + 1, :], decay
                )
                weights.append((inner_product * both).astype(jnp.bfloat16))
                content.append(jnp.where(head_of == r, cells, jnp.zeros_like(cells)))
            inner[rows_of(k), g * span : (g + 1) * span] = dot(
                jnp.concatenate(weights, axis=1), jnp.concatenate(content, axis=0)
            )

    lo_second.forward()
    hi_second.forward()
    for by in (3, 1):
        across("o", wo, "z", by, (0, 2))
        across("o", wo, "y", by, (2, 2))

    project((3,), (OUTWARD,))

    @pl.loop(0, 4)
    def _(k):
        filtered(lax.rem(away + 7 + k, blocks), half + lead, wide)


    @pl.loop(0, blocks // 2)
    def _(k):
        within(k)

    wire.landed(arrived.at[pl.ds(0, 31)], state_flags[1])

    flip = me >= 16

    def hop(k, state):
        at = jnp.where(flip, 31 - k, k)
        onward[at] = state.astype(jnp.bfloat16)
        message = arrived[at].astype(jnp.float32)
        decay = message[32:33] + message[33:34] + message[34:35]
        return state * decay + message[0:32]

    lax.fori_loop(0, 32, hop, jnp.zeros((32, 128), jnp.float32))

    disperse(onward, incoming, *state_flags[2:])

    incoming[me] = onward[me]

    crossed("g", wg)
    project_gate((0, 1, 2))
    project_gate((3,))

    @pl.loop(blocks // 2, blocks)
    def _(k):
        within(k)

    wire.landed(incoming.at[pl.ds(0, 31)], state_flags[3])

    @pl.loop(0, wide // 128)
    def _(j):
        lanes = pl.ds(pl.multiple_of(j * 128, 128), 128)
        backward = j >= half // 128
        state = jnp.concatenate([incoming[4 * j + q] for q in range(4)], axis=0).astype(jnp.float32)
        for k in range(blocks):
            at = jnp.where(backward, blocks - 1 - k, k)
            before[at, :, lanes] = state.astype(jnp.bfloat16)
            state = state * decays[at, 0:1, lanes] + states[at, :, lanes]

    spread_read = spread(1).astype(jnp.bfloat16)

    def finish(k):
        scale = dot(column[rows_of(k), :].astype(jnp.bfloat16), spread_read)
        for g in range(groups):
            lanes = slice(g * span, (g + 1) * span)
            read = outward[rows_of(k), g * STATE : (g + 1) * STATE]
            total = inner[rows_of(k), lanes]
            for way in range(2):
                placed = slice(way * half + g * span, way * half + (g + 1) * span)
                total = total + dot(read, before[k, :, placed]) * scale[:, placed]
            gated = total * gates[rows_of(k), lanes].astype(jnp.float32)
            level = lax.rsqrt(jnp.mean(gated * gated, axis=-1, keepdims=True) + EPSILON)
            mixed[rows_of(k), lanes] = (gated * level * gain_ref[:, lanes]).astype(jnp.bfloat16)

    def finish_shard(shard):
        @pl.loop(0, 2)
        def _(b):
            finish(2 * shard + b)

    def part(shard, some):
        start, size = some
        return mixed.at[pl.ds(pl.multiple_of(shard * rows + start, middle), size)]

    mixed_out, relayed, from_below, from_above, from_far = [wire.flag() for _ in range(5)]
    wire.sent.append((shards, mixed_out))
    finish(2 * step(x, 2))
    wire.go(part(step(x, 2), (0, middle)), up, mixed_out, relayed, relay.at[0])
    finish(2 * step(x, 2) + 1)
    wire.go(part(step(x, 2), (middle, middle)), down, mixed_out, relayed, relay.at[1])
    finish_shard(step(x, 1))
    wire.go(part(step(x, 1), (0, rows)), up, mixed_out, from_below, shards.at[x])
    finish_shard(step(x, 3))
    wire.go(part(step(x, 3), (0, rows)), down, mixed_out, from_above, shards.at[x])
    lo_second.finish()
    across("o", wo, "z", 2, (0, 2))
    hi_second.finish()
    across("o", wo, "y", 2, (2, 2))
    finish_shard(x)
    shards[x] = mixed[pl.ds(pl.multiple_of(x * rows, rows), rows), :]
    wire.landed(relay, relayed)
    wire.go(relay.at[0], up, mixed_out, from_far, shards.at[step(x, 3), low])
    wire.go(relay.at[1], down, mixed_out, from_far, shards.at[step(x, 1), high])
    crossed("o", wo)

    def contribute(at, begin, end):
        @pl.loop(0, 2)
        def _(k):
            lines = pl.ds(pl.multiple_of(k * 1024, 1024), 1024)
            total = dot_nt(wo[pl.ds(2 * k, 2), :, :, at].reshape(1024, -1), shards[at])
            if not begin:
                total = total + summed[lines, :]
            if end:
                out_ref[:, lines] = total.T.astype(out_ref.dtype)
            else:
                summed[lines, :] = total

    contribute(x, True, False)
    wire.landed(shards.at[0], from_below)
    contribute(step(x, 3), False, False)
    wire.landed(shards.at[0], from_above)
    contribute(step(x, 1), False, False)
    wire.landed(shards.at[0], from_far)
    contribute(step(x, 2), False, True)

    wire.drain()


FLAGS = 57


def mix(
    tokens,
    norm_gain,
    w_gate,
    w_value,
    w_state_in,
    w_state_out,
    w_step_forward,
    w_step_backward,
    step_offset,
    fading_speed,
    conv_value,
    conv_state_in,
    conv_state_out,
    out_gain,
    w_out,
):
    rows, width = tokens.shape
    depth, half = w_value.shape
    states = w_state_in.shape[1]
    blocks = 4 * rows // BLOCK
    anywhere = pl.BlockSpec(memory_space=pl.ANY)
    bf16, f32 = jnp.bfloat16, jnp.float32
    return pl.pallas_call(
        functools.partial(mixer_kernel, math.log(4 * rows * lax.axis_size(SP))),
        out_shape=pltpu.VMEM((rows, width), OUT_TYPE),
        in_specs=[anywhere] * 15,
        out_specs=pl.BlockSpec(memory_space=pltpu.VMEM),
        scratch_shapes=[
            pltpu.VMEM((1, width), f32),
            pltpu.VMEM(w_step_forward.shape[::-1], bf16),
            pltpu.VMEM(w_step_backward.shape[::-1], bf16),
            pltpu.VMEM(conv_value.shape, f32),
            pltpu.VMEM(conv_state_in.shape, f32),
            pltpu.VMEM(conv_state_out.shape, f32),
            pltpu.VMEM(step_offset.shape, f32),
            pltpu.VMEM(fading_speed.shape, f32),
            pltpu.VMEM((1, half), f32),
            pltpu.VMEM((16, 128), f32),
            pltpu.VMEM((rows, 128), f32),
            pltpu.VMEM((blocks, 8, 128), f32),
            pltpu.VMEM((4, rows, width), bf16),
            pltpu.VMEM((2 * HALO, width), bf16),
            pltpu.VMEM((4 * rows + 2 * HALO, width), bf16),
            pltpu.VMEM((4, 4, 2, depth, half), bf16),
            pltpu.VMEM((4, 4, 2, depth, 2 * states + 128), bf16),
            pltpu.VMEM((4, 4, 2, depth, half), bf16),
            pltpu.VMEM((4, 4, 2, 4, depth, half), bf16),
            pltpu.VMEM((4 * rows + 2 * HALO, 2 * half), bf16),
            pltpu.VMEM((4 * rows, half), bf16),
            pltpu.VMEM((4 * rows, 128), bf16),
            pltpu.VMEM((4 * rows, half), bf16),
            pltpu.VMEM((4 * rows, states), bf16),
            pltpu.VMEM((4 * rows, states), bf16),
            pltpu.VMEM((4 * rows, 128), f32),
            pltpu.VMEM((blocks, 24, 128), f32),
            pltpu.VMEM((blocks, STATE, 2 * half), f32),
            pltpu.VMEM((blocks, 8, 2 * half), f32),
            pltpu.VMEM((blocks, STATE, 2 * half), bf16),
            pltpu.VMEM((4 * rows, half), f32),
            pltpu.VMEM((32, 48, 128), bf16),
            pltpu.VMEM((32, 48, 128), bf16),
            pltpu.VMEM((32, 32, 128), bf16),
            pltpu.VMEM((32, 32, 128), bf16),
            pltpu.VMEM((4 * rows, half), bf16),
            pltpu.VMEM((4, rows, half), bf16),
            pltpu.VMEM((2, rows // 2, half), bf16),
            pltpu.VMEM((width, rows), f32),
            pltpu.SemaphoreType.DMA((FLAGS,)),
            pltpu.SemaphoreType.DMA((15,)),
        ],
        compiler_params=pltpu.CompilerParams(
            collective_id=0, has_side_effects=True, vmem_limit_bytes=60 * 2**20
        ),
        name="mixer",
    )(
        tokens,
        w_value,
        w_state_in,
        w_state_out,
        w_gate,
        w_out.T,
        norm_gain.reshape(1, -1),
        w_step_forward.T,
        w_step_backward.T,
        conv_value,
        conv_state_in,
        conv_state_out,
        step_offset,
        fading_speed,
        out_gain.reshape(1, -1),
    )


OUT_TYPE = jnp.bfloat16


def local(
    input_activations,
    norm_gain,
    w_gate,
    w_value,
    w_state_in,
    w_state_out,
    w_step_forward,
    w_step_backward,
    step_offset,
    fading_speed,
    conv_value,
    conv_state_in,
    conv_state_out,
    out_gain,
    w_out,
):
    return mix(
        input_activations,
        norm_gain,
        w_gate,
        w_value,
        w_state_in,
        w_state_out,
        w_step_forward,
        w_step_backward,
        step_offset,
        fading_speed,
        conv_value,
        conv_state_in,
        conv_state_out,
        out_gain,
        w_out,
    )


def solution(mesh):
    torus = Mesh(mesh.devices.reshape(4, 4, 2, 4), SP_TP)
    return jax.shard_map(
        local,
        mesh=torus,
        in_specs=(
            P(SP_TP, None),
            P(),
            P(SP, "x"),
            P(SP, "x"),
            P(SP, "x"),
            P(SP, "x"),
            P(SP, "x"),
            P(SP, "x"),
            P(None, "x"),
            P(None, "x"),
            P(None, "x"),
            P(None, "x"),
            P(None, "x"),
            P("x"),
            P("x", SP),
        ),
        out_specs=P(SP_TP, None),
        check_vma=False,
    )
```

```python
import functools
import math

import jax
import jax.numpy as jnp
from jax import lax
from jax.experimental import pallas as pl
from jax.experimental.pallas import tpu as pltpu
from jax.sharding import Mesh
from jax.sharding import PartitionSpec as P

HEAD_DIM = 64
STATE = 128
BLOCK = 128
SP = ("z", "y", "c")
SP_TP = ("z", "y", "c", "x")
EPSILON = 1e-06
MESH = pl.DeviceIdType.MESH
VALUE, INWARD, OUTWARD, STEPS, VALUE_FIRST, VALUE_SECOND = range(6)
HALO = 16


def place():
    return [lax.axis_index(name) for name in ("z", "y", "c", "x")]


def step(at, by):
    return lax.rem(at + by + 4, 4)


def stretch_at(z, y, c, by):
    n = lax.rem(z * 8 + y * 2 + c + by + 32, 32)
    return {"z": n // 8, "y": lax.rem(n // 2, 4), "c": lax.rem(n, 2)}


class Wire:
    def __init__(self, flags, self_free):
        self.flags, self.count, self.to, self.sent = flags, 0, self_free, []

    def flag(self):
        self.count += 1
        return self.flags.at[self.count - 1]

    def go(self, source, to, send, recv, target=None):
        pltpu.make_async_remote_copy(
            src_ref=source,
            dst_ref=source if target is None else target,
            send_sem=send,
            recv_sem=recv,
            device_id=to,
            device_id_type=MESH,
        ).start()

    def span(self, ref, flag):
        return pltpu.make_async_remote_copy(
            src_ref=ref,
            dst_ref=ref,
            send_sem=flag,
            recv_sem=flag,
            device_id=self.to,
            device_id_type=MESH,
        )

    def landed(self, ref, flag):
        self.span(ref, flag).wait_recv()

    def drain(self):
        for ref, flag in self.sent:
            self.span(ref, flag).wait_send()


class Ring:
    def __init__(self, wire, axis, at, block, low, high, many):
        self.wire, self.at = wire, at
        self.up, self.down = {axis: step(at, 1)}, {axis: step(at, 3)}
        self.block, self.low, self.high, self.many = block, low, high, many
        self.out, self.near, self.away = wire.flag(), wire.flag(), wire.flag()
        wire.sent.append((many(3), self.out))

    def start(self):
        self.wire.go(self.block(self.at), self.up, self.out, self.near)
        self.wire.go(self.block(self.at), self.down, self.out, self.near)

    def forward(self):
        self.wire.landed(self.many(2), self.near)
        self.wire.go(self.low(step(self.at, 3)), self.up, self.out, self.away)
        self.wire.go(self.high(step(self.at, 1)), self.down, self.out, self.away)

    def finish(self):
        self.wire.landed(self.many(1), self.away)


LOG2E = 1.4426950408889634


def dot_nt(a, b):
    return lax.dot_general(a, b, (((1,), (1,)), ((), ())), preferred_element_type=jnp.float32)


def dot_tn(a, b):
    return lax.dot_general(a, b, (((0,), (0,)), ((), ())), preferred_element_type=jnp.float32)


def dot(a, b, precision=None):
    return lax.dot_general(
        a, b, (((1,), (0,)), ((), ())), precision=precision, preferred_element_type=jnp.float32
    )


def iota(shape, dim):
    return lax.broadcasted_iota(jnp.int32, shape, dim)


def silu(v):
    part = 0.5 * v
    return part + part * jnp.tanh(part)


def mixer_kernel(
    shift,
    tokens_hbm,
    value_hbm,
    state_in_hbm,
    state_out_hbm,
    gate_hbm,
    w_out_hbm,
    norm_gain_hbm,
    step_forward_hbm,
    step_backward_hbm,
    tap_value_hbm,
    tap_in_hbm,
    tap_out_hbm,
    offset_hbm,
    speed_hbm,
    gain_hbm,
    out_ref,
    norm_gain_ref,
    step_forward_ref,
    step_backward_ref,
    tap_value_ref,
    tap_in_ref,
    tap_out_ref,
    offset_ref,
    speed_ref,
    gain_ref,
    heads_ref,
    squares,
    fades,
    tokens,
    edges,
    normed,
    wv,
    ws,
    wg,
    wo,
    projected,
    gates,
    raw,
    signal,
    inward,
    outward,
    column,
    rowwise,
    states,
    decays,
    before,
    inner,
    totals,
    arrived,
    onward,
    incoming,
    mixed,
    shards,
    relay,
    summed,
    flags,
    local_sem,
):
    z, y, c, x = place()
    me = z * 8 + y * 2 + c
    wire = Wire(flags, {"c": 1 - c})
    rows = tokens.shape[1]
    middle = rows // 2
    count = 4 * rows
    blocks = count // BLOCK
    half = signal.shape[1]
    wide = 2 * half
    groups = inward.shape[1] // STATE
    ratio = half // HEAD_DIM // groups
    heads = groups * ratio
    span = ratio * HEAD_DIM
    lead = inward.shape[1]
    partner = {"c": 1 - c}

    def stretch(n):
        return {"z": n // 8, "y": lax.rem(n // 2, 4), "c": lax.rem(n, 2)}

    own = [
        pltpu.make_async_copy(tokens_hbm, tokens.at[x], local_sem.at[0]),
        pltpu.make_async_copy(value_hbm, wv.at[z, y, c], local_sem.at[1]),
        pltpu.make_async_copy(state_in_hbm, ws.at[z, y, c, :, pl.ds(0, lead)], local_sem.at[2]),
        pltpu.make_async_copy(state_out_hbm, ws.at[z, y, c, :, pl.ds(lead, lead)], local_sem.at[3]),
        pltpu.make_async_copy(gate_hbm, wg.at[z, y, c], local_sem.at[4]),
        pltpu.make_async_copy(w_out_hbm, wo.at[z, y, c, x], local_sem.at[5]),
    ]
    small = (
        (step_forward_hbm, step_forward_ref),
        (step_backward_hbm, step_backward_ref),
        (offset_hbm, offset_ref),
        (speed_hbm, speed_ref),
        (norm_gain_hbm, norm_gain_ref),
        (tap_value_hbm, tap_value_ref),
        (tap_in_hbm, tap_in_ref),
        (tap_out_hbm, tap_out_ref),
        (gain_hbm, gain_ref),
    )
    own += [
        pltpu.make_async_copy(source, target, local_sem.at[6 + k])
        for k, (source, target) in enumerate(small)
    ]
    for copy in own:
        copy.start()
    barrier = pltpu.get_barrier_semaphore()

    near = [{axis: step(at, by)} for axis, at in (("x", x), ("y", y), ("z", z)) for by in (1, 3)]
    for other in near + [partner]:
        pl.semaphore_signal(barrier, inc=1, device_id=other, device_id_type=MESH)
    for copy in own:
        copy.wait()
    depth = step_forward_ref.shape[1]
    steps = jnp.concatenate(
        [
            step_forward_ref[...].astype(jnp.float32),
            step_backward_ref[...].astype(jnp.float32),
            jnp.zeros((128 - 2 * heads, depth), jnp.float32),
        ],
        axis=0,
    )
    steps = jnp.concatenate([steps, jnp.zeros((128, 128 - depth), jnp.float32)], axis=1).T
    ws[z, y, c, :, 2 * lead :] = steps[0:depth].astype(jnp.bfloat16)
    lines = jnp.concatenate(
        [
            jnp.concatenate([ref[w : w + 1, :] * sign for w in range(2)], axis=1)
            for ref, sign in ((offset_ref, 1.0), (speed_ref, -1.0))
        ],
        axis=0,
    )
    lines = jnp.concatenate([lines, jnp.zeros((2, 128 - 2 * heads), jnp.float32)], axis=1)
    heads_ref[...] = jnp.concatenate([lines, jnp.zeros((126, 128), jnp.float32)], axis=0).T[
        0 : 2 * heads
    ]
    pl.semaphore_wait(barrier, 7)

    wo_x = Ring(
        wire,
        "x",
        x,
        lambda at: wo.at[z, y, c, at],
        lambda at: wo.at[z, y, c, at, pl.ds(0, 32)],
        lambda at: wo.at[z, y, c, at, pl.ds(32, 32)],
        lambda n: wo.at[z, y, c, pl.ds(0, n)],
    )
    wo_x.start()

    low, high = pl.ds(0, middle), pl.ds(middle, middle)
    up, down = {"x": step(x, 1)}, {"x": step(x, 3)}
    tokens_out, first_half, second_half = wire.flag(), wire.flag(), wire.flag()
    far_ends, far_rest = wire.flag(), wire.flag()
    wire.sent.append((tokens.at[pl.ds(0, 3)], tokens_out))
    wire.go(tokens.at[x, low], up, tokens_out, first_half)
    wire.go(tokens.at[x, high], down, tokens_out, first_half)

    def first(buffer, axis, keep=()):
        def at(n, part):
            spot = (z, n, c) if axis == "y" else (n, y, c)
            if keep:
                start, size = keep
                return buffer.at[(*spot, pl.ds(start, size) if part is None else start + part)]
            return buffer.at[spot] if part is None else buffer.at[(*spot, pl.ds(32 * part, 32))]

        here = y if axis == "y" else z

        def many(n):
            spot = (z, pl.ds(0, n), c) if axis == "y" else (pl.ds(0, n), y, c)
            return buffer.at[(*spot, pl.ds(*keep))] if keep else buffer.at[spot]

        return Ring(
            wire, axis, here, lambda n: at(n, None), lambda n: at(n, 0), lambda n: at(n, 1), many
        )

    def group(buffer, axis, n, part, keep):
        some = pl.ds(0, 4) if part is None else pl.ds(2 * part, 2)
        spot = (n, some, c) if axis == "z" else (some, n, c)
        return buffer.at[(*spot, pl.ds(*keep))] if keep else buffer.at[spot]

    def second(buffer, axis, keep=()):
        here = y if axis == "y" else z
        return Ring(
            wire,
            axis,
            here,
            lambda n: group(buffer, axis, n, None, keep),
            lambda n: group(buffer, axis, n, 0, keep),
            lambda n: group(buffer, axis, n, 1, keep),
            lambda n: group(buffer, axis, pl.ds(0, n), None, keep),
        )

    pairs = {}
    for name, buffer in (("v", wv), ("s", ws), ("g", wg), ("o", wo)):
        pairs[name] = wire.flag(), wire.flag()
        wire.sent.append((buffer.at[:, :, 1 - c], pairs[name][0]))

    def across(name, buffer, axis, by, keep=()):
        here = y if axis == "y" else z
        wire.go(group(buffer, axis, step(here, by), None, keep), partner, *pairs[name])

    def crossed(name, buffer):
        wire.landed(buffer.at[:, :, 1 - c], pairs[name][1])

    v_first, s_first = first(wv, "y"), first(ws, "z")
    v_first.start()
    s_first.start()

    def main_row(shard):
        return HALO + shard * rows

    def normalize(ref, size, to):
        width = ref.shape[-1]

        @pl.loop(0, size // 32, unroll=2)
        def _(k):
            taken = pl.ds(pl.multiple_of(k * 32, 32), 32)
            cells = ref[taken, :].astype(jnp.float32)
            total = cells[:, 0:128] * cells[:, 0:128]
            for at in range(128, width, 128):
                total = total + cells[:, at : at + 128] * cells[:, at : at + 128]
            squares[taken, :] = total

        level = lax.rsqrt(
            jnp.sum(squares[0:size, :], axis=-1, keepdims=True) * (1.0 / width) + EPSILON
        )
        squares[0:size, :] = jnp.broadcast_to(level, (size, 128))

        @pl.loop(0, size // 32, unroll=2)
        def _(k):
            taken = pl.ds(pl.multiple_of(k * 32, 32), 32)
            scale = squares[taken, :]
            cells = ref[taken, :].astype(jnp.float32)
            placed = pl.ds(pl.multiple_of(to + k * 32, 16), 32)
            for at in range(0, width, 128):
                normed[placed, at : at + 128] = (
                    cells[:, at : at + 128] * scale * norm_gain_ref[:, at : at + 128]
                ).astype(jnp.bfloat16)

    shard_in = (x, step(x, 3), step(x, 1), step(x, 2))

    def project(slots, parts):
        edge = not slots
        begin, size = (slots[0] * rows, len(slots) * rows) if slots else (4 * rows, 2 * HALO)
        taken = pl.ds(begin, size)

        def put(values, columns):
            for k, slot in enumerate(slots):
                placed = pl.ds(pl.multiple_of(main_row(shard_in[slot]), 16), rows)
                projected[placed, columns] = values[k * rows : (k + 1) * rows]
            if edge:
                projected[0:HALO, columns] = jnp.where(me > 0, values[0:HALO], 0).astype(
                    values.dtype
                )
                projected[main_row(4) : main_row(4) + HALO, columns] = jnp.where(
                    me < 31, values[HALO:], 0
                ).astype(values.dtype)

        def product(weights, columns):
            return dot(normed[taken, :], weights[:, :, :, :, columns].reshape(-1, 256)).astype(
                jnp.bfloat16
            )

        if VALUE in parts:

            @pl.loop(0, half // 256)
            def _(k):
                columns = pl.ds(pl.multiple_of(k * 256, 256), 256)
                put(product(wv, columns), columns)

        for name, start in ((VALUE_FIRST, 0), (VALUE_SECOND, half // 2)):
            if name in parts:
                columns = slice(start, start + half // 2)
                put(product(wv, columns), columns)
        if INWARD in parts:
            put(product(ws, slice(0, lead)), slice(half, half + lead))
        if OUTWARD in parts:
            put(product(ws, slice(lead, 2 * lead)), slice(half + lead, wide))
        if STEPS in parts:
            values = dot(normed[taken, :], ws[:, :, :, :, 2 * lead :].reshape(-1, 128)).astype(
                jnp.bfloat16
            )
            for k, slot in enumerate(slots):
                placed = pl.ds(pl.multiple_of(shard_in[slot] * rows, rows), rows)
                raw[placed, :] = values[k * rows : (k + 1) * rows]

    def project_gate(slots):
        taken = pl.ds(slots[0] * rows, len(slots) * rows)

        @pl.loop(0, half // 256)
        def _(k):
            columns = pl.ds(pl.multiple_of(k * 256, 256), 256)
            values = dot(normed[taken, :], wg[:, :, :, :, columns].reshape(-1, 256))
            values = silu(values.astype(jnp.bfloat16).astype(jnp.float32)).astype(jnp.bfloat16)
            for k, slot in enumerate(slots):
                placed = pl.ds(pl.multiple_of(shard_in[slot] * rows, rows), rows)
                gates[placed, columns] = values[k * rows : (k + 1) * rows]

    normalize(tokens.at[x], rows, 0)

    v_first.forward()
    wo_x.forward()
    wire.go(tokens.at[x, high], up, tokens_out, second_half)
    wire.go(tokens.at[x, low], down, tokens_out, second_half)
    s_first.forward()
    v_first.finish()
    v_second = second(wv, "z")
    v_second.start()
    across("v", wv, "z", 0)
    s_first.finish()
    s_second = second(ws, "y")
    s_second.start()
    across("s", ws, "y", 0)
    g_first = first(wg, "z")
    g_first.start()

    wire.landed(tokens.at[0], first_half)
    for by, start, to, flag in (
        (3, (0, HALO), up, far_ends),
        (1, (rows - HALO, HALO), down, far_ends),
        (3, (HALO, middle - HALO), up, far_rest),
        (1, (middle, middle - HALO), down, far_rest),
    ):
        wire.go(tokens.at[step(x, by), pl.ds(*start)], to, tokens_out, flag)
    wo_x.finish()
    lo_first, hi_first = first(wo, "y", (0, 2)), first(wo, "z", (2, 2))
    lo_first.start()
    hi_first.start()
    normalize(tokens.at[step(x, 3), low], middle, rows)
    normalize(tokens.at[step(x, 1), high], middle, 2 * rows + middle)

    v_second.forward()
    s_second.forward()
    for by in (3, 1):
        across("v", wv, "z", by)
        across("s", ws, "y", by)
    g_first.forward()
    v_second.finish()
    across("v", wv, "z", 2)
    s_second.finish()
    across("s", ws, "y", 2)
    g_first.finish()
    g_second = second(wg, "y")
    g_second.start()
    across("g", wg, "y", 0)
    lo_first.forward()
    hi_first.forward()
    crossed("v", wv)
    crossed("s", ws)
    project((0,), (VALUE, INWARD, OUTWARD, STEPS))

    wire.landed(tokens.at[0], second_half)
    normalize(tokens.at[step(x, 3), high], middle, rows + middle)
    normalize(tokens.at[step(x, 1), low], middle, 2 * rows)
    wire.landed(edges, far_ends)
    edge_out, edge_in = wire.flag(), wire.flag()
    wire.sent.append((edges, edge_out))
    for slot, (shard, offset, by) in enumerate(((3, rows - HALO, 1), (0, 0, 31))):
        wire.go(
            tokens.at[shard, pl.ds(offset, HALO)],
            stretch_at(z, y, c, by),
            edge_out,
            edge_in,
            edges.at[pl.ds(slot * HALO, HALO)],
        )
    lo_first.finish()
    lo_second = second(wo, "z", (0, 2))
    lo_second.start()
    across("o", wo, "z", 0, (0, 2))
    hi_first.finish()
    hi_second = second(wo, "y", (2, 2))
    hi_second.start()
    across("o", wo, "y", 0, (2, 2))
    project((1, 2), (VALUE, INWARD, OUTWARD, STEPS))
    g_second.forward()
    across("g", wg, "y", 3)
    across("g", wg, "y", 1)
    wire.landed(edges, edge_in)
    normalize(edges, 2 * HALO, 4 * rows)
    project((), (VALUE, INWARD, OUTWARD))

    row, col = iota((BLOCK, BLOCK), 0), iota((BLOCK, BLOCK), 1)
    lower = row >= col
    triangle = jnp.where(row <= col, 1.0, 0.0)

    def spread(kind):
        place_of = iota((128, wide), 1) // HEAD_DIM + 2 * heads * kind
        return jnp.where(place_of == iota((128, wide), 0), 1.0, 0.0)

    spread_weight = spread(2).astype(jnp.bfloat16)

    def rows_of(k):
        return pl.ds(pl.multiple_of(k * BLOCK, BLOCK), BLOCK)

    def filtered(k, begin, end):
        window = pl.ds(pl.multiple_of(k * BLOCK, BLOCK), BLOCK + 2 * HALO)
        for at in range(begin, end, 128):
            if at < half:
                tap_ref, target, start = tap_value_ref, signal, at
            elif at < half + lead:
                tap_ref, target, start = tap_in_ref, inward, at - half
            else:
                tap_ref, target, start = tap_out_ref, outward, at - half - lead
            cells = projected[window, at : at + 128].astype(jnp.float32)
            tap = tap_ref[:, start : start + 128]
            here = slice(HALO, HALO + BLOCK)
            total = (
                tap[0:1] * pltpu.roll(cells, 1, 0)[here]
                + tap[1:2] * cells[here]
                + tap[2:3] * pltpu.roll(cells, BLOCK + 2 * HALO - 1, 0)[here]
            )
            target[rows_of(k), start : start + 128] = silu(total).astype(jnp.bfloat16)

    def four(first_block):
        return [lax.rem(first_block + n, blocks) for n in range(4)]

    def prepare_steps(first_block):
        some = four(first_block)
        both = 2 * heads
        forward_row = lax.rem(iota((4 * both, BLOCK), 0), both) < heads
        size = jax.nn.softplus(
            jnp.concatenate(
                [raw[rows_of(k), :].astype(jnp.float32).T[0:both] for k in some], axis=0
            )
            + jnp.concatenate([heads_ref[:, 0:1]] * 4, axis=0)
            - shift
        )
        logs = size * jnp.concatenate([heads_ref[:, 1:2]] * 4, axis=0)
        through = dot(logs, triangle, lax.Precision.HIGHEST)
        until = through - logs
        whole = through[:, BLOCK - 1 : BLOCK]
        logsize = jnp.log(size)
        lines = jnp.where(forward_row, logsize - through, logsize + until) * LOG2E
        kinds = (
            jnp.where(forward_row, through, -until) * LOG2E,
            jnp.exp(jnp.where(forward_row, through, whole - until)),
            size * jnp.exp(jnp.where(forward_row, whole - through, until)),
            jnp.broadcast_to(jnp.exp(whole), (4 * both, BLOCK)),
        )
        for n, k in enumerate(some):
            own_rows = slice(n * both, (n + 1) * both)
            rowwise[k, 0:both, :] = lines[own_rows]
            rowwise[k, both : both + heads, :] = (
                size[n * both : n * both + heads] + size[n * both + heads : (n + 1) * both]
            )
            block = jnp.concatenate(
                [kind[own_rows] for kind in kinds]
                + [jnp.zeros((128 - 4 * both, BLOCK), jnp.float32)],
                axis=0,
            ).T
            column[rows_of(k), :] = block
            fades[k] = block[0:8]

    def prepare_states(first_block, chosen):
        some = four(first_block)
        turned = jnp.concatenate(
            [column[rows_of(k), :].astype(jnp.bfloat16) for k in some], axis=0
        )
        for g in chosen:
            across_in = [
                inward[rows_of(k), g * STATE : (g + 1) * STATE].astype(jnp.float32).T.astype(
                    jnp.bfloat16
                )
                for k in some
            ]
            cells = jnp.concatenate(
                [signal[rows_of(k), g * span : (g + 1) * span] for k in some], axis=0
            )
            for way in range(2):
                placed = slice(way * half + g * span, way * half + (g + 1) * span)
                content = (
                    cells.astype(jnp.float32) * dot(turned, spread_weight[:, placed])
                ).astype(jnp.bfloat16)
                for n, k in enumerate(some):
                    states[k, :, placed] = dot(
                        across_in[n], content[n * BLOCK : (n + 1) * BLOCK]
                    )

    away = 2 * step(x, 2)

    @pl.loop(0, 4)
    def _(k):
        filtered(lax.rem(away + 3 + k, blocks), 0, wide)

    prepare_steps(away + 3)
    prepare_states(away + 3, range(groups))

    wire.landed(tokens.at[0, pl.ds(0, rows - 2 * HALO)], far_rest)
    normalize(tokens.at[step(x, 2)], rows, 3 * rows)
    project((3,), (STEPS, INWARD, VALUE_FIRST))

    @pl.loop(0, 4)
    def _(k):
        filtered(lax.rem(away + 7 + k, blocks), 0, half // 2)
        filtered(lax.rem(away + 7 + k, blocks), half, half + lead)

    prepare_steps(away + 7)
    prepare_states(away + 7, (0,))

    over = dot(
        jnp.concatenate([fades[k, 0:1, :] for k in range(blocks)], axis=0),
        spread(3),
        lax.Precision.HIGHEST,
    )
    for k in range(blocks):
        decays[k] = jnp.broadcast_to(over[k : k + 1], (8, wide))

    tiles = span // 128
    ways = half // 128

    def tile_of(g, n):
        return n // tiles * ways + g * tiles + lax.rem(n, tiles)

    def total_up(g):
        @pl.loop(0, 2 * tiles)
        def _(n):
            j = tile_of(g, n)
            lanes = pl.ds(pl.multiple_of(j * 128, 128), 128)
            backward = n >= tiles
            total = jnp.zeros((STATE, 128), jnp.float32)
            decay = jnp.ones((1, 128), jnp.float32)
            for k in range(blocks):
                at = jnp.where(backward, blocks - 1 - k, k)
                part = decays[at, 0:1, lanes]
                total = total * part + states[at, :, lanes]
                decay = decay * part
            upper = decay.astype(jnp.bfloat16).astype(jnp.float32)
            centre = (decay - upper).astype(jnp.bfloat16).astype(jnp.float32)
            rest = decay - upper - centre
            place_row = iota((16, 128), 0)
            tail = jnp.where(place_row == 0, upper, jnp.where(place_row == 1, centre, rest))
            for q in range(4):
                totals[4 * j + q, 0:32, :] = total[32 * q : 32 * q + 32].astype(jnp.bfloat16)
                totals[4 * j + q, 32:48, :] = tail.astype(jnp.bfloat16)

    totals_out = [wire.flag() for _ in range(groups)]
    totals_in, onward_out = wire.flag(), wire.flag()
    onward_in = [wire.flag() for _ in range(groups)]
    wire.sent.append((onward.at[pl.ds(0, 31)], onward_out))
    mine = lax.rem(me // (4 * tiles), groups)
    share = 32 // groups

    def each_of(g, act):
        @pl.when(mine == g)
        def _():
            act(share - 1)

        @pl.when(mine != g)
        def _():
            act(share)

    def disperse_totals(g):
        @pl.loop(0, 2 * tiles)
        def _(n):
            for q in range(4):
                to = 4 * tile_of(g, n) + q

                @pl.when(to != me)
                def _():
                    wire.go(
                        totals.at[to], stretch(to), totals_out[g], totals_in, arrived.at[me]
                    )

    total_up(0)
    disperse_totals(0)
    project((3,), (VALUE_SECOND,))

    @pl.loop(0, 4)
    def _(k):
        filtered(lax.rem(away + 7 + k, blocks), half // 2, half)

    prepare_states(away + 7, (1,))
    total_up(1)
    disperse_totals(1)
    arrived[me] = totals[me]

    g_second.finish()
    across("g", wg, "y", 2)

    def within(k):
        for g in range(groups):
            inner_product = dot_nt(
                outward[rows_of(k), g * STATE : (g + 1) * STATE],
                inward[rows_of(k), g * STATE : (g + 1) * STATE],
            )
            cells = signal[rows_of(k), g * span : (g + 1) * span]
            head_of = iota((BLOCK, span), 1) // HEAD_DIM
            weights, content = [], []
            for r in range(ratio):
                h = g * ratio + r
                below = column[rows_of(k), h : h + 1] + rowwise[k, h : h + 1, :]
                above = (
                    column[rows_of(k), heads + h : heads + h + 1]
                    + rowwise[k, heads + h : heads + h + 1, :]
                )
                decay = jnp.exp2(jnp.where(lower, below, above))
                both = jnp.where(
                    row == col, rowwise[k, 2 * heads + h : 2 * heads + h + 1, :], decay
                )
                weights.append((inner_product * both).astype(jnp.bfloat16))
                content.append(jnp.where(head_of == r, cells, jnp.zeros_like(cells)))
            inner[rows_of(k), g * span : (g + 1) * span] = dot(
                jnp.concatenate(weights, axis=1), jnp.concatenate(content, axis=0)
            )

    lo_second.forward()
    hi_second.forward()
    for by in (3, 1):
        across("o", wo, "z", by, (0, 2))
        across("o", wo, "y", by, (2, 2))

    project((3,), (OUTWARD,))

    @pl.loop(0, 4)
    def _(k):
        filtered(lax.rem(away + 7 + k, blocks), half + lead, wide)


    @pl.loop(0, blocks // 2)
    def _(k):
        within(k)

    wire.landed(arrived.at[pl.ds(0, 31)], totals_in)

    flip = me >= 16

    def hop(k, state):
        at = jnp.where(flip, 31 - k, k)
        onward[at] = state.astype(jnp.bfloat16)
        message = arrived[at].astype(jnp.float32)
        decay = message[32:33] + message[33:34] + message[34:35]
        return state * decay + message[0:32]

    lax.fori_loop(0, 32, hop, jnp.zeros((32, 128), jnp.float32))

    for g in range(groups):

        @pl.when(mine == g)
        def _():
            @pl.loop(0, 31)
            def _(k):
                to = lax.rem(me + lax.rem(k + 15, 31) + 1, 32)
                wire.go(onward.at[to], stretch(to), onward_out, onward_in[g], incoming.at[me])


    incoming[me] = onward[me]

    crossed("g", wg)
    project_gate((0, 1, 2))
    project_gate((3,))

    @pl.loop(blocks // 2, blocks)
    def _(k):
        within(k)

    spread_read = spread(1).astype(jnp.bfloat16)

    def carry(g):
        each_of(g, lambda n: wire.landed(incoming.at[pl.ds(0, n)], onward_in[g]))

        @pl.loop(0, 2 * tiles)
        def _(n):
            j = tile_of(g, n)
            lanes = pl.ds(pl.multiple_of(j * 128, 128), 128)
            backward = n >= tiles
            state = jnp.concatenate([incoming[4 * j + q] for q in range(4)], axis=0).astype(
                jnp.float32
            )
            for k in range(blocks):
                at = jnp.where(backward, blocks - 1 - k, k)
                before[at, :, lanes] = state.astype(jnp.bfloat16)
                state = state * decays[at, 0:1, lanes] + states[at, :, lanes]

    def finish(k, g):
        lanes = slice(g * span, (g + 1) * span)
        read = outward[rows_of(k), g * STATE : (g + 1) * STATE]
        scale = column[rows_of(k), :].astype(jnp.bfloat16)
        total = inner[rows_of(k), lanes]
        for way in range(2):
            placed = slice(way * half + g * span, way * half + (g + 1) * span)
            total = total + dot(read, before[k, :, placed]) * dot(scale, spread_read[:, placed])
        gated = total * gates[rows_of(k), lanes].astype(jnp.float32)
        level = lax.rsqrt(jnp.mean(gated * gated, axis=-1, keepdims=True) + EPSILON)
        mixed[rows_of(k), lanes] = (gated * level * gain_ref[:, lanes]).astype(jnp.bfloat16)

    def finish_shard(shard, g):
        @pl.loop(0, 2)
        def _(b):
            finish(2 * shard + b, g)

    def lanes_of(g):
        return pl.ds(g * span, span)

    def part(shard, some, g):
        start, size = some
        return mixed.at[
            pl.ds(pl.multiple_of(shard * rows + start, middle), size), lanes_of(g)
        ]

    mixed_out, from_below, from_above, from_far = [wire.flag() for _ in range(4)]
    relayed = [wire.flag() for _ in range(groups)]
    wire.sent.append((shards, mixed_out))

    def hand_on(g):
        wire.landed(relay.at[:, :, lanes_of(g)], relayed[g])
        for half_at, to, target in (
            (0, up, shards.at[step(x, 3), low, lanes_of(g)]),
            (1, down, shards.at[step(x, 1), high, lanes_of(g)]),
        ):
            wire.go(relay.at[half_at, :, lanes_of(g)], to, mixed_out, from_far, target)

    for g in range(groups):
        carry(g)
        for half_at, to in ((0, up), (1, down)):
            finish(2 * step(x, 2) + half_at, g)
            wire.go(
                part(step(x, 2), (half_at * middle, middle), g),
                to,
                mixed_out,
                relayed[g],
                relay.at[half_at, :, lanes_of(g)],
            )
        for by, to, flag in ((1, up, from_below), (3, down, from_above)):
            finish_shard(step(x, by), g)
            wire.go(
                part(step(x, by), (0, rows), g), to, mixed_out, flag, shards.at[x, :, lanes_of(g)]
            )
        if g == 0:
            lo_second.finish()
            across("o", wo, "z", 2, (0, 2))
            hi_second.finish()
            across("o", wo, "y", 2, (2, 2))
        finish_shard(x, g)
        if g:
            hand_on(g - 1)
    shards[x] = mixed[pl.ds(pl.multiple_of(x * rows, rows), rows), :]
    hand_on(groups - 1)
    crossed("o", wo)

    def contribute(at, begin, end):
        @pl.loop(0, 2)
        def _(k):
            lines = pl.ds(pl.multiple_of(k * 1024, 1024), 1024)
            total = dot_nt(wo[pl.ds(2 * k, 2), :, :, at].reshape(1024, -1), shards[at])
            if not begin:
                total = total + summed[lines, :]
            if end:
                out_ref[:, lines] = total.T.astype(out_ref.dtype)
            else:
                summed[lines, :] = total

    contribute(x, True, False)
    wire.landed(shards.at[0], from_below)
    contribute(step(x, 3), False, False)
    wire.landed(shards.at[0], from_above)
    contribute(step(x, 1), False, False)
    wire.landed(shards.at[0], from_far)
    contribute(step(x, 2), False, True)

    wire.drain()
    for g in range(groups):
        each_of(g, lambda n: wire.span(totals.at[pl.ds(0, n)], totals_out[g]).wait_send())


FLAGS = 60


def mix(
    tokens,
    norm_gain,
    w_gate,
    w_value,
    w_state_in,
    w_state_out,
    w_step_forward,
    w_step_backward,
    step_offset,
    fading_speed,
    conv_value,
    conv_state_in,
    conv_state_out,
    out_gain,
    w_out,
):
    rows, width = tokens.shape
    depth, half = w_value.shape
    states = w_state_in.shape[1]
    blocks = 4 * rows // BLOCK
    anywhere = pl.BlockSpec(memory_space=pl.ANY)
    bf16, f32 = jnp.bfloat16, jnp.float32
    return pl.pallas_call(
        functools.partial(mixer_kernel, math.log(4 * rows * lax.axis_size(SP))),
        out_shape=pltpu.VMEM((rows, width), OUT_TYPE),
        in_specs=[anywhere] * 15,
        out_specs=pl.BlockSpec(memory_space=pltpu.VMEM),
        scratch_shapes=[
            pltpu.VMEM((1, width), f32),
            pltpu.VMEM(w_step_forward.shape[::-1], bf16),
            pltpu.VMEM(w_step_backward.shape[::-1], bf16),
            pltpu.VMEM(conv_value.shape, f32),
            pltpu.VMEM(conv_state_in.shape, f32),
            pltpu.VMEM(conv_state_out.shape, f32),
            pltpu.VMEM(step_offset.shape, f32),
            pltpu.VMEM(fading_speed.shape, f32),
            pltpu.VMEM((1, half), f32),
            pltpu.VMEM((16, 128), f32),
            pltpu.VMEM((rows, 128), f32),
            pltpu.VMEM((blocks, 8, 128), f32),
            pltpu.VMEM((4, rows, width), bf16),
            pltpu.VMEM((2 * HALO, width), bf16),
            pltpu.VMEM((4 * rows + 2 * HALO, width), bf16),
            pltpu.VMEM((4, 4, 2, depth, half), bf16),
            pltpu.VMEM((4, 4, 2, depth, 2 * states + 128), bf16),
            pltpu.VMEM((4, 4, 2, depth, half), bf16),
            pltpu.VMEM((4, 4, 2, 4, depth, half), bf16),
            pltpu.VMEM((4 * rows + 2 * HALO, 2 * half), bf16),
            pltpu.VMEM((4 * rows, half), bf16),
            pltpu.VMEM((4 * rows, 128), bf16),
            pltpu.VMEM((4 * rows, half), bf16),
            pltpu.VMEM((4 * rows, states), bf16),
            pltpu.VMEM((4 * rows, states), bf16),
            pltpu.VMEM((4 * rows, 128), f32),
            pltpu.VMEM((blocks, 24, 128), f32),
            pltpu.VMEM((blocks, STATE, 2 * half), f32),
            pltpu.VMEM((blocks, 8, 2 * half), f32),
            pltpu.VMEM((blocks, STATE, 2 * half), bf16),
            pltpu.VMEM((4 * rows, half), f32),
            pltpu.VMEM((32, 48, 128), bf16),
            pltpu.VMEM((32, 48, 128), bf16),
            pltpu.VMEM((32, 32, 128), bf16),
            pltpu.VMEM((32, 32, 128), bf16),
            pltpu.VMEM((4 * rows, half), bf16),
            pltpu.VMEM((4, rows, half), bf16),
            pltpu.VMEM((2, rows // 2, half), bf16),
            pltpu.VMEM((width, rows), f32),
            pltpu.SemaphoreType.DMA((FLAGS,)),
            pltpu.SemaphoreType.DMA((15,)),
        ],
        compiler_params=pltpu.CompilerParams(
            collective_id=0, has_side_effects=True, vmem_limit_bytes=60 * 2**20
        ),
        name="mixer",
    )(
        tokens,
        w_value,
        w_state_in,
        w_state_out,
        w_gate,
        w_out.T,
        norm_gain.reshape(1, -1),
        w_step_forward.T,
        w_step_backward.T,
        conv_value,
        conv_state_in,
        conv_state_out,
        step_offset,
        fading_speed,
        out_gain.reshape(1, -1),
    )


OUT_TYPE = jnp.bfloat16


def local(
    input_activations,
    norm_gain,
    w_gate,
    w_value,
    w_state_in,
    w_state_out,
    w_step_forward,
    w_step_backward,
    step_offset,
    fading_speed,
    conv_value,
    conv_state_in,
    conv_state_out,
    out_gain,
    w_out,
):
    return mix(
        input_activations,
        norm_gain,
        w_gate,
        w_value,
        w_state_in,
        w_state_out,
        w_step_forward,
        w_step_backward,
        step_offset,
        fading_speed,
        conv_value,
        conv_state_in,
        conv_state_out,
        out_gain,
        w_out,
    )


def solution(mesh):
    torus = Mesh(mesh.devices.reshape(4, 4, 2, 4), SP_TP)
    return jax.shard_map(
        local,
        mesh=torus,
        in_specs=(
            P(SP_TP, None),
            P(),
            P(SP, "x"),
            P(SP, "x"),
            P(SP, "x"),
            P(SP, "x"),
            P(SP, "x"),
            P(SP, "x"),
            P(None, "x"),
            P(None, "x"),
            P(None, "x"),
            P(None, "x"),
            P(None, "x"),
            P("x"),
            P("x", SP),
        ),
        out_specs=P(SP_TP, None),
        check_vma=False,
    )
```

```python
import functools
import math

import jax
import jax.numpy as jnp
from jax import lax
from jax.experimental import pallas as pl
from jax.experimental.pallas import tpu as pltpu
from jax.sharding import Mesh
from jax.sharding import PartitionSpec as P

HEAD_DIM = 64
STATE = 128
BLOCK = 128
SP = ("z", "y", "c")
SP_TP = ("z", "y", "c", "x")
EPSILON = 1e-06
MESH = pl.DeviceIdType.MESH
VALUE, INWARD, OUTWARD, STEPS, VALUE_FIRST, VALUE_SECOND = range(6)
HALO = 16


def place():
    return [lax.axis_index(name) for name in ("z", "y", "c", "x")]


def step(at, by):
    return lax.rem(at + by + 4, 4)


def stretch_at(z, y, c, by):
    n = lax.rem(z * 8 + y * 2 + c + by + 32, 32)
    return {"z": n // 8, "y": lax.rem(n // 2, 4), "c": lax.rem(n, 2)}


class Wire:
    def __init__(self, flags, self_free):
        self.flags, self.count, self.to, self.sent = flags, 0, self_free, []

    def flag(self):
        self.count += 1
        return self.flags.at[self.count - 1]

    def go(self, source, to, send, recv, target=None):
        pltpu.make_async_remote_copy(
            src_ref=source,
            dst_ref=source if target is None else target,
            send_sem=send,
            recv_sem=recv,
            device_id=to,
            device_id_type=MESH,
        ).start()

    def span(self, ref, flag):
        return pltpu.make_async_remote_copy(
            src_ref=ref,
            dst_ref=ref,
            send_sem=flag,
            recv_sem=flag,
            device_id=self.to,
            device_id_type=MESH,
        )

    def landed(self, ref, flag):
        self.span(ref, flag).wait_recv()

    def drain(self):
        for ref, flag in self.sent:
            self.span(ref, flag).wait_send()


class Ring:
    def __init__(self, wire, axis, at, block, low, high, many):
        self.wire, self.at = wire, at
        self.up, self.down = {axis: step(at, 1)}, {axis: step(at, 3)}
        self.block, self.low, self.high, self.many = block, low, high, many
        self.out, self.near, self.away = wire.flag(), wire.flag(), wire.flag()
        wire.sent.append((many(3), self.out))

    def start(self):
        self.wire.go(self.block(self.at), self.up, self.out, self.near)
        self.wire.go(self.block(self.at), self.down, self.out, self.near)

    def forward(self):
        self.wire.landed(self.many(2), self.near)
        self.wire.go(self.low(step(self.at, 3)), self.up, self.out, self.away)
        self.wire.go(self.high(step(self.at, 1)), self.down, self.out, self.away)

    def finish(self):
        self.wire.landed(self.many(1), self.away)


LOG2E = 1.4426950408889634


def dot_nt(a, b):
    return lax.dot_general(a, b, (((1,), (1,)), ((), ())), preferred_element_type=jnp.float32)


def dot_tn(a, b):
    return lax.dot_general(a, b, (((0,), (0,)), ((), ())), preferred_element_type=jnp.float32)


def dot(a, b, precision=None):
    return lax.dot_general(
        a, b, (((1,), (0,)), ((), ())), precision=precision, preferred_element_type=jnp.float32
    )


def iota(shape, dim):
    return lax.broadcasted_iota(jnp.int32, shape, dim)


def silu(v):
    part = 0.5 * v
    return part + part * jnp.tanh(part)


def mixer_kernel(
    shift,
    tokens_hbm,
    value_hbm,
    state_in_hbm,
    state_out_hbm,
    gate_hbm,
    w_out_hbm,
    norm_gain_hbm,
    step_forward_hbm,
    step_backward_hbm,
    tap_value_hbm,
    tap_in_hbm,
    tap_out_hbm,
    offset_hbm,
    speed_hbm,
    gain_hbm,
    out_ref,
    norm_gain_ref,
    step_forward_ref,
    step_backward_ref,
    tap_value_ref,
    tap_in_ref,
    tap_out_ref,
    offset_ref,
    speed_ref,
    gain_ref,
    heads_ref,
    squares,
    fades,
    tokens,
    edges,
    normed,
    wv,
    ws,
    wg,
    wo,
    projected,
    gates,
    raw,
    signal,
    inward,
    outward,
    column,
    rowwise,
    states,
    decays,
    before,
    inner,
    totals,
    arrived,
    onward,
    incoming,
    mixed,
    shards,
    relay,
    summed,
    flags,
    local_sem,
):
    z, y, c, x = place()
    me = z * 8 + y * 2 + c
    wire = Wire(flags, {"c": 1 - c})
    rows = tokens.shape[1]
    middle = rows // 2
    count = 4 * rows
    blocks = count // BLOCK
    half = signal.shape[1]
    wide = 2 * half
    groups = inward.shape[1] // STATE
    ratio = half // HEAD_DIM // groups
    heads = groups * ratio
    span = ratio * HEAD_DIM
    lead = inward.shape[1]
    partner = {"c": 1 - c}

    def stretch(n):
        return {"z": n // 8, "y": lax.rem(n // 2, 4), "c": lax.rem(n, 2)}

    own = [
        pltpu.make_async_copy(tokens_hbm, tokens.at[x], local_sem.at[0]),
        pltpu.make_async_copy(value_hbm, wv.at[z, y, c], local_sem.at[1]),
        pltpu.make_async_copy(state_in_hbm, ws.at[z, y, c, :, pl.ds(0, lead)], local_sem.at[2]),
        pltpu.make_async_copy(state_out_hbm, ws.at[z, y, c, :, pl.ds(lead, lead)], local_sem.at[3]),
        pltpu.make_async_copy(gate_hbm, wg.at[z, y, c], local_sem.at[4]),
        pltpu.make_async_copy(w_out_hbm, wo.at[z, y, c, x], local_sem.at[5]),
    ]
    small = (
        (step_forward_hbm, step_forward_ref),
        (step_backward_hbm, step_backward_ref),
        (offset_hbm, offset_ref),
        (speed_hbm, speed_ref),
        (norm_gain_hbm, norm_gain_ref),
        (tap_value_hbm, tap_value_ref),
        (tap_in_hbm, tap_in_ref),
        (tap_out_hbm, tap_out_ref),
        (gain_hbm, gain_ref),
    )
    own += [
        pltpu.make_async_copy(source, target, local_sem.at[6 + k])
        for k, (source, target) in enumerate(small)
    ]
    for copy in own:
        copy.start()
    barrier = pltpu.get_barrier_semaphore()

    near = [{axis: step(at, by)} for axis, at in (("x", x), ("y", y), ("z", z)) for by in (1, 3)]
    for other in near + [partner]:
        pl.semaphore_signal(barrier, inc=1, device_id=other, device_id_type=MESH)
    for copy in own:
        copy.wait()
    depth = step_forward_ref.shape[1]
    steps = jnp.concatenate(
        [
            step_forward_ref[...].astype(jnp.float32),
            step_backward_ref[...].astype(jnp.float32),
            jnp.zeros((128 - 2 * heads, depth), jnp.float32),
        ],
        axis=0,
    )
    steps = jnp.concatenate([steps, jnp.zeros((128, 128 - depth), jnp.float32)], axis=1).T
    ws[z, y, c, :, 2 * lead :] = steps[0:depth].astype(jnp.bfloat16)
    lines = jnp.concatenate(
        [
            jnp.concatenate([ref[w : w + 1, :] * sign for w in range(2)], axis=1)
            for ref, sign in ((offset_ref, 1.0), (speed_ref, -1.0))
        ],
        axis=0,
    )
    lines = jnp.concatenate([lines, jnp.zeros((2, 128 - 2 * heads), jnp.float32)], axis=1)
    heads_ref[...] = jnp.concatenate([lines, jnp.zeros((126, 128), jnp.float32)], axis=0).T[
        0 : 2 * heads
    ]
    pl.semaphore_wait(barrier, 7)

    wo_x = Ring(
        wire,
        "x",
        x,
        lambda at: wo.at[z, y, c, at],
        lambda at: wo.at[z, y, c, at, pl.ds(0, 32)],
        lambda at: wo.at[z, y, c, at, pl.ds(32, 32)],
        lambda n: wo.at[z, y, c, pl.ds(0, n)],
    )
    wo_x.start()

    low, high = pl.ds(0, middle), pl.ds(middle, middle)
    up, down = {"x": step(x, 1)}, {"x": step(x, 3)}
    tokens_out, first_half, second_half = wire.flag(), wire.flag(), wire.flag()
    far_ends, far_rest = wire.flag(), wire.flag()
    wire.sent.append((tokens.at[pl.ds(0, 3)], tokens_out))
    wire.go(tokens.at[x, low], up, tokens_out, first_half)
    wire.go(tokens.at[x, high], down, tokens_out, first_half)

    def first(buffer, axis, keep=()):
        def at(n, part):
            spot = (z, n, c) if axis == "y" else (n, y, c)
            if keep:
                start, size = keep
                return buffer.at[(*spot, pl.ds(start, size) if part is None else start + part)]
            return buffer.at[spot] if part is None else buffer.at[(*spot, pl.ds(32 * part, 32))]

        here = y if axis == "y" else z

        def many(n):
            spot = (z, pl.ds(0, n), c) if axis == "y" else (pl.ds(0, n), y, c)
            return buffer.at[(*spot, pl.ds(*keep))] if keep else buffer.at[spot]

        return Ring(
            wire, axis, here, lambda n: at(n, None), lambda n: at(n, 0), lambda n: at(n, 1), many
        )

    def group(buffer, axis, n, part, keep):
        some = pl.ds(0, 4) if part is None else pl.ds(2 * part, 2)
        spot = (n, some, c) if axis == "z" else (some, n, c)
        return buffer.at[(*spot, pl.ds(*keep))] if keep else buffer.at[spot]

    def second(buffer, axis, keep=()):
        here = y if axis == "y" else z
        return Ring(
            wire,
            axis,
            here,
            lambda n: group(buffer, axis, n, None, keep),
            lambda n: group(buffer, axis, n, 0, keep),
            lambda n: group(buffer, axis, n, 1, keep),
            lambda n: group(buffer, axis, pl.ds(0, n), None, keep),
        )

    pairs = {}
    for name, buffer in (("v", wv), ("s", ws), ("g", wg), ("o", wo)):
        pairs[name] = wire.flag(), wire.flag()
        wire.sent.append((buffer.at[:, :, 1 - c], pairs[name][0]))

    def across(name, buffer, axis, by, keep=()):
        here = y if axis == "y" else z
        wire.go(group(buffer, axis, step(here, by), None, keep), partner, *pairs[name])

    def crossed(name, buffer):
        wire.landed(buffer.at[:, :, 1 - c], pairs[name][1])

    v_first, s_first = first(wv, "y"), first(ws, "z")
    v_first.start()
    s_first.start()

    def main_row(shard):
        return HALO + shard * rows

    def normalize(ref, size, to):
        width = ref.shape[-1]

        @pl.loop(0, size // 32, unroll=2)
        def _(k):
            taken = pl.ds(pl.multiple_of(k * 32, 32), 32)
            cells = ref[taken, :].astype(jnp.float32)
            total = cells[:, 0:128] * cells[:, 0:128]
            for at in range(128, width, 128):
                total = total + cells[:, at : at + 128] * cells[:, at : at + 128]
            squares[taken, :] = total

        level = lax.rsqrt(
            jnp.sum(squares[0:size, :], axis=-1, keepdims=True) * (1.0 / width) + EPSILON
        )
        squares[0:size, :] = jnp.broadcast_to(level, (size, 128))

        @pl.loop(0, size // 32, unroll=2)
        def _(k):
            taken = pl.ds(pl.multiple_of(k * 32, 32), 32)
            scale = squares[taken, :]
            cells = ref[taken, :].astype(jnp.float32)
            placed = pl.ds(pl.multiple_of(to + k * 32, 16), 32)
            for at in range(0, width, 128):
                normed[placed, at : at + 128] = (
                    cells[:, at : at + 128] * scale * norm_gain_ref[:, at : at + 128]
                ).astype(jnp.bfloat16)

    shard_in = (x, step(x, 3), step(x, 1), step(x, 2))

    def project(slots, parts):
        edge = not slots
        begin, size = (slots[0] * rows, len(slots) * rows) if slots else (4 * rows, 2 * HALO)
        taken = pl.ds(begin, size)

        def put(values, columns):
            for k, slot in enumerate(slots):
                placed = pl.ds(pl.multiple_of(main_row(shard_in[slot]), 16), rows)
                projected[placed, columns] = values[k * rows : (k + 1) * rows]
            if edge:
                projected[0:HALO, columns] = jnp.where(me > 0, values[0:HALO], 0).astype(
                    values.dtype
                )
                projected[main_row(4) : main_row(4) + HALO, columns] = jnp.where(
                    me < 31, values[HALO:], 0
                ).astype(values.dtype)

        def product(weights, columns):
            return dot(normed[taken, :], weights[:, :, :, :, columns].reshape(-1, 256)).astype(
                jnp.bfloat16
            )

        if VALUE in parts:

            @pl.loop(0, half // 256)
            def _(k):
                columns = pl.ds(pl.multiple_of(k * 256, 256), 256)
                put(product(wv, columns), columns)

        for name, start in ((VALUE_FIRST, 0), (VALUE_SECOND, half // 2)):
            if name in parts:
                columns = slice(start, start + half // 2)
                put(product(wv, columns), columns)
        if INWARD in parts:
            put(product(ws, slice(0, lead)), slice(half, half + lead))
        if OUTWARD in parts:
            put(product(ws, slice(lead, 2 * lead)), slice(half + lead, wide))
        if STEPS in parts:
            values = dot(normed[taken, :], ws[:, :, :, :, 2 * lead :].reshape(-1, 128)).astype(
                jnp.bfloat16
            )
            for k, slot in enumerate(slots):
                placed = pl.ds(pl.multiple_of(shard_in[slot] * rows, rows), rows)
                raw[placed, :] = values[k * rows : (k + 1) * rows]

    def project_gate(slots):
        taken = pl.ds(slots[0] * rows, len(slots) * rows)

        @pl.loop(0, half // 256)
        def _(k):
            columns = pl.ds(pl.multiple_of(k * 256, 256), 256)
            values = dot(normed[taken, :], wg[:, :, :, :, columns].reshape(-1, 256))
            values = silu(values.astype(jnp.bfloat16).astype(jnp.float32)).astype(jnp.bfloat16)
            for k, slot in enumerate(slots):
                placed = pl.ds(pl.multiple_of(shard_in[slot] * rows, rows), rows)
                gates[placed, columns] = values[k * rows : (k + 1) * rows]

    normalize(tokens.at[x], rows, 0)

    v_first.forward()
    wo_x.forward()
    wire.go(tokens.at[x, high], up, tokens_out, second_half)
    wire.go(tokens.at[x, low], down, tokens_out, second_half)
    s_first.forward()
    v_first.finish()
    v_second = second(wv, "z")
    v_second.start()
    across("v", wv, "z", 0)
    s_first.finish()
    s_second = second(ws, "y")
    s_second.start()
    across("s", ws, "y", 0)
    g_first = first(wg, "z")
    g_first.start()

    wire.landed(tokens.at[0], first_half)
    for by, start, to, flag in (
        (3, (0, HALO), up, far_ends),
        (1, (rows - HALO, HALO), down, far_ends),
        (3, (HALO, middle - HALO), up, far_rest),
        (1, (middle, middle - HALO), down, far_rest),
    ):
        wire.go(tokens.at[step(x, by), pl.ds(*start)], to, tokens_out, flag)
    wo_x.finish()
    lo_first, hi_first = first(wo, "y", (0, 2)), first(wo, "z", (2, 2))
    lo_first.start()
    hi_first.start()
    normalize(tokens.at[step(x, 3), low], middle, rows)
    normalize(tokens.at[step(x, 1), high], middle, 2 * rows + middle)

    v_second.forward()
    s_second.forward()
    for by in (3, 1):
        across("v", wv, "z", by)
        across("s", ws, "y", by)
    g_first.forward()
    v_second.finish()
    across("v", wv, "z", 2)
    s_second.finish()
    across("s", ws, "y", 2)
    g_first.finish()
    g_second = second(wg, "y")
    g_second.start()
    across("g", wg, "y", 0)
    lo_first.forward()
    hi_first.forward()
    crossed("v", wv)
    crossed("s", ws)
    project((0,), (VALUE, INWARD, OUTWARD, STEPS))

    wire.landed(tokens.at[0], second_half)
    normalize(tokens.at[step(x, 3), high], middle, rows + middle)
    normalize(tokens.at[step(x, 1), low], middle, 2 * rows)
    wire.landed(edges, far_ends)
    edge_out, edge_in = wire.flag(), wire.flag()
    wire.sent.append((edges, edge_out))
    for slot, (shard, offset, by) in enumerate(((3, rows - HALO, 1), (0, 0, 31))):
        wire.go(
            tokens.at[shard, pl.ds(offset, HALO)],
            stretch_at(z, y, c, by),
            edge_out,
            edge_in,
            edges.at[pl.ds(slot * HALO, HALO)],
        )
    lo_first.finish()
    lo_second = second(wo, "z", (0, 2))
    lo_second.start()
    across("o", wo, "z", 0, (0, 2))
    hi_first.finish()
    hi_second = second(wo, "y", (2, 2))
    hi_second.start()
    across("o", wo, "y", 0, (2, 2))
    project((1, 2), (VALUE, INWARD, OUTWARD, STEPS))
    g_second.forward()
    across("g", wg, "y", 3)
    across("g", wg, "y", 1)
    wire.landed(edges, edge_in)
    normalize(edges, 2 * HALO, 4 * rows)
    project((), (VALUE, INWARD, OUTWARD))

    row, col = iota((BLOCK, BLOCK), 0), iota((BLOCK, BLOCK), 1)
    lower = row >= col
    triangle = jnp.where(row <= col, 1.0, 0.0)

    def spread(kind):
        place_of = iota((128, wide), 1) // HEAD_DIM + 2 * heads * kind
        return jnp.where(place_of == iota((128, wide), 0), 1.0, 0.0)

    spread_weight = spread(2).astype(jnp.bfloat16)

    def rows_of(k):
        return pl.ds(pl.multiple_of(k * BLOCK, BLOCK), BLOCK)

    def filtered(k, begin, end):
        window = pl.ds(pl.multiple_of(k * BLOCK, BLOCK), BLOCK + 2 * HALO)
        for at in range(begin, end, 128):
            if at < half:
                tap_ref, target, start = tap_value_ref, signal, at
            elif at < half + lead:
                tap_ref, target, start = tap_in_ref, inward, at - half
            else:
                tap_ref, target, start = tap_out_ref, outward, at - half - lead
            cells = projected[window, at : at + 128].astype(jnp.float32)
            tap = tap_ref[:, start : start + 128]
            here = slice(HALO, HALO + BLOCK)
            total = (
                tap[0:1] * pltpu.roll(cells, 1, 0)[here]
                + tap[1:2] * cells[here]
                + tap[2:3] * pltpu.roll(cells, BLOCK + 2 * HALO - 1, 0)[here]
            )
            target[rows_of(k), start : start + 128] = silu(total).astype(jnp.bfloat16)

    def four(first_block):
        return [lax.rem(first_block + n, blocks) for n in range(4)]

    def prepare_steps(first_block):
        some = four(first_block)
        both = 2 * heads
        forward_row = lax.rem(iota((4 * both, BLOCK), 0), both) < heads
        size = jax.nn.softplus(
            jnp.concatenate(
                [raw[rows_of(k), :].astype(jnp.float32).T[0:both] for k in some], axis=0
            )
            + jnp.concatenate([heads_ref[:, 0:1]] * 4, axis=0)
            - shift
        )
        logs = size * jnp.concatenate([heads_ref[:, 1:2]] * 4, axis=0)
        through = dot(logs, triangle, lax.Precision.HIGHEST)
        until = through - logs
        whole = through[:, BLOCK - 1 : BLOCK]
        logsize = jnp.log(size)
        lines = jnp.where(forward_row, logsize - through, logsize + until) * LOG2E
        kinds = (
            jnp.where(forward_row, through, -until) * LOG2E,
            jnp.exp(jnp.where(forward_row, through, whole - until)),
            size * jnp.exp(jnp.where(forward_row, whole - through, until)),
            jnp.broadcast_to(jnp.exp(whole), (4 * both, BLOCK)),
        )
        for n, k in enumerate(some):
            own_rows = slice(n * both, (n + 1) * both)
            rowwise[k, 0:both, :] = lines[own_rows]
            rowwise[k, both : both + heads, :] = (
                size[n * both : n * both + heads] + size[n * both + heads : (n + 1) * both]
            )
            block = jnp.concatenate(
                [kind[own_rows] for kind in kinds]
                + [jnp.zeros((128 - 4 * both, BLOCK), jnp.float32)],
                axis=0,
            ).T
            column[rows_of(k), :] = block
            fades[k] = block[0:8]

    def prepare_states(first_block, chosen):
        some = four(first_block)
        turned = jnp.concatenate(
            [column[rows_of(k), :].astype(jnp.bfloat16) for k in some], axis=0
        )
        for g in chosen:
            across_in = [
                inward[rows_of(k), g * STATE : (g + 1) * STATE].astype(jnp.float32).T.astype(
                    jnp.bfloat16
                )
                for k in some
            ]
            cells = jnp.concatenate(
                [signal[rows_of(k), g * span : (g + 1) * span] for k in some], axis=0
            )
            for way in range(2):
                placed = slice(way * half + g * span, way * half + (g + 1) * span)
                content = (
                    cells.astype(jnp.float32) * dot(turned, spread_weight[:, placed])
                ).astype(jnp.bfloat16)
                for n, k in enumerate(some):
                    states[k, :, placed] = dot(
                        across_in[n], content[n * BLOCK : (n + 1) * BLOCK]
                    )

    away = 2 * step(x, 2)

    @pl.loop(0, 4)
    def _(k):
        filtered(lax.rem(away + 3 + k, blocks), 0, half + lead)

    prepare_steps(away + 3)
    prepare_states(away + 3, (0,))

    wire.landed(tokens.at[0, pl.ds(0, rows - 2 * HALO)], far_rest)
    normalize(tokens.at[step(x, 2)], rows, 3 * rows)
    project((3,), (STEPS, INWARD, VALUE_FIRST))

    @pl.loop(0, 4)
    def _(k):
        filtered(lax.rem(away + 7 + k, blocks), 0, half // 2)
        filtered(lax.rem(away + 7 + k, blocks), half, half + lead)

    prepare_steps(away + 7)
    over = dot(
        jnp.concatenate([fades[k, 0:1, :] for k in range(blocks)], axis=0),
        spread(3),
        lax.Precision.HIGHEST,
    )
    for k in range(blocks):
        decays[k] = jnp.broadcast_to(over[k : k + 1], (8, wide))
    prepare_states(away + 7, (0,))

    tiles = span // 128
    ways = half // 128

    def tile_of(g, n):
        return n // tiles * ways + g * tiles + lax.rem(n, tiles)

    def total_up(g):
        @pl.loop(0, 2 * tiles)
        def _(n):
            j = tile_of(g, n)
            lanes = pl.ds(pl.multiple_of(j * 128, 128), 128)
            backward = n >= tiles
            total = jnp.zeros((STATE, 128), jnp.float32)
            decay = jnp.ones((1, 128), jnp.float32)
            for k in range(blocks):
                at = jnp.where(backward, blocks - 1 - k, k)
                part = decays[at, 0:1, lanes]
                total = total * part + states[at, :, lanes]
                decay = decay * part
            upper = decay.astype(jnp.bfloat16).astype(jnp.float32)
            centre = (decay - upper).astype(jnp.bfloat16).astype(jnp.float32)
            rest = decay - upper - centre
            place_row = iota((16, 128), 0)
            tail = jnp.where(place_row == 0, upper, jnp.where(place_row == 1, centre, rest))
            for q in range(4):
                totals[4 * j + q, 0:32, :] = total[32 * q : 32 * q + 32].astype(jnp.bfloat16)
                totals[4 * j + q, 32:48, :] = tail.astype(jnp.bfloat16)

    totals_out = [wire.flag() for _ in range(groups)]
    totals_in, onward_out = wire.flag(), wire.flag()
    onward_in = [wire.flag() for _ in range(groups)]
    wire.sent.append((onward.at[pl.ds(0, 31)], onward_out))
    mine = lax.rem(me // (4 * tiles), groups)
    share = 32 // groups

    def each_of(g, act):
        @pl.when(mine == g)
        def _():
            act(share - 1)

        @pl.when(mine != g)
        def _():
            act(share)

    def disperse_totals(g):
        @pl.loop(0, 2 * tiles)
        def _(n):
            for q in range(4):
                to = 4 * tile_of(g, n) + q

                @pl.when(to != me)
                def _():
                    wire.go(
                        totals.at[to], stretch(to), totals_out[g], totals_in, arrived.at[me]
                    )

    total_up(0)
    disperse_totals(0)
    project((3,), (VALUE_SECOND,))

    @pl.loop(0, 4)
    def _(k):
        filtered(lax.rem(away + 7 + k, blocks), half // 2, half)

    prepare_states(away + 3, (1,))
    prepare_states(away + 7, (1,))
    total_up(1)
    disperse_totals(1)
    arrived[me] = totals[me]


    def within(k):
        for g in range(groups):
            inner_product = dot_nt(
                outward[rows_of(k), g * STATE : (g + 1) * STATE],
                inward[rows_of(k), g * STATE : (g + 1) * STATE],
            )
            cells = signal[rows_of(k), g * span : (g + 1) * span]
            head_of = iota((BLOCK, span), 1) // HEAD_DIM
            weights, content = [], []
            for r in range(ratio):
                h = g * ratio + r
                below = column[rows_of(k), h : h + 1] + rowwise[k, h : h + 1, :]
                above = (
                    column[rows_of(k), heads + h : heads + h + 1]
                    + rowwise[k, heads + h : heads + h + 1, :]
                )
                decay = jnp.exp2(jnp.where(lower, below, above))
                both = jnp.where(
                    row == col, rowwise[k, 2 * heads + h : 2 * heads + h + 1, :], decay
                )
                weights.append((inner_product * both).astype(jnp.bfloat16))
                content.append(jnp.where(head_of == r, cells, jnp.zeros_like(cells)))
            inner[rows_of(k), g * span : (g + 1) * span] = dot(
                jnp.concatenate(weights, axis=1), jnp.concatenate(content, axis=0)
            )

    project((3,), (OUTWARD,))

    @pl.loop(0, blocks)
    def _(k):
        filtered(k, half + lead, wide)


    @pl.loop(0, blocks // 2)
    def _(k):
        within(k)

    wire.landed(arrived.at[pl.ds(0, 31)], totals_in)

    flip = me >= 16

    def hop(k, state):
        at = jnp.where(flip, 31 - k, k)
        onward[at] = state.astype(jnp.bfloat16)
        message = arrived[at].astype(jnp.float32)
        decay = message[32:33] + message[33:34] + message[34:35]
        return state * decay + message[0:32]

    lax.fori_loop(0, 32, hop, jnp.zeros((32, 128), jnp.float32))

    for g in range(groups):

        @pl.when(mine == g)
        def _():
            @pl.loop(0, 31)
            def _(k):
                to = lax.rem(me + lax.rem(k + 15, 31) + 1, 32)
                wire.go(onward.at[to], stretch(to), onward_out, onward_in[g], incoming.at[me])


    incoming[me] = onward[me]

    g_second.finish()
    across("g", wg, "y", 2)

    @pl.loop(blocks // 2, blocks)
    def _(k):
        within(k)

    lo_second.forward()
    hi_second.forward()
    for by in (3, 1):
        across("o", wo, "z", by, (0, 2))
        across("o", wo, "y", by, (2, 2))

    crossed("g", wg)
    project_gate((0, 1, 2))
    project_gate((3,))

    spread_read = spread(1).astype(jnp.bfloat16)

    def carry(g):
        each_of(g, lambda n: wire.landed(incoming.at[pl.ds(0, n)], onward_in[g]))

        @pl.loop(0, 2 * tiles)
        def _(n):
            j = tile_of(g, n)
            lanes = pl.ds(pl.multiple_of(j * 128, 128), 128)
            backward = n >= tiles
            state = jnp.concatenate([incoming[4 * j + q] for q in range(4)], axis=0).astype(
                jnp.float32
            )
            for k in range(blocks):
                at = jnp.where(backward, blocks - 1 - k, k)
                before[at, :, lanes] = state.astype(jnp.bfloat16)
                state = state * decays[at, 0:1, lanes] + states[at, :, lanes]

    def finish(k, g):
        lanes = slice(g * span, (g + 1) * span)
        read = outward[rows_of(k), g * STATE : (g + 1) * STATE]
        scale = column[rows_of(k), :].astype(jnp.bfloat16)
        total = inner[rows_of(k), lanes]
        for way in range(2):
            placed = slice(way * half + g * span, way * half + (g + 1) * span)
            total = total + dot(read, before[k, :, placed]) * dot(scale, spread_read[:, placed])
        gated = total * gates[rows_of(k), lanes].astype(jnp.float32)
        level = lax.rsqrt(jnp.mean(gated * gated, axis=-1, keepdims=True) + EPSILON)
        mixed[rows_of(k), lanes] = (gated * level * gain_ref[:, lanes]).astype(jnp.bfloat16)

    def finish_shard(shard, g):
        @pl.loop(0, 2)
        def _(b):
            finish(2 * shard + b, g)

    def lanes_of(g):
        return pl.ds(g * span, span)

    def part(shard, some, g):
        start, size = some
        return mixed.at[
            pl.ds(pl.multiple_of(shard * rows + start, middle), size), lanes_of(g)
        ]

    mixed_out, from_below, from_above, from_far = [wire.flag() for _ in range(4)]
    relayed = [wire.flag() for _ in range(groups)]
    wire.sent.append((shards, mixed_out))

    def hand_on(g):
        wire.landed(relay.at[:, :, lanes_of(g)], relayed[g])
        for half_at, to, target in (
            (0, up, shards.at[step(x, 3), low, lanes_of(g)]),
            (1, down, shards.at[step(x, 1), high, lanes_of(g)]),
        ):
            wire.go(relay.at[half_at, :, lanes_of(g)], to, mixed_out, from_far, target)

    for g in range(groups):
        carry(g)
        for half_at, to in ((0, up), (1, down)):
            finish(2 * step(x, 2) + half_at, g)
            wire.go(
                part(step(x, 2), (half_at * middle, middle), g),
                to,
                mixed_out,
                relayed[g],
                relay.at[half_at, :, lanes_of(g)],
            )
        for by, to, flag in ((1, up, from_below), (3, down, from_above)):
            finish_shard(step(x, by), g)
            wire.go(
                part(step(x, by), (0, rows), g), to, mixed_out, flag, shards.at[x, :, lanes_of(g)]
            )
        finish_shard(x, g)
        if g:
            hand_on(g - 1)
    lo_second.finish()
    across("o", wo, "z", 2, (0, 2))
    hi_second.finish()
    across("o", wo, "y", 2, (2, 2))
    shards[x] = mixed[pl.ds(pl.multiple_of(x * rows, rows), rows), :]
    def contribute(at, begin, end):
        @pl.loop(0, 2)
        def _(k):
            lines = pl.ds(pl.multiple_of(k * 1024, 1024), 1024)
            total = dot_nt(wo[pl.ds(2 * k, 2), :, :, at].reshape(1024, -1), shards[at])
            if not begin:
                total = total + summed[lines, :]
            if end:
                out_ref[:, lines] = total.T.astype(out_ref.dtype)
            else:
                summed[lines, :] = total

    hand_on(groups - 1)
    crossed("o", wo)
    contribute(x, True, False)

    wire.landed(shards.at[0], from_below)
    contribute(step(x, 3), False, False)
    wire.landed(shards.at[0], from_above)
    contribute(step(x, 1), False, False)
    wire.landed(shards.at[0], from_far)
    contribute(step(x, 2), False, True)

    wire.drain()
    for g in range(groups):
        each_of(g, lambda n: wire.span(totals.at[pl.ds(0, n)], totals_out[g]).wait_send())


FLAGS = 60


def mix(
    tokens,
    norm_gain,
    w_gate,
    w_value,
    w_state_in,
    w_state_out,
    w_step_forward,
    w_step_backward,
    step_offset,
    fading_speed,
    conv_value,
    conv_state_in,
    conv_state_out,
    out_gain,
    w_out,
):
    rows, width = tokens.shape
    depth, half = w_value.shape
    states = w_state_in.shape[1]
    blocks = 4 * rows // BLOCK
    anywhere = pl.BlockSpec(memory_space=pl.ANY)
    bf16, f32 = jnp.bfloat16, jnp.float32
    return pl.pallas_call(
        functools.partial(mixer_kernel, math.log(4 * rows * lax.axis_size(SP))),
        out_shape=pltpu.VMEM((rows, width), OUT_TYPE),
        in_specs=[anywhere] * 15,
        out_specs=pl.BlockSpec(memory_space=pltpu.VMEM),
        scratch_shapes=[
            pltpu.VMEM((1, width), f32),
            pltpu.VMEM(w_step_forward.shape[::-1], bf16),
            pltpu.VMEM(w_step_backward.shape[::-1], bf16),
            pltpu.VMEM(conv_value.shape, f32),
            pltpu.VMEM(conv_state_in.shape, f32),
            pltpu.VMEM(conv_state_out.shape, f32),
            pltpu.VMEM(step_offset.shape, f32),
            pltpu.VMEM(fading_speed.shape, f32),
            pltpu.VMEM((1, half), f32),
            pltpu.VMEM((16, 128), f32),
            pltpu.VMEM((rows, 128), f32),
            pltpu.VMEM((blocks, 8, 128), f32),
            pltpu.VMEM((4, rows, width), bf16),
            pltpu.VMEM((2 * HALO, width), bf16),
            pltpu.VMEM((4 * rows + 2 * HALO, width), bf16),
            pltpu.VMEM((4, 4, 2, depth, half), bf16),
            pltpu.VMEM((4, 4, 2, depth, 2 * states + 128), bf16),
            pltpu.VMEM((4, 4, 2, depth, half), bf16),
            pltpu.VMEM((4, 4, 2, 4, depth, half), bf16),
            pltpu.VMEM((4 * rows + 2 * HALO, 2 * half), bf16),
            pltpu.VMEM((4 * rows, half), bf16),
            pltpu.VMEM((4 * rows, 128), bf16),
            pltpu.VMEM((4 * rows, half), bf16),
            pltpu.VMEM((4 * rows, states), bf16),
            pltpu.VMEM((4 * rows, states), bf16),
            pltpu.VMEM((4 * rows, 128), f32),
            pltpu.VMEM((blocks, 24, 128), f32),
            pltpu.VMEM((blocks, STATE, 2 * half), f32),
            pltpu.VMEM((blocks, 8, 2 * half), f32),
            pltpu.VMEM((blocks, STATE, 2 * half), bf16),
            pltpu.VMEM((4 * rows, half), f32),
            pltpu.VMEM((32, 48, 128), bf16),
            pltpu.VMEM((32, 48, 128), bf16),
            pltpu.VMEM((32, 32, 128), bf16),
            pltpu.VMEM((32, 32, 128), bf16),
            pltpu.VMEM((4 * rows, half), bf16),
            pltpu.VMEM((4, rows, half), bf16),
            pltpu.VMEM((2, rows // 2, half), bf16),
            pltpu.VMEM((width, rows), f32),
            pltpu.SemaphoreType.DMA((FLAGS,)),
            pltpu.SemaphoreType.DMA((15,)),
        ],
        compiler_params=pltpu.CompilerParams(
            collective_id=0, has_side_effects=True, vmem_limit_bytes=60 * 2**20
        ),
        name="mixer",
    )(
        tokens,
        w_value,
        w_state_in,
        w_state_out,
        w_gate,
        w_out.T,
        norm_gain.reshape(1, -1),
        w_step_forward.T,
        w_step_backward.T,
        conv_value,
        conv_state_in,
        conv_state_out,
        step_offset,
        fading_speed,
        out_gain.reshape(1, -1),
    )


OUT_TYPE = jnp.bfloat16


def local(
    input_activations,
    norm_gain,
    w_gate,
    w_value,
    w_state_in,
    w_state_out,
    w_step_forward,
    w_step_backward,
    step_offset,
    fading_speed,
    conv_value,
    conv_state_in,
    conv_state_out,
    out_gain,
    w_out,
):
    return mix(
        input_activations,
        norm_gain,
        w_gate,
        w_value,
        w_state_in,
        w_state_out,
        w_step_forward,
        w_step_backward,
        step_offset,
        fading_speed,
        conv_value,
        conv_state_in,
        conv_state_out,
        out_gain,
        w_out,
    )


def solution(mesh):
    torus = Mesh(mesh.devices.reshape(4, 4, 2, 4), SP_TP)
    return jax.shard_map(
        local,
        mesh=torus,
        in_specs=(
            P(SP_TP, None),
            P(),
            P(SP, "x"),
            P(SP, "x"),
            P(SP, "x"),
            P(SP, "x"),
            P(SP, "x"),
            P(SP, "x"),
            P(None, "x"),
            P(None, "x"),
            P(None, "x"),
            P(None, "x"),
            P(None, "x"),
            P("x"),
            P("x", SP),
        ),
        out_specs=P(SP_TP, None),
        check_vma=False,
    )
```
